32 devices in a mesh: ep: 8 (over z, x), tp: 4 (over y, core).
Axes of the slice: x: 2, y: 2, z: 4, core: 2. Of those that a mesh axis runs over, the one named last changes fastest.
Arguments:
- query_latent: bfloat16 [2048, 768], P('ep'), may hold values from -600 to 600
- shared_latent: bfloat16 [2048, 512], P('ep'), may hold values from -600 to 600
- rotary_key: bfloat16 [2048, 64], P('ep'), may hold values from -2500 to 2500
- query_gain: float32 [768], replicated, may hold values from 0.1 to 1.9
- shared_gain: float32 [512], replicated, may hold values from 0.1 to 1.9
- query_plain_weight: bfloat16 [768, 2048], P(None, 'tp'), may hold values from -0.21875 to 0.21875
- query_turn_weight: bfloat16 [768, 1024], P(None, 'tp'), may hold values from -0.21875 to 0.21875
- key_weight: bfloat16 [512, 2048], P(None, 'tp'), may hold values from -0.25 to 0.25
- value_weight: bfloat16 [512, 2048], P(None, 'tp'), may hold values from -0.25 to 0.25
- mixer_out_weight: bfloat16 [2048, 2048], P('tp'), may hold values from -1 to 1
- expert_input: bfloat16 [1024, 2048], P('ep'), may hold values from -600 to 600
- expert_gain: float32 [2048], replicated, may hold values from 0.1 to 1.9
- routing: int32 [1024, 4], P('ep'), may hold values from 0 to 7, all different within a row; in each aligned block of 128 rows (0 to 127, 128 to 255, ...) at most 85 rows name the same one
- routing_weight: float32 [1024, 4], P('ep'), may hold values from 0.05 to 1
- gate_weight: bfloat16 [8, 2048, 2048], P('ep', None, 'tp'), may hold values from -0.375 to 0.375
- up_weight: bfloat16 [8, 2048, 2048], P('ep', None, 'tp'), may hold values from -0.375 to 0.375
- down_weight: bfloat16 [8, 2048, 2048], P('ep', 'tp'), may hold values from -0.01953125 to 0.01953125
Outputs:
- mixer_output: bfloat16 [2048, 2048], P('ep')
- expert_output: bfloat16 [1024, 2048], P('ep')
The draws below stay inside these ranges and needn't reach their ends.
Inputs may be any that keep to these rules, and one draw needn't show every extreme that they name: `routing`: each row names 4 different experts. In each aligned block of 128 rows (the rows of one index of ep) no expert is named by more than 85 rows, and in some block some expert is named by exactly 85.
All inputs are finite; a program needn't handle non-finite values.
Results may differ from the reference program's by a relative error of at most 0.019.
Values may be sent and summed in bfloat16 or wider, within the bound.
A program may use at most 128 MiB of HBM per device.

```python
import math
import jax
import jax.numpy as jnp
import numpy as np
from jax import lax

D = 2048
HEADS = 16
NOPE = 128
ROPE = 64
VDIM = 128
Q_RANK = 768
KV_RANK = 512
FF = 2048
TOPK = 4
M_DEV = 128
SEQ = 2048
TOK_M = 1024
EXPERTS = 8
CAP_DEV = 85
N_EP = 8
N_TP = 4


def spread_normal(key, row_count, col_count):
    key_base = jax.random.fold_in(key, 0)
    base_draw = jnp.clip(jax.random.normal(key_base, (row_count, col_count), jnp.float32), -6.0, 6.0)
    return base_draw


def draw_query_latent(key, part):
    return spread_normal(jax.random.fold_in(key, 11), SEQ, Q_RANK).astype(jnp.bfloat16)


def draw_shared_latent(key, part):
    return spread_normal(jax.random.fold_in(key, 12), SEQ, KV_RANK).astype(jnp.bfloat16)


def draw_expert_input(key, part):
    return spread_normal(jax.random.fold_in(key, 13), TOK_M, D).astype(jnp.bfloat16)


def draw_rotary_key(key, part):
    key_base = jax.random.fold_in(jax.random.fold_in(key, 14), 0)
    base_draw = jnp.clip(jax.random.normal(key_base, (SEQ, ROPE), jnp.float32), -6.0, 6.0)
    return base_draw.astype(jnp.bfloat16)


def block_levels(key, extent, shards, least, top_value):
    level, own = 1.0, jax.random.fold_in(key, 6)
    for axis_at, parts in shards:
        steps = jnp.exp(jax.random.uniform(jax.random.fold_in(own, axis_at), (parts,), jnp.float32, least / len(shards), top_value / len(shards)))
        level = level * jnp.repeat(steps, extent[axis_at] // parts).reshape([-1 if axis == axis_at else 1 for axis in range(len(extent))])
    return level


def shared_out(stream_key, own, number, rows, count, top, reach, slope):
    order = jax.random.permutation(stream_key, count)
    crowded, ordinary = load_shares(count, rows * top, reach, slope, True), load_shares(count, rows * top, reach, slope, False)
    places = jnp.arange(count)

    def named(sizes, offset_by):
        used = int((sizes > 0).sum())
        fixed = max(1, used // 4)
        shifted = fixed + (places - fixed + offset_by * (used - fixed)) % max(1, count - fixed)
        return jnp.zeros((count,), jnp.int32).at[order[jnp.where(places < fixed, places, shifted)]].set(jnp.asarray(sizes, jnp.int32))

    sizes = jnp.where(number % 4 == 0, named(crowded, number // 4), named(ordinary, number - number // 4 - 1))
    mixed = jax.random.permutation(jax.random.fold_in(own, 3), count)
    source_of, receiver = mixed[0:count // 2 * 2:2], mixed[1:count // 2 * 2:2]
    margin = jnp.minimum(sizes[source_of] - 1, reach - sizes[receiver]) // 2
    margin = jnp.where((source_of == order[0]) | (receiver == order[0]) | (sizes[receiver] == 0), 0, jnp.maximum(margin, 0))
    shifted = jax.random.randint(jax.random.fold_in(own, 4), (count // 2,), 0, 1 << 20) % (margin + 1)
    sizes = sizes.at[source_of].add(-shifted).at[receiver].add(shifted)
    members = jnp.searchsorted(jnp.cumsum(sizes), jnp.arange(rows * top), side="right").astype(jnp.int32)
    listing = members.reshape(top, rows).T
    listing = listing[jax.random.permutation(jax.random.fold_in(own, 1), rows)]
    offset_by = jax.random.randint(jax.random.fold_in(own, 2), (rows, 1), 0, top)
    return jnp.take_along_axis(listing, (jnp.arange(top)[None, :] + offset_by) % top, axis=1)


def load_shares(number_of, total, most, skew, full):
    loads = [(1 << 20) // math.isqrt(rank ** skew) + 1 for rank in range(1, number_of + 1)]
    largest = most if full else min(most, max(-(-total // number_of), total * loads[0] // sum(loads)))
    least = 1 if total - largest >= number_of - 1 else 0
    counts, surplus = [largest] + [least] * (number_of - 1), total - largest - least * (number_of - 1)
    while surplus > 0:
        candidates = [i for i in range(1, number_of) if counts[i] < largest] or [i for i in range(1, number_of) if counts[i] < most]
        pool, left = sum([loads[i] for i in candidates]), surplus
        for i in candidates:
            addition = min(most - counts[i], max(1, left * loads[i] // pool), surplus)
            counts[i] = counts[i] + addition
            surplus = surplus - addition
    return np.array(counts)


def bell_draw(stream_key, extent, spread, reach, pieces=(), kind=jnp.bfloat16):
    values = spread * jax.random.normal(stream_key, extent, jnp.float32)
    if pieces:
        values = values * block_levels(stream_key, extent, pieces, -0.22, 0.18)
    return jnp.clip(values, -reach, reach).astype(kind)


def setup_inputs(seed: int = 0) -> dict:
    streams_of = jax.random.split(jax.random.key(seed), 18)
    query_latent = draw_query_latent(jax.random.fold_in(streams_of[17], 71), 0)
    shared_latent = draw_shared_latent(jax.random.fold_in(streams_of[17], 71), 0)
    rotary_key = draw_rotary_key(jax.random.fold_in(streams_of[17], 71), 0)
    query_gain = jnp.clip(1.0 + 0.18 * jax.random.normal(streams_of[3], (Q_RANK,), jnp.float32), 0.1, 1.9)
    shared_gain = jnp.clip(1.0 + 0.18 * jax.random.normal(streams_of[4], (KV_RANK,), jnp.float32), 0.1, 1.9)
    query_plain_weight = bell_draw(streams_of[5], (Q_RANK, HEADS * NOPE), Q_RANK ** -0.5, 0.21875, ((1, 4),))
    query_turn_weight = bell_draw(streams_of[6], (Q_RANK, HEADS * ROPE), Q_RANK ** -0.5, 0.21875, ((1, 4),))
    key_weight = bell_draw(streams_of[7], (KV_RANK, HEADS * NOPE), KV_RANK ** -0.5, 0.25, ((1, 4),))
    value_weight = bell_draw(streams_of[8], (KV_RANK, HEADS * VDIM), KV_RANK ** -0.5, 0.25, ((1, 4),))
    mixer_out_weight = bell_draw(streams_of[9], (HEADS * VDIM, D), (HEADS * VDIM // 64) ** -0.5, 1.0, ((0, 4),))
    expert_input = draw_expert_input(jax.random.fold_in(streams_of[17], 71), 0)
    expert_gain = jnp.clip(1.0 + 0.18 * jax.random.normal(streams_of[11], (D,), jnp.float32), 0.1, 1.9)
    routing_keys = jax.random.split(jax.random.fold_in(streams_of[12], 1), TOK_M // M_DEV)
    routing_turns = jax.random.permutation(jax.random.fold_in(streams_of[12], 3), TOK_M // M_DEV)
    routing = jax.vmap(lambda own, number: shared_out(jax.random.fold_in(streams_of[12], 2), own, number, M_DEV, EXPERTS, TOPK, CAP_DEV, 1))(routing_keys, routing_turns).reshape((TOK_M, TOPK))
    routing_weight = jnp.clip(jnp.exp(math.log(1.0) - 2.9957323 * jax.random.uniform(streams_of[13], (TOK_M, TOPK), jnp.float32) ** block_levels(streams_of[13], (TOK_M, TOPK), ((0, 8),), -0.2, 0.2)), 0.05, 1.0)
    gate_weight = bell_draw(streams_of[14], (EXPERTS, D, FF), (D // 9) ** -0.5, 0.375, ((0, 8), (2, 4)))
    up_weight = bell_draw(streams_of[15], (EXPERTS, D, FF), (D // 9) ** -0.5, 0.375, ((0, 8), (2, 4)))
    down_weight = bell_draw(streams_of[16], (EXPERTS, FF, D), (FF * 40) ** -0.5, 0.01953125, ((0, 8), (1, 4)))
    return dict(query_latent=query_latent, shared_latent=shared_latent, rotary_key=rotary_key, query_gain=query_gain, shared_gain=shared_gain, query_plain_weight=query_plain_weight, query_turn_weight=query_turn_weight, key_weight=key_weight, value_weight=value_weight, mixer_out_weight=mixer_out_weight, expert_input=expert_input, expert_gain=expert_gain, routing=routing, routing_weight=routing_weight, gate_weight=gate_weight, up_weight=up_weight, down_weight=down_weight)


EPSILON = 1e-06
CLAMP_LIMIT = 7.0
SLOPE = 1.702
ROTARY_BASE = 10000.0

def norm_rows(values, gains):
    widened = values.astype(jnp.float32)
    normed = widened * lax.rsqrt(lax.optimization_barrier(jnp.mean(widened * widened, axis=-1, keepdims=True)) + EPSILON)
    return (normed * gains).astype(jnp.bfloat16)

def rotary(values, position):
    half_dim = values.shape[-1] // 2
    frequency = ROTARY_BASE ** (-2.0 * jnp.arange(half_dim, dtype=jnp.float32) / values.shape[-1])
    angles = position.astype(jnp.float32)[:, None, None] * frequency[None, None, :]
    cosine = jnp.cos(angles)
    sine_part = jnp.sin(angles)
    lower = values[..., :half_dim]
    upper = values[..., half_dim:]
    return jnp.concatenate([lower * cosine - upper * sine_part, upper * cosine + lower * sine_part], axis=-1)

def mixer_reference(query_latent, shared_latent, rotary_key, query_gain, shared_gain, query_plain_weight, query_turn_weight, key_weight, value_weight, mixer_out_weight):
    seq_len = query_latent.shape[0]
    position = jnp.arange(seq_len, dtype=jnp.int32)
    query_normed = norm_rows(query_latent, query_gain)
    shared_normed = norm_rows(shared_latent, shared_gain)
    query_plain = jnp.dot(query_normed, query_plain_weight, preferred_element_type=jnp.float32).astype(jnp.bfloat16)
    query_plain = query_plain.reshape(seq_len, HEADS, NOPE)
    query_raw = jnp.dot(query_normed, query_turn_weight, preferred_element_type=jnp.float32)
    query_turned = rotary(query_raw.reshape(seq_len, HEADS, ROPE), position).astype(jnp.bfloat16)
    key_plain = jnp.dot(shared_normed, key_weight, preferred_element_type=jnp.float32).astype(jnp.bfloat16)
    key_plain = key_plain.reshape(seq_len, HEADS, NOPE).astype(jnp.float32)
    values = jnp.dot(shared_normed, value_weight, preferred_element_type=jnp.float32).astype(jnp.bfloat16)
    values = values.reshape(seq_len, HEADS, VDIM).astype(jnp.float32)
    key_turned = rotary(rotary_key.astype(jnp.float32).reshape(seq_len, 1, ROPE), position)
    key_turned = key_turned.astype(jnp.bfloat16).reshape(seq_len, ROPE).astype(jnp.float32)
    scaling = (NOPE + ROPE) ** (-0.5)
    block_rows = 256 if seq_len % 256 == 0 else seq_len
    block_count = seq_len // block_rows
    key_index = jnp.arange(seq_len, dtype=jnp.int32)

    def attend(first_row):
        plain_block = lax.dynamic_slice_in_dim(query_plain, first_row, block_rows, 0).astype(jnp.float32)
        turned_block = lax.dynamic_slice_in_dim(query_turned, first_row, block_rows, 0).astype(jnp.float32)
        scores = jnp.einsum('qhd,khd->hqk', plain_block, key_plain)
        scores = (scores + jnp.einsum('qhr,kr->hqk', turned_block, key_turned)) * scaling
        query_index = first_row + jnp.arange(block_rows, dtype=jnp.int32)
        visible = key_index[None, :] <= query_index[:, None]
        scores = jnp.where(visible[None], scores, -jnp.inf)
        peak = lax.optimization_barrier(jnp.max(scores, axis=-1, keepdims=True))
        probs = jnp.exp(scores - peak)
        totals = lax.optimization_barrier(jnp.sum(probs, axis=-1))
        rounded = lax.optimization_barrier(probs.astype(jnp.bfloat16))
        summed = jnp.einsum('hqk,khd->qhd', rounded.astype(jnp.float32), values)
        return (summed / jnp.transpose(totals)[:, :, None]).astype(jnp.bfloat16)
    starts = jnp.arange(block_count, dtype=jnp.int32) * block_rows
    heads_out = lax.map(attend, starts).reshape(seq_len, HEADS * VDIM)
    group_width = HEADS // N_TP * VDIM
    groups = jnp.transpose(heads_out.reshape(seq_len, N_TP, group_width), (1, 0, 2))
    weight_groups = mixer_out_weight.reshape(N_TP, group_width, D)

    def add_group(running, pair):
        part_rows, part_weight = pair
        term = jnp.dot(part_rows, part_weight, preferred_element_type=jnp.float32).astype(jnp.bfloat16)
        term = lax.optimization_barrier(term)
        return (running + term.astype(jnp.float32), None)
    summed, unused = lax.scan(add_group, jnp.zeros((seq_len, D), jnp.float32), (groups, weight_groups))
    return summed.astype(jnp.bfloat16)

def expert_reference(expert_input, expert_gain, routing, routing_weight, gate_weight, up_weight, down_weight):
    normed = norm_rows(expert_input, expert_gain)
    token_count = normed.shape[0]
    capacity_all = N_EP * CAP_DEV
    token_ids = jnp.arange(token_count, dtype=jnp.int32)
    ff_group = FF // N_TP

    def one_expert(running, inputs):
        expert, gate_part, up_part, down_part = inputs
        matches = routing == expert
        weight = lax.optimization_barrier(jnp.sum(jnp.where(matches, routing_weight, 0.0), axis=1))
        is_member = jnp.any(matches, axis=1)
        placed = jnp.cumsum(is_member.astype(jnp.int32)) - 1
        placed = jnp.where(is_member, placed, capacity_all).astype(jnp.int32)
        chosen = jnp.zeros((capacity_all,), jnp.int32).at[placed].set(token_ids, mode='drop')
        chosen_weight = jnp.zeros((capacity_all,), jnp.float32).at[placed].set(weight, mode='drop')
        picked = normed[chosen]
        gate_pre = jnp.minimum(jnp.dot(picked, gate_part, preferred_element_type=jnp.float32), CLAMP_LIMIT)
        up_pre = jnp.clip(jnp.dot(picked, up_part, preferred_element_type=jnp.float32), -CLAMP_LIMIT, CLAMP_LIMIT)
        hidden = ((up_pre + 1.0) * (gate_pre * jax.nn.sigmoid(SLOPE * gate_pre))).astype(jnp.bfloat16)
        grouped = hidden.reshape(capacity_all, N_TP, ff_group).astype(jnp.float32)
        down_groups = down_part.reshape(N_TP, ff_group, D).astype(jnp.float32)
        partial_value = jnp.einsum('mnf,nfd->nmd', grouped, down_groups).astype(jnp.bfloat16)
        partial_value = lax.optimization_barrier(partial_value)
        result = lax.optimization_barrier(jnp.sum(partial_value.astype(jnp.float32), axis=0)).astype(jnp.bfloat16)
        result = lax.optimization_barrier(result)
        running = running.at[chosen].add(chosen_weight[:, None] * result.astype(jnp.float32))
        return (running, None)
    experts = jnp.arange(gate_weight.shape[0], dtype=jnp.int32)
    total, unused = lax.scan(one_expert, jnp.zeros((token_count, D), jnp.float32), (experts, gate_weight, up_weight, down_weight))
    return total.astype(jnp.bfloat16)

def reference(query_latent, shared_latent, rotary_key, query_gain, shared_gain, query_plain_weight, query_turn_weight, key_weight, value_weight, mixer_out_weight, expert_input, expert_gain, routing, routing_weight, gate_weight, up_weight, down_weight):
    mixer_output = mixer_reference(query_latent, shared_latent, rotary_key, query_gain, shared_gain, query_plain_weight, query_turn_weight, key_weight, value_weight, mixer_out_weight)
    expert_output = expert_reference(expert_input, expert_gain, routing, routing_weight, gate_weight, up_weight, down_weight)
    return (mixer_output, expert_output)
```

```python
import functools

import jax
import jax.numpy as jnp
import numpy as np
from jax import lax
from jax.experimental import pallas as pl
from jax.experimental.pallas import tpu as pltpu
from jax.sharding import PartitionSpec as P

NOPE = 128
ROPE = 64
VDIM = 128
LANES = 128
CORES = 2

EPSILON = 1e-06
CLAMP_LIMIT = 7.0
SLOPE = 1.702
ROTARY_BASE = 10000.0
NEGATIVE = -1e30
VMEM_LIMIT = 60 * 1024 * 1024
F32 = jnp.float32
BF16 = jnp.bfloat16


def norm_scale(values):
    widened = values.astype(F32)
    return widened * lax.rsqrt(jnp.mean(widened * widened, axis=-1, keepdims=True) + EPSILON)


def norm_rows(values, gains):
    return (norm_scale(values) * gains).astype(BF16)


def rotate_heads(values, position):
    half = ROPE // 2
    lane = jnp.arange(values.shape[-1], dtype=jnp.int32)
    frequency = ROTARY_BASE ** (-2.0 * (lane % half).astype(F32) / ROPE)
    angles = position.astype(F32)[:, None] * frequency[None, :]
    upper = (lane % ROPE >= half)[None, :]
    swapped = jnp.where(upper, jnp.roll(values, half, axis=1), -jnp.roll(values, -half, axis=1))
    return values * jnp.cos(angles) + swapped * jnp.sin(angles)


def remote(src, dst, send_sem, recv_sem, ep, tp):
    return pltpu.make_async_remote_copy(
        src_ref=src,
        dst_ref=dst,
        send_sem=send_sem,
        recv_sem=recv_sem,
        device_id=(ep, tp),
        device_id_type=pl.DeviceIdType.MESH,
    )


def enter(n_ep, n_tp, me_e, me_t):
    barrier = pltpu.get_barrier_semaphore()
    for d in range(1, n_ep):
        pl.semaphore_signal(
            barrier,
            inc=1,
            device_id=(lax.rem(me_e + d, n_ep), me_t),
            device_id_type=pl.DeviceIdType.MESH,
        )
    for k in range(1, n_tp):
        pl.semaphore_signal(
            barrier,
            inc=1,
            device_id=(me_e, lax.rem(me_t + k, n_tp)),
            device_id_type=pl.DeviceIdType.MESH,
        )
    pl.semaphore_wait(barrier, n_ep - 1 + n_tp - 1)


def gather_kernel(
    n_ep,
    n_tp,
    heads,
    lat,
    disp,
    queries,
    key_w,
    value_w,
    mixer_w,
    arr,
    mpart,
    lat_all,
    out,
    keys,
    values,
    loc_sem,
    ep_s,
    ep_r,
    y_s,
    y_r,
    c_s,
    c_r,
):
    me_e = lax.axis_index("ep")
    me_t = lax.axis_index("tp")
    n_y = n_tp // CORES
    y = me_t // CORES
    c = lax.rem(me_t, CORES)
    mate = y * CORES + (1 - c)
    width = disp.shape[2]

    def place(j, e, t):
        if j == 0:
            return lat_all.at[e, t]
        return arr.at[e, :, pl.ds(pl.multiple_of(t * width, LANES), width)]

    local = []
    for j in range(2):
        copy = pltpu.make_async_copy(
            lat if j == 0 else disp.at[me_e], place(j, me_e, me_t), loc_sem.at[j]
        )
        copy.start()
        local.append(copy)
    enter(n_ep, n_tp, me_e, me_t)
    sends = []
    for j in range(2):
        for d in range(1, n_ep):
            peer = lax.rem(me_e + d, n_ep)
            copy = remote(
                lat if j == 0 else disp.at[peer],
                place(j, me_e, me_t),
                ep_s.at[d, j],
                ep_r.at[d, j],
                peer,
                me_t,
            )
            copy.start()
            sends.append(copy)

    def relay(j, d):
        src = lax.rem(me_e - d + n_ep, n_ep)
        here = place(j, src, me_t)
        if d == 0:
            local[j].wait()
        else:
            remote(here, here, ep_s.at[d, j], ep_r.at[d, j], src, me_t).wait_recv()
        for k in range(1, n_y):
            to = lax.rem(y + k, n_y) * CORES + c
            copy = remote(here, here, y_s.at[d, k, j], y_r.at[d, k, j], me_e, to)
            copy.start()
            sends.append(copy)
        copy = remote(here, here, c_s.at[d, 0, j], c_r.at[d, 0, j], me_e, mate)
        copy.start()
        sends.append(copy)

    def forward(j, d):
        src = lax.rem(me_e - d + n_ep, n_ep)
        for k in range(1, n_y):
            got = place(j, src, lax.rem(y - k + n_y, n_y) * CORES + c)
            remote(got, got, y_s.at[d, k, j], y_r.at[d, k, j], me_e, me_t).wait_recv()
            copy = remote(got, got, c_s.at[d, k, j], c_r.at[d, k, j], me_e, mate)
            copy.start()
            sends.append(copy)

    def arrive(j, d):
        src = lax.rem(me_e - d + n_ep, n_ep)
        for k in range(n_y):
            got = place(j, src, lax.rem(y - k + n_y, n_y) * CORES + (1 - c))
            remote(got, got, c_s.at[d, k, j], c_r.at[d, k, j], me_e, mate).wait_recv()

    for d in range(n_ep):
        relay(0, d)
        if d > 0:
            forward(0, d - 1)
    relay(1, 0)
    forward(0, n_ep - 1)
    for d in range(n_ep):
        arrive(0, d)
        if d % 2 == 1 and d // 2 + 1 < n_ep // 2:
            relay(1, d // 2 + 1)
        project(
            lax.rem(me_e - d + n_ep, n_ep), n_tp, heads, lat_all, key_w, value_w, keys, values
        )
    done = n_ep // 2
    for h in range(heads):
        attend(h, me_e, queries, keys, values, out)
        until = n_ep if h == heads - 1 else n_ep // 2 + (h + 1) * (n_ep // 2) // heads
        for d in range(done, until):
            relay(1, d)
        done = until
    mpart[...] = jnp.dot(out[...], mixer_w[...], preferred_element_type=F32).astype(BF16)
    for d in range(n_ep):
        forward(1, d)
    for d in range(n_ep):
        arrive(1, d)
    for copy in sends:
        copy.wait_send()


def project(e, n_tp, heads, lat_all, key_w, value_w, keys, values):
    share = lat_all.shape[2]
    rows = n_tp * share
    rank = key_w.shape[0]
    head_keys = NOPE + LANES
    at = pl.ds(pl.multiple_of(e * rows, rows), rows)
    block = lat_all[e].reshape(rows, rank + LANES)
    latent = block[:, :rank]
    k = jnp.dot(latent, key_w[...], preferred_element_type=F32).astype(BF16)
    values[at, :] = jnp.dot(latent, value_w[...], preferred_element_type=F32).astype(BF16)
    for h in range(heads):
        keys[at, h * head_keys : h * head_keys + NOPE] = k[:, h * NOPE : (h + 1) * NOPE]
        keys[at, h * head_keys + NOPE : (h + 1) * head_keys] = block[:, rank:]


def attend(h, me_e, queries, keys, values, out):
    rows = queries.shape[0]
    total = keys.shape[0]
    head_keys = NOPE + LANES
    row = lax.broadcasted_iota(jnp.int32, (rows, total), 0) + me_e * rows
    visible = lax.broadcasted_iota(jnp.int32, (rows, total), 1) <= row
    scaling = (NOPE + ROPE) ** (-0.5)
    cols = slice(h * head_keys, (h + 1) * head_keys)
    scores = lax.dot_general(
        queries[:, cols], keys[:, cols], (((1,), (1,)), ((), ())), preferred_element_type=F32
    )
    scores = jnp.where(visible, scores * scaling, NEGATIVE)
    weight = jnp.exp(scores - jnp.max(scores, axis=-1, keepdims=True))
    sums = jnp.sum(weight, axis=-1, keepdims=True)
    mixed = jnp.dot(
        weight.astype(BF16), values[:, h * VDIM : (h + 1) * VDIM], preferred_element_type=F32
    )
    out[:, h * VDIM : (h + 1) * VDIM] = (mixed / sums).astype(BF16)


def return_kernel(
    n_ep,
    n_tp,
    arrived,
    gate_hbm,
    up_hbm,
    down_hbm,
    mix,
    mpart,
    eout,
    mout,
    gate_w,
    up_w,
    down_w,
    load_sem,
    part,
    ca,
    sums,
    ya,
    res,
    ret,
    mca,
    msums,
    mya,
    ca_s,
    ca_r,
    ya_s,
    ya_r,
    ep_s,
    ep_r,
    oy_s,
    oy_r,
    oc_s,
    oc_r,
):
    me_e = lax.axis_index("ep")
    me_t = lax.axis_index("tp")
    n_y = n_tp // CORES
    y = me_t // CORES
    c = lax.rem(me_t, CORES)
    mate = y * CORES + (1 - c)
    width = res.shape[2]
    capacity = res.shape[1]
    pairs = n_ep // 2
    parity = lax.rem(me_e, 2)
    loads = []
    for n, (src, dst) in enumerate(((gate_hbm, gate_w), (up_hbm, up_w), (down_hbm, down_w))):
        copy = pltpu.make_async_copy(src.at[0], dst, load_sem.at[n])
        copy.start()
        loads.append(copy)

    def twin(i):
        return parity if i % 2 == 0 else 1 - parity

    def dest(i):
        return lax.rem(me_e // 2 + i // 2, pairs) * 2 + twin(i)

    def source(i):
        return lax.rem(me_e // 2 - i // 2 + pairs, pairs) * 2 + twin(i)

    def cols(t):
        return pl.ds(pl.multiple_of(t * width, LANES), width)

    def part_at(i, t):
        if i == n_ep:
            return mpart.at[:, cols(t)]
        return part.at[dest(i), :, cols(t)]

    def part_load(i, t):
        if i == n_ep:
            return mpart[:, cols(t)].astype(F32)
        return part[dest(i), :, cols(t)].astype(F32)

    enter(n_ep, n_tp, me_e, me_t)
    sends = []

    def go(copy):
        copy.start()
        sends.append(copy)

    def core_copy(i, k):
        dst = mca.at[k] if i == n_ep else ca.at[i, k]
        return remote(
            part_at(i, lax.rem(y + k, n_y) * CORES + (1 - c)),
            dst,
            ca_s.at[i, k],
            ca_r.at[i, k],
            me_e,
            mate,
        )

    def y_copy(i, k):
        src, dst = (msums, mya) if i == n_ep else (sums.at[i], ya.at[i])
        to = lax.rem(y + k, n_y) * CORES + c
        return remote(src.at[k - 1], dst.at[k - 1], ya_s.at[i, k], ya_r.at[i, k], me_e, to)

    def core_step(i):
        for k in list(range(1, n_y)) + [0]:
            go(core_copy(i, k))

    def y_step(i):
        for k in range(1, n_y):
            core_copy(i, k).wait_recv()
            got = (mca[k] if i == n_ep else ca[i, k]).astype(F32)
            value = (got + part_load(i, lax.rem(y + k, n_y) * CORES + c)).astype(BF16)
            if i == n_ep:
                msums[k - 1] = value
            else:
                sums[i, k - 1] = value
            go(y_copy(i, k))

    def ep_copy(i, e):
        return remote(res.at[i], ret.at[i], ep_s.at[i], ep_r.at[i], e, me_t)

    def sum_step(i):
        core_copy(i, 0).wait_recv()
        value = (mca[0] if i == n_ep else ca[i, 0]).astype(F32) + part_load(i, me_t)
        for k in range(1, n_y):
            y_copy(i, k).wait_recv()
            value = value + (mya[k - 1] if i == n_ep else ya[i, k - 1]).astype(F32)
        if i == n_ep:
            mout[:, cols(me_t)] = value.astype(BF16)
        elif i == 0:
            ret[0] = value.astype(BF16)
        else:
            res[i] = value.astype(BF16)
            go(ep_copy(i, dest(i)))

    def expert_step(s):
        base = lax.rem(me_e // 2 + s, pairs) * 2
        rows = arrived[pl.ds(pl.multiple_of(base * capacity, 2 * capacity), 2 * capacity), :]
        if s == 1 % pairs:
            loads[0].wait()
            loads[1].wait()
        gate = jnp.minimum(jnp.dot(rows, gate_w[...], preferred_element_type=F32), CLAMP_LIMIT)
        up = jnp.clip(
            jnp.dot(rows, up_w[...], preferred_element_type=F32), -CLAMP_LIMIT, CLAMP_LIMIT
        )
        hidden = ((up + 1.0) * (gate * jax.nn.sigmoid(SLOPE * gate))).astype(BF16)
        if s == 1 % pairs:
            loads[2].wait()
        value = jnp.dot(hidden, down_w[...], preferred_element_type=F32)
        part[base] = value[:capacity].astype(BF16)
        part[base + 1] = value[capacity:].astype(BF16)

    def out_copy(j, k, t, to, sem_s, sem_r):
        ref = (mout if j == 0 else eout).at[:, cols(t)]
        return remote(ref, ref, sem_s.at[j, k], sem_r.at[j, k], me_e, to)

    def out_send(j):
        for k in range(1, n_y):
            go(out_copy(j, k, me_t, lax.rem(y + k, n_y) * CORES + c, oy_s, oy_r))
        go(out_copy(j, 0, me_t, mate, oc_s, oc_r))

    core_step(n_ep)
    turns = [n % pairs for n in range(1, pairs + 1)]
    for n, turn in enumerate(turns):
        expert_step(turn)
        for i in (2 * turn, 2 * turn + 1):
            core_step(i)
        if n == 0:
            y_step(n_ep)
        for i in (2 * turn, 2 * turn + 1):
            y_step(i)
        if n > 0:
            for i in (2 * turns[n - 1], 2 * turns[n - 1] + 1):
                sum_step(i)
    sum_step(n_ep)
    out_send(0)
    for i in (1, 0):
        sum_step(i)
    acc = None
    for i in [0] + list(range(2, n_ep)) + [1]:
        if i > 0:
            ep_copy(i, source(i)).wait_recv()
        mixing = mix[source(i)]
        high = mixing.astype(BF16)
        low = (mixing - high.astype(F32)).astype(BF16)
        rows = ret[i]
        term = jnp.dot(high, rows, preferred_element_type=F32) + jnp.dot(
            low, rows, preferred_element_type=F32
        )
        acc = term if acc is None else acc + term
    eout[:, cols(me_t)] = acc.astype(BF16)
    out_send(1)
    for j in range(2):
        for k in range(1, n_y):
            t = lax.rem(y - k + n_y, n_y) * CORES + c
            out_copy(j, k, t, me_t, oy_s, oy_r).wait_recv()
            go(out_copy(j, k, t, mate, oc_s, oc_r))
    for j in range(2):
        for k in range(n_y):
            t = lax.rem(y - k + n_y, n_y) * CORES + (1 - c)
            out_copy(j, k, t, mate, oc_s, oc_r).wait_recv()
    for copy in sends:
        copy.wait_send()


def vmem(count):
    return [pl.BlockSpec(memory_space=pltpu.VMEM)] * count


def per_device(
    n_ep,
    n_tp,
    query_latent,
    shared_latent,
    rotary_key,
    query_gain,
    shared_gain,
    query_plain_weight,
    query_turn_weight,
    key_weight,
    value_weight,
    mixer_out_weight,
    expert_input,
    expert_gain,
    routing,
    routing_weight,
    gate_weight,
    up_weight,
    down_weight,
):
    me_e = lax.axis_index("ep")
    me_t = lax.axis_index("tp")
    n_y = n_tp // CORES
    row_count = query_latent.shape[0]
    heads = query_plain_weight.shape[1] // NOPE
    rank = shared_latent.shape[1]

    share = row_count // n_tp
    first = me_t * share
    lat = norm_rows(lax.dynamic_slice_in_dim(shared_latent, first, share, 0), shared_gain)
    own_position = me_e * row_count + first + jnp.arange(share, dtype=jnp.int32)
    turned = rotate_heads(
        lax.dynamic_slice_in_dim(rotary_key, first, share, 0).astype(F32), own_position
    ).astype(BF16)
    lat = jnp.concatenate([lat, turned, jnp.zeros((share, LANES - ROPE), BF16)], axis=1)

    token_count, width = expert_input.shape
    top_count = routing.shape[1]
    capacity = 4 * token_count * top_count // (3 * n_ep)
    capacity = -(-capacity // 8) * 8
    part_width = width // n_tp
    normed = norm_rows(expert_input, expert_gain)
    normed = lax.dynamic_slice_in_dim(normed, me_t * part_width, part_width, 1)
    flattened = routing.reshape(token_count * top_count)
    matches = flattened[:, None] == jnp.arange(n_ep, dtype=jnp.int32)[None, :]
    count = token_count * top_count
    lower = jnp.arange(count)[:, None] > jnp.arange(count)[None, :]
    ranking = jnp.dot(
        lower.astype(BF16), matches.astype(BF16), preferred_element_type=F32
    ).astype(jnp.int32)
    slot_index = jnp.sum(jnp.where(matches, ranking, 0), axis=1)
    target = (flattened * capacity + slot_index).reshape(token_count, top_count)
    slot_ids = jnp.arange(n_ep * capacity, dtype=jnp.int32)
    table = jnp.zeros((n_ep * capacity, token_count), jnp.bool_)
    mixing = jnp.zeros((token_count, n_ep * capacity), F32)
    for k in range(top_count):
        table = table | (target[:, k][None, :] == slot_ids[:, None])
        mixing = mixing + jnp.where(
            target[:, k][:, None] == slot_ids[None, :], routing_weight[:, k][:, None], 0.0
        )
    disp = jnp.dot(table.astype(BF16), normed, preferred_element_type=F32).astype(BF16)
    disp = disp.reshape(n_ep, capacity, part_width)
    mixing = jnp.transpose(mixing.reshape(token_count, n_ep, capacity), (1, 0, 2))

    position = me_e * row_count + jnp.arange(row_count, dtype=jnp.int32)
    query_normed = norm_rows(query_latent, query_gain)
    query_plain = jnp.dot(query_normed, query_plain_weight, preferred_element_type=F32)
    query_plain = query_plain.astype(BF16)
    query_raw = jnp.dot(query_normed, query_turn_weight, preferred_element_type=F32)
    query_turned = rotate_heads(query_raw, position).astype(BF16)
    blank = jnp.zeros((row_count, LANES - ROPE), BF16)
    pieces = []
    for h in range(heads):
        pieces.append(query_plain[:, h * NOPE : (h + 1) * NOPE])
        pieces.append(query_turned[:, h * ROPE : (h + 1) * ROPE])
        pieces.append(blank)
    queries = jnp.concatenate(pieces, axis=1)
    total = n_ep * row_count
    dma = pltpu.SemaphoreType.DMA
    arrived, mixer_partial = pl.pallas_call(
        functools.partial(gather_kernel, n_ep, n_tp, heads),
        out_shape=(
            jax.ShapeDtypeStruct((n_ep, capacity, width), BF16),
            jax.ShapeDtypeStruct((row_count, width), BF16),
        ),
        in_specs=vmem(6),
        out_specs=vmem(2),
        scratch_shapes=[
            pltpu.VMEM((n_ep, n_tp, share, rank + LANES), BF16),
            pltpu.VMEM((row_count, heads * VDIM), BF16),
            pltpu.VMEM((total, heads * (NOPE + LANES)), BF16),
            pltpu.VMEM((total, heads * VDIM), BF16),
            dma((2,)),
            dma((n_ep, 2)),
            dma((n_ep, 2)),
            dma((n_ep, n_y, 2)),
            dma((n_ep, n_y, 2)),
            dma((n_ep, n_y, 2)),
            dma((n_ep, n_y, 2)),
        ],
        compiler_params=pltpu.CompilerParams(
            collective_id=0, has_side_effects=True, vmem_limit_bytes=VMEM_LIMIT
        ),
    )(lat, disp, queries, key_weight, value_weight, mixer_out_weight)
    arrived = arrived.reshape(n_ep * capacity, width)
    units = gate_weight.shape[2]

    expert_output, mixer_output = pl.pallas_call(
        functools.partial(return_kernel, n_ep, n_tp),
        out_shape=(
            jax.ShapeDtypeStruct((token_count, width), BF16),
            jax.ShapeDtypeStruct((row_count, width), BF16),
        ),
        in_specs=vmem(1) + [pl.BlockSpec(memory_space=pl.ANY)] * 3 + vmem(2),
        out_specs=vmem(2),
        scratch_shapes=[
            pltpu.VMEM((width, units), BF16),
            pltpu.VMEM((width, units), BF16),
            pltpu.VMEM((units, width), BF16),
            dma((3,)),
            pltpu.VMEM((n_ep, capacity, width), BF16),
            pltpu.VMEM((n_ep, n_y, capacity, part_width), BF16),
            pltpu.VMEM((n_ep, n_y - 1, capacity, part_width), BF16),
            pltpu.VMEM((n_ep, n_y - 1, capacity, part_width), BF16),
            pltpu.VMEM((n_ep, capacity, part_width), BF16),
            pltpu.VMEM((n_ep, capacity, part_width), BF16),
            pltpu.VMEM((n_y, row_count, part_width), BF16),
            pltpu.VMEM((n_y - 1, row_count, part_width), BF16),
            pltpu.VMEM((n_y - 1, row_count, part_width), BF16),
            dma((n_ep + 1, n_y)),
            dma((n_ep + 1, n_y)),
            dma((n_ep + 1, n_y)),
            dma((n_ep + 1, n_y)),
            dma((n_ep,)),
            dma((n_ep,)),
            dma((2, n_y)),
            dma((2, n_y)),
            dma((2, n_y)),
            dma((2, n_y)),
        ],
        compiler_params=pltpu.CompilerParams(
            collective_id=1, has_side_effects=True, vmem_limit_bytes=VMEM_LIMIT
        ),
    )(arrived, gate_weight, up_weight, down_weight, mixing, mixer_partial)
    return (mixer_output, expert_output)


def take(src, dst, sem):
    copy = pltpu.make_async_copy(src, dst, sem)
    copy.start()
    return copy


def turn_pair(values, cosine, sine):
    half = ROPE // 2
    lane = lax.broadcasted_iota(jnp.int32, values.shape, 1)
    upper = lax.rem(lane, ROPE) >= half
    swapped = jnp.where(
        upper, pltpu.roll(values, half, 1), -pltpu.roll(values, LANES - half, 1)
    )
    return values * cosine + swapped * sine


def step_kernel(n_ep, n_tp, heads, *refs):
    (
        routing_h, share_h, ein_h, egain_h, slat_h, sgain_h, rkey_h, qlat_h, qgain_h, freq_h,
        qp_h, qt_h, kw_h, vw_h, mw_h, gate_h, up_h, down_h,
        eout, mout,
        routing, share, ein, egain, slat, sgain, rkey, qlat, qgain, freq,
        qp_w, qt_w, key_w, value_w, mixer_w, gate_w, up_w, down_w,
        load_sem,
        normed, ranks, weights, disp, arr, mixing,
        lat_all, queries, keys, values, top, total, mixed, out,
        part, ca, sums, ya, res, ret,
        msend, mown, mca, msum, mya,
        d_s, d_r, dy_s, dy_r, dc_s, dc_r,
        lz_s, lz_r, lx_s, lx_r, lc_s, lc_r,
        rc_s, rc_r, ry_s, ry_r, re_s, re_r,
        mc_s, mc_r, my_s, my_r, mo_s, mo_r,
        oy_s, oy_r, oc_s, oc_r,
    ) = refs
    me_e = lax.axis_index("ep")
    me_t = lax.axis_index("tp")
    depth = n_ep // 2
    z = me_e // 2
    x = lax.rem(me_e, 2)
    y = me_t // CORES
    c = lax.rem(me_t, CORES)
    mate = y * CORES + (1 - c)
    over = (1 - y) * CORES + c
    far = (1 - y) * CORES + (1 - c)
    tokens, width = ein.shape
    capacity = arr.shape[1]
    quarter = width // n_tp
    half = width // CORES
    rows = slat.shape[0]
    rank = slat.shape[1]
    head_keys = NOPE + LANES

    loads = []
    pairs = (
        (routing_h, routing), (share_h, share), (ein_h, ein), (egain_h, egain),
        (slat_h, slat), (sgain_h, sgain), (rkey_h, rkey), (freq_h, freq),
        (qlat_h, qlat), (qgain_h, qgain), (qp_h, qp_w), (qt_h, qt_w),
        (gate_h.at[0], gate_w), (up_h.at[0], up_w), (down_h.at[0], down_w),
        (kw_h, key_w), (vw_h, value_w), (mw_h, mixer_w),
    )
    for n, (src, dst) in enumerate(pairs):
        loads.append(take(src, dst, load_sem.at[n]))

    def ready(first, last):
        for n in range(first, last):
            loads[n].wait()

    def ep_at(d, f):
        return lax.rem(z + d + depth, depth) * 2 + (x if f == 0 else 1 - x)

    def cols(t):
        return pl.ds(pl.multiple_of(t * quarter, LANES), quarter)

    def side(core):
        return pl.ds(pl.multiple_of(core * half, LANES), half)

    barrier = pltpu.get_barrier_semaphore()
    peers = [(ep_at(d, f), me_t) for d in range(depth) for f in range(2) if d or f]
    peers += [(me_e, t) for t in (mate, over)]
    for peer in peers:
        pl.semaphore_signal(
            barrier, inc=1, device_id=peer, device_id_type=pl.DeviceIdType.MESH
        )

    sends = []

    def go(copy):
        copy.start()
        sends.append(copy)

    ready(0, 2)
    expert = lax.broadcasted_iota(jnp.int32, (n_ep, tokens), 0)
    member = jnp.zeros((n_ep, tokens), F32)
    weight = jnp.zeros((n_ep, tokens), F32)
    for k in range(routing.shape[0]):
        named = routing[k : k + 1, :] == expert
        member = member + jnp.where(named, 1.0, 0.0)
        weight = weight + jnp.where(named, share[k : k + 1, :], 0.0)
    before = lax.broadcasted_iota(jnp.int32, (tokens, tokens), 0) < lax.broadcasted_iota(
        jnp.int32, (tokens, tokens), 1
    )
    placed = jnp.dot(
        member.astype(BF16),
        jnp.where(before, 1.0, 0.0).astype(BF16),
        preferred_element_type=F32,
    )
    placed = jnp.where(member > 0.0, placed, -1.0)
    ranks[...] = placed
    ready(2, 4)
    normed[...] = norm_rows(ein[...], egain[...])
    slot_row = lax.broadcasted_iota(jnp.int32, (capacity, tokens), 0).astype(F32)

    def chosen(e):
        return jnp.where(ranks[pl.ds(e, 1), :] == slot_row, 1.0, 0.0).astype(BF16)

    own_cols = normed[:, cols(me_t)]
    for d in range(depth):
        for f in range(2):
            if d or f:
                disp[2 * d + f] = jnp.dot(
                    chosen(ep_at(d, f)), own_cols, preferred_element_type=F32
                ).astype(BF16)
    pl.semaphore_wait(barrier, len(peers))

    def disp_at(i, t):
        return arr.at[i, :, cols(t)]

    def direct(i):
        return remote(
            disp.at[i], disp_at(i, me_t), d_s.at[i], d_r.at[i], ep_at(i // 2, i % 2), me_t
        )

    for i in range(1, n_ep):
        go(direct(i))

    ready(4, 8)
    position = lax.broadcasted_iota(jnp.int32, (rows, LANES), 0) + me_e * rows
    angles = position.astype(F32) * freq[...]
    cosine = jnp.cos(angles)
    sine = jnp.sin(angles)
    latent = norm_rows(slat[...], sgain[...])
    lat_all[0, :, :rank] = latent
    key_rows = rkey[...].astype(F32)
    lat_all[0, :, rank:] = turn_pair(
        jnp.concatenate([key_rows, key_rows], axis=1), cosine, sine
    ).astype(BF16)
    lat_rows = rows // CORES

    def lat_at(i, core):
        return lat_all.at[i, pl.ds(pl.multiple_of(core * lat_rows, lat_rows), lat_rows), :]

    def lat_z(d):
        return remote(
            lat_at(0, c), lat_at(2 * d, c), lz_s.at[d], lz_r.at[d], ep_at(d, 0), me_t
        )

    def lat_x(d):
        return remote(
            lat_at(2 * d, c), lat_at(2 * d + 1, c), lx_s.at[d], lx_r.at[d], ep_at(0, 1), me_t
        )

    def lat_c(i, core):
        return remote(lat_at(i, core), lat_at(i, core), lc_s.at[i], lc_r.at[i], me_e, mate)

    go(lat_x(0))
    for d in range(1, depth):
        go(lat_z(d))

    def z_arr(d):
        lat_z(d).wait_recv()
        go(lat_x(d))
        go(lat_c(2 * d, c))

    def x_arr(d):
        lat_x(d).wait_recv()
        go(lat_c(2 * d + 1, c))

    arr[0] = jnp.dot(chosen(me_e), normed[...], preferred_element_type=F32).astype(BF16)
    placed_t = jnp.transpose(placed)
    weight_t = jnp.transpose(weight)
    lane = lax.broadcasted_iota(jnp.int32, (tokens, n_ep), 1)
    slot_col = lax.broadcasted_iota(jnp.int32, (tokens, capacity), 1).astype(F32)
    for i in range(n_ep):
        mine = lane == ep_at(i // 2, i % 2)
        place = jnp.sum(jnp.where(mine, placed_t, 0.0), axis=1, keepdims=True)
        scale = jnp.sum(jnp.where(mine, weight_t, 0.0), axis=1, keepdims=True)
        mixing[i] = jnp.where(place == slot_col, scale, 0.0)

    ready(8, 12)
    query = norm_rows(qlat[...], qgain[...])
    plain = jnp.dot(query, qp_w[...], preferred_element_type=F32).astype(BF16)
    raw = jnp.dot(query, qt_w[...], preferred_element_type=F32)
    group = lax.broadcasted_iota(jnp.int32, (rows, LANES), 1) // ROPE
    for h in range(heads):
        j = h * ROPE // LANES
        turned = turn_pair(raw[:, j * LANES : (j + 1) * LANES], cosine, sine)
        turned = jnp.where(group == h % (LANES // ROPE), turned, 0.0)
        queries[:, h * head_keys : h * head_keys + NOPE] = plain[:, h * NOPE : (h + 1) * NOPE]
        queries[:, h * head_keys + NOPE : (h + 1) * head_keys] = turned.astype(BF16)

    def relay(i):
        direct(i).wait_recv()
        here = disp_at(i, me_t)
        go(remote(here, here, dy_s.at[i], dy_r.at[i], me_e, over))
        go(remote(here, here, dc_s.at[i, 0], dc_r.at[i, 0], me_e, mate))

    def forward(i):
        got = disp_at(i, over)
        remote(got, got, dy_s.at[i], dy_r.at[i], me_e, over).wait_recv()
        go(remote(got, got, dc_s.at[i, 1], dc_r.at[i, 1], me_e, mate))

    def arrive(i):
        for k, t in enumerate((mate, far)):
            got = disp_at(i, t)
            remote(got, got, dc_s.at[i, k], dc_r.at[i, k], me_e, mate).wait_recv()

    def project(i):
        at = slice(i * rows, (i + 1) * rows)
        latent = lat_all[i, :, :rank]
        k = jnp.dot(latent, key_w[...], preferred_element_type=F32).astype(BF16)
        values[at, :] = jnp.dot(latent, value_w[...], preferred_element_type=F32).astype(BF16)
        for h in range(heads):
            keys[at, h * head_keys : h * head_keys + NOPE] = k[:, h * NOPE : (h + 1) * NOPE]
            keys[at, h * head_keys + NOPE : (h + 1) * head_keys] = lat_all[i, :, rank:]

    def core_copy(i, k):
        t = mate if k == 0 else far
        return remote(
            part.at[i, :, cols(t)], ca.at[i, k], rc_s.at[i, k], rc_r.at[i, k], me_e, mate
        )

    def y_copy(i):
        return remote(sums.at[i], ya.at[i], ry_s.at[i], ry_r.at[i], me_e, over)

    def back(i):
        return remote(res.at[i], ret.at[i], re_s.at[i], re_r.at[i], ep_at(-(i // 2), i % 2), me_t)

    def y_step(i):
        core_copy(i, 1).wait_recv()
        sums[i] = (ca[i, 1].astype(F32) + part[i, :, cols(over)].astype(F32)).astype(BF16)
        go(y_copy(i))

    def sum_step(i):
        core_copy(i, 0).wait_recv()
        value = ca[i, 0].astype(F32) + part[i, :, cols(me_t)].astype(F32)
        y_copy(i).wait_recv()
        value = (value + ya[i].astype(F32)).astype(BF16)
        if i == 0:
            ret[0] = value
        else:
            res[i] = value
            go(back(i))

    def chunk(d, between):
        rows_in = arr[2 * d : 2 * d + 2].reshape(2 * capacity, width)
        gate = jnp.minimum(jnp.dot(rows_in, gate_w[...], preferred_element_type=F32), CLAMP_LIMIT)
        between()
        up = jnp.clip(
            jnp.dot(rows_in, up_w[...], preferred_element_type=F32), -CLAMP_LIMIT, CLAMP_LIMIT
        )
        hidden = ((up + 1.0) * (gate * jax.nn.sigmoid(SLOPE * gate))).astype(BF16)
        value = jnp.dot(hidden, down_w[...], preferred_element_type=F32)
        part[2 * d] = value[:capacity].astype(BF16)
        part[2 * d + 1] = value[capacity:].astype(BF16)
        for i in (2 * d, 2 * d + 1):
            for k in (1, 0):
                go(core_copy(i, k))

    log2e = 1.4426950408889634
    scaling = (NOPE + ROPE) ** (-0.5) * log2e

    def attend(h, first, last):
        at = slice(first * rows, last * rows)
        head = slice(h * head_keys, (h + 1) * head_keys)
        scores = lax.dot_general(
            queries[:, head], keys[at, head], (((1,), (1,)), ((), ())), preferred_element_type=F32
        )
        pieces = []
        for i in range(first, last):
            piece = scores[:, (i - first) * rows : (i - first + 1) * rows]
            if i == 0:
                row = lax.broadcasted_iota(jnp.int32, (rows, rows), 0)
                piece = jnp.where(
                    lax.broadcasted_iota(jnp.int32, (rows, rows), 1) <= row, piece, NEGATIVE
                )
            else:
                piece = piece + jnp.where(ep_at(-(i // 2), i % 2) < me_e, 0.0, NEGATIVE)
            pieces.append(piece)
        scores = jnp.concatenate(pieces, axis=1)
        peak = jnp.max(scores, axis=-1, keepdims=True)
        if first > 0:
            old = top[h]
            peak = jnp.maximum(peak, old)
        weight = jnp.exp2((scores - peak) * scaling)
        sum_of = jnp.sum(weight, axis=-1, keepdims=True)
        term = jnp.dot(
            weight.astype(BF16), values[at, h * VDIM : (h + 1) * VDIM], preferred_element_type=F32
        )
        if first > 0:
            fade = jnp.exp2((old - peak) * scaling)
            sum_of = sum_of + fade * total[h]
            term = term + fade * mixed[h]
        if last < n_ep:
            top[h] = peak
            total[h] = sum_of
            mixed[h] = term
        else:
            out[:, h * VDIM : (h + 1) * VDIM] = (term / sum_of).astype(BF16)

    def lat_arrive(i):
        lat_c(i, 1 - c).wait_recv()

    acc = []

    def mix(i):
        if i > 0:
            back(i).wait_recv()
        table = mixing[i]
        high = table.astype(BF16)
        low = (table - high.astype(F32)).astype(BF16)
        term = jnp.dot(high, ret[i], preferred_element_type=F32) + jnp.dot(
            low, ret[i], preferred_element_type=F32
        )
        acc[:] = [term if not acc else acc[0] + term]

    def out_copy(k, t, to):
        ref = eout.at[:, cols(t)]
        s, r = (oy_s, oy_r) if k == 0 else (oc_s, oc_r)
        n = 0 if k < 2 else 1
        return remote(ref, ref, s.at[n], r.at[n], me_e, to)

    def mix_rows(n):
        return slice(n * lat_rows, (n + 1) * lat_rows)

    def mixer_core(n):
        return remote(
            msend.at[mix_rows(n)], mca.at[mix_rows(n)], mc_s.at[n], mc_r.at[n], me_e, mate
        )

    def mixer_y(n):
        return remote(
            msum.at[mix_rows(n)], mya.at[mix_rows(n)], my_s.at[n], my_r.at[n], me_e, over
        )

    def mixer_out(n, core):
        ref = mout.at[mix_rows(n), side(core)]
        return remote(ref, ref, mo_s.at[n], mo_r.at[n], me_e, mate)

    ready(15, 17)
    project(0)
    relay(1)
    relay(2)
    forward(1)
    relay(3)
    forward(2)
    arrive(1)
    ready(12, 15)
    for d in range(depth):

        def between(d=d):
            if d + 2 < depth:
                relay(2 * d + 4)
                forward(2 * d + 3)
                relay(2 * d + 5)
                forward(2 * d + 4)
            elif d + 2 == depth:
                forward(2 * d + 3)
                x_arr(0)
            else:
                z_arr(1)

        chunk(d, between)
        if d > 0:
            for i in (2 * d - 2, 2 * d - 1):
                y_step(i)
        if d > 1:
            for i in (2 * d - 4, 2 * d - 3):
                sum_step(i)
        if d + 1 < depth:
            for i in (2 * d + 2, 2 * d + 3):
                arrive(i)
    lat_arrive(1)
    project(1)
    y_step(n_ep - 2)
    y_step(n_ep - 1)
    x_arr(1)
    lat_arrive(2)
    project(2)
    for d in range(2, depth):
        z_arr(d)
    sum_step(n_ep - 4)
    sum_step(n_ep - 3)
    lat_arrive(3)
    project(3)
    middle = n_ep // 2
    attend(0, 0, middle)
    sum_step(n_ep - 2)
    sum_step(n_ep - 1)
    for d in range(2, depth):
        x_arr(d)
    for h in range(1, heads):
        attend(h, 0, middle)
    for i in range(middle, n_ep):
        lat_arrive(i)
        project(i)
    todo = list(range(n_ep))
    for h in range(heads):
        attend(h, middle, n_ep)
        for i in todo[h * n_ep // heads : (h + 1) * n_ep // heads]:
            mix(i)
    eout[:, cols(me_t)] = acc[0].astype(BF16)
    go(out_copy(0, me_t, over))
    go(out_copy(1, me_t, mate))
    ready(17, 18)
    msend[...] = jnp.dot(
        out[...], mixer_w[:, side(1 - c)], preferred_element_type=F32
    ).astype(BF16)
    for n in range(2):
        go(mixer_core(n))
    mown[...] = jnp.dot(out[...], mixer_w[:, side(c)], preferred_element_type=F32)
    for n in range(2):
        mixer_core(n).wait_recv()
        at = mix_rows(n)
        msum[at] = (mown[at] + mca[at].astype(F32)).astype(BF16)
        go(mixer_y(n))
    out_copy(0, over, over).wait_recv()
    go(out_copy(2, over, mate))
    for n in range(2):
        mixer_y(n).wait_recv()
        at = mix_rows(n)
        mout[at, side(c)] = (msum[at].astype(F32) + mya[at].astype(F32)).astype(BF16)
        go(mixer_out(n, c))
    out_copy(1, mate, mate).wait_recv()
    out_copy(2, far, mate).wait_recv()
    for n in range(2):
        mixer_out(n, 1 - c).wait_recv()
    for copy in sends:
        copy.wait_send()


def fused(
    n_ep,
    n_tp,
    query_latent,
    shared_latent,
    rotary_key,
    query_gain,
    shared_gain,
    query_plain_weight,
    query_turn_weight,
    key_weight,
    value_weight,
    mixer_out_weight,
    expert_input,
    expert_gain,
    routing,
    routing_weight,
    gate_weight,
    up_weight,
    down_weight,
):
    rows, query_rank = query_latent.shape
    rank = shared_latent.shape[1]
    heads = query_plain_weight.shape[1] // NOPE
    tokens, width = expert_input.shape
    top_count = routing.shape[1]
    units = gate_weight.shape[2]
    capacity = 4 * tokens * top_count // (3 * n_ep)
    capacity = -(-capacity // 8) * 8
    quarter = width // n_tp
    half = width // CORES
    depth = n_ep // 2
    total = n_ep * rows
    lane = np.arange(LANES)
    freq = ROTARY_BASE ** (-2.0 * (lane % (ROPE // 2)) / ROPE)
    freq = jnp.asarray(freq.astype(np.float32)[None, :])
    args = (
        routing.T,
        routing_weight.T,
        expert_input,
        expert_gain[None, :],
        shared_latent,
        shared_gain[None, :],
        rotary_key,
        query_latent,
        query_gain[None, :],
        freq,
        query_plain_weight,
        query_turn_weight,
        key_weight,
        value_weight,
        mixer_out_weight,
        gate_weight,
        up_weight,
        down_weight,
    )
    dma = pltpu.SemaphoreType.DMA
    held = [pltpu.VMEM(a.shape if a.ndim == 2 else a.shape[1:], a.dtype) for a in args]
    expert_output, mixer_output = pl.pallas_call(
        functools.partial(step_kernel, n_ep, n_tp, heads),
        out_shape=(
            jax.ShapeDtypeStruct((tokens, width), BF16),
            jax.ShapeDtypeStruct((rows, width), BF16),
        ),
        in_specs=[pl.BlockSpec(memory_space=pl.ANY)] * len(args),
        out_specs=vmem(2),
        scratch_shapes=held
        + [
            dma((len(args),)),
            pltpu.VMEM((tokens, width), BF16),
            pltpu.VMEM((n_ep, tokens), F32),
            pltpu.VMEM((n_ep, tokens), F32),
            pltpu.VMEM((n_ep, capacity, quarter), BF16),
            pltpu.VMEM((n_ep, capacity, width), BF16),
            pltpu.VMEM((n_ep, tokens, capacity), F32),
            pltpu.VMEM((n_ep, rows, rank + LANES), BF16),
            pltpu.VMEM((rows, heads * (NOPE + LANES)), BF16),
            pltpu.VMEM((total, heads * (NOPE + LANES)), BF16),
            pltpu.VMEM((total, heads * VDIM), BF16),
            pltpu.VMEM((heads, rows, 1), F32),
            pltpu.VMEM((heads, rows, 1), F32),
            pltpu.VMEM((heads, rows, VDIM), F32),
            pltpu.VMEM((rows, heads * VDIM), BF16),
            pltpu.VMEM((n_ep, capacity, width), BF16),
            pltpu.VMEM((n_ep, CORES, capacity, quarter), BF16),
            pltpu.VMEM((n_ep, capacity, quarter), BF16),
            pltpu.VMEM((n_ep, capacity, quarter), BF16),
            pltpu.VMEM((n_ep, capacity, quarter), BF16),
            pltpu.VMEM((n_ep, capacity, quarter), BF16),
            pltpu.VMEM((rows, half), BF16),
            pltpu.VMEM((rows, half), F32),
            pltpu.VMEM((rows, half), BF16),
            pltpu.VMEM((rows, half), BF16),
            pltpu.VMEM((rows, half), BF16),
            dma((n_ep,)),
            dma((n_ep,)),
            dma((n_ep,)),
            dma((n_ep,)),
            dma((n_ep, 2)),
            dma((n_ep, 2)),
            dma((depth,)),
            dma((depth,)),
            dma((depth,)),
            dma((depth,)),
            dma((n_ep,)),
            dma((n_ep,)),
            dma((n_ep, 2)),
            dma((n_ep, 2)),
            dma((n_ep,)),
            dma((n_ep,)),
            dma((n_ep,)),
            dma((n_ep,)),
            dma((2,)),
            dma((2,)),
            dma((2,)),
            dma((2,)),
            dma((2,)),
            dma((2,)),
            dma((1,)),
            dma((1,)),
            dma((2,)),
            dma((2,)),
        ],
        compiler_params=pltpu.CompilerParams(
            collective_id=2, has_side_effects=True, vmem_limit_bytes=VMEM_LIMIT
        ),
    )(*args)
    return (mixer_output, expert_output)


def pick(mesh):
    small = mesh.shape["tp"] == 2 * CORES and mesh.shape["ep"] <= 8 and mesh.shape["ep"] % 4 == 0
    return fused if small else per_device


def solution(mesh):
    return jax.shard_map(
        functools.partial(pick(mesh), mesh.shape["ep"], mesh.shape["tp"]),
        mesh=mesh,
        in_specs=(
            P("ep", None),
            P("ep", None),
            P("ep", None),
            P(),
            P(),
            P(None, "tp"),
            P(None, "tp"),
            P(None, "tp"),
            P(None, "tp"),
            P("tp", None),
            P("ep", None),
            P(),
            P("ep", None),
            P("ep", None),
            P("ep", None, "tp"),
            P("ep", None, "tp"),
            P("ep", "tp", None),
        ),
        out_specs=(P("ep", None), P("ep", None)),
        check_vma=False,
    )
```

```python
import functools

import jax
import jax.numpy as jnp
import numpy as np
from jax import lax
from jax.experimental import pallas as pl
from jax.experimental.pallas import tpu as pltpu
from jax.sharding import PartitionSpec as P

NOPE = 128
ROPE = 64
VDIM = 128
LANES = 128
CORES = 2

EPSILON = 1e-06
CLAMP_LIMIT = 7.0
SLOPE = 1.702
ROTARY_BASE = 10000.0
NEGATIVE = -1e30
VMEM_LIMIT = 60 * 1024 * 1024
FUSED_LIMIT = 58 * 1024 * 1024
F32 = jnp.float32
BF16 = jnp.bfloat16


def norm_scale(values):
    widened = values.astype(F32)
    return widened * lax.rsqrt(jnp.mean(widened * widened, axis=-1, keepdims=True) + EPSILON)


def norm_rows(values, gains):
    return (norm_scale(values) * gains).astype(BF16)


def rotate_heads(values, position):
    half = ROPE // 2
    lane = jnp.arange(values.shape[-1], dtype=jnp.int32)
    frequency = ROTARY_BASE ** (-2.0 * (lane % half).astype(F32) / ROPE)
    angles = position.astype(F32)[:, None] * frequency[None, :]
    upper = (lane % ROPE >= half)[None, :]
    swapped = jnp.where(upper, jnp.roll(values, half, axis=1), -jnp.roll(values, -half, axis=1))
    return values * jnp.cos(angles) + swapped * jnp.sin(angles)


def remote(src, dst, send_sem, recv_sem, ep, tp):
    return pltpu.make_async_remote_copy(
        src_ref=src,
        dst_ref=dst,
        send_sem=send_sem,
        recv_sem=recv_sem,
        device_id=(ep, tp),
        device_id_type=pl.DeviceIdType.MESH,
    )


def enter(n_ep, n_tp, me_e, me_t):
    barrier = pltpu.get_barrier_semaphore()
    for d in range(1, n_ep):
        pl.semaphore_signal(
            barrier,
            inc=1,
            device_id=(lax.rem(me_e + d, n_ep), me_t),
            device_id_type=pl.DeviceIdType.MESH,
        )
    for k in range(1, n_tp):
        pl.semaphore_signal(
            barrier,
            inc=1,
            device_id=(me_e, lax.rem(me_t + k, n_tp)),
            device_id_type=pl.DeviceIdType.MESH,
        )
    pl.semaphore_wait(barrier, n_ep - 1 + n_tp - 1)


def gather_kernel(
    n_ep,
    n_tp,
    heads,
    lat,
    disp,
    queries,
    key_w,
    value_w,
    mixer_w,
    arr,
    mpart,
    lat_all,
    out,
    keys,
    values,
    loc_sem,
    ep_s,
    ep_r,
    y_s,
    y_r,
    c_s,
    c_r,
):
    me_e = lax.axis_index("ep")
    me_t = lax.axis_index("tp")
    n_y = n_tp // CORES
    y = me_t // CORES
    c = lax.rem(me_t, CORES)
    mate = y * CORES + (1 - c)
    width = disp.shape[2]

    def place(j, e, t):
        if j == 0:
            return lat_all.at[e, t]
        return arr.at[e, :, pl.ds(pl.multiple_of(t * width, LANES), width)]

    local = []
    for j in range(2):
        copy = pltpu.make_async_copy(
            lat if j == 0 else disp.at[me_e], place(j, me_e, me_t), loc_sem.at[j]
        )
        copy.start()
        local.append(copy)
    enter(n_ep, n_tp, me_e, me_t)
    sends = []
    for j in range(2):
        for d in range(1, n_ep):
            peer = lax.rem(me_e + d, n_ep)
            copy = remote(
                lat if j == 0 else disp.at[peer],
                place(j, me_e, me_t),
                ep_s.at[d, j],
                ep_r.at[d, j],
                peer,
                me_t,
            )
            copy.start()
            sends.append(copy)

    def relay(j, d):
        src = lax.rem(me_e - d + n_ep, n_ep)
        here = place(j, src, me_t)
        if d == 0:
            local[j].wait()
        else:
            remote(here, here, ep_s.at[d, j], ep_r.at[d, j], src, me_t).wait_recv()
        for k in range(1, n_y):
            to = lax.rem(y + k, n_y) * CORES + c
            copy = remote(here, here, y_s.at[d, k, j], y_r.at[d, k, j], me_e, to)
            copy.start()
            sends.append(copy)
        copy = remote(here, here, c_s.at[d, 0, j], c_r.at[d, 0, j], me_e, mate)
        copy.start()
        sends.append(copy)

    def forward(j, d):
        src = lax.rem(me_e - d + n_ep, n_ep)
        for k in range(1, n_y):
            got = place(j, src, lax.rem(y - k + n_y, n_y) * CORES + c)
            remote(got, got, y_s.at[d, k, j], y_r.at[d, k, j], me_e, me_t).wait_recv()
            copy = remote(got, got, c_s.at[d, k, j], c_r.at[d, k, j], me_e, mate)
            copy.start()
            sends.append(copy)

    def arrive(j, d):
        src = lax.rem(me_e - d + n_ep, n_ep)
        for k in range(n_y):
            got = place(j, src, lax.rem(y - k + n_y, n_y) * CORES + (1 - c))
            remote(got, got, c_s.at[d, k, j], c_r.at[d, k, j], me_e, mate).wait_recv()

    for d in range(n_ep):
        relay(0, d)
        if d > 0:
            forward(0, d - 1)
    relay(1, 0)
    forward(0, n_ep - 1)
    for d in range(n_ep):
        arrive(0, d)
        if d % 2 == 1 and d // 2 + 1 < n_ep // 2:
            relay(1, d // 2 + 1)
        project(
            lax.rem(me_e - d + n_ep, n_ep), n_tp, heads, lat_all, key_w, value_w, keys, values
        )
    done = n_ep // 2
    for h in range(heads):
        attend(h, me_e, queries, keys, values, out)
        until = n_ep if h == heads - 1 else n_ep // 2 + (h + 1) * (n_ep // 2) // heads
        for d in range(done, until):
            relay(1, d)
        done = until
    mpart[...] = jnp.dot(out[...], mixer_w[...], preferred_element_type=F32).astype(BF16)
    for d in range(n_ep):
        forward(1, d)
    for d in range(n_ep):
        arrive(1, d)
    for copy in sends:
        copy.wait_send()


def project(e, n_tp, heads, lat_all, key_w, value_w, keys, values):
    share = lat_all.shape[2]
    rows = n_tp * share
    rank = key_w.shape[0]
    head_keys = NOPE + LANES
    at = pl.ds(pl.multiple_of(e * rows, rows), rows)
    block = lat_all[e].reshape(rows, rank + LANES)
    latent = block[:, :rank]
    k = jnp.dot(latent, key_w[...], preferred_element_type=F32).astype(BF16)
    values[at, :] = jnp.dot(latent, value_w[...], preferred_element_type=F32).astype(BF16)
    for h in range(heads):
        keys[at, h * head_keys : h * head_keys + NOPE] = k[:, h * NOPE : (h + 1) * NOPE]
        keys[at, h * head_keys + NOPE : (h + 1) * head_keys] = block[:, rank:]


def attend(h, me_e, queries, keys, values, out):
    rows = queries.shape[0]
    total = keys.shape[0]
    head_keys = NOPE + LANES
    row = lax.broadcasted_iota(jnp.int32, (rows, total), 0) + me_e * rows
    visible = lax.broadcasted_iota(jnp.int32, (rows, total), 1) <= row
    scaling = (NOPE + ROPE) ** (-0.5)
    cols = slice(h * head_keys, (h + 1) * head_keys)
    scores = lax.dot_general(
        queries[:, cols], keys[:, cols], (((1,), (1,)), ((), ())), preferred_element_type=F32
    )
    scores = jnp.where(visible, scores * scaling, NEGATIVE)
    weight = jnp.exp(scores - jnp.max(scores, axis=-1, keepdims=True))
    sums = jnp.sum(weight, axis=-1, keepdims=True)
    mixed = jnp.dot(
        weight.astype(BF16), values[:, h * VDIM : (h + 1) * VDIM], preferred_element_type=F32
    )
    out[:, h * VDIM : (h + 1) * VDIM] = (mixed / sums).astype(BF16)


def return_kernel(
    n_ep,
    n_tp,
    arrived,
    gate_hbm,
    up_hbm,
    down_hbm,
    mix,
    mpart,
    eout,
    mout,
    gate_w,
    up_w,
    down_w,
    load_sem,
    part,
    ca,
    sums,
    ya,
    res,
    ret,
    mca,
    msums,
    mya,
    ca_s,
    ca_r,
    ya_s,
    ya_r,
    ep_s,
    ep_r,
    oy_s,
    oy_r,
    oc_s,
    oc_r,
):
    me_e = lax.axis_index("ep")
    me_t = lax.axis_index("tp")
    n_y = n_tp // CORES
    y = me_t // CORES
    c = lax.rem(me_t, CORES)
    mate = y * CORES + (1 - c)
    width = res.shape[2]
    capacity = res.shape[1]
    pairs = n_ep // 2
    parity = lax.rem(me_e, 2)
    loads = []
    for n, (src, dst) in enumerate(((gate_hbm, gate_w), (up_hbm, up_w), (down_hbm, down_w))):
        copy = pltpu.make_async_copy(src.at[0], dst, load_sem.at[n])
        copy.start()
        loads.append(copy)

    def twin(i):
        return parity if i % 2 == 0 else 1 - parity

    def dest(i):
        return lax.rem(me_e // 2 + i // 2, pairs) * 2 + twin(i)

    def source(i):
        return lax.rem(me_e // 2 - i // 2 + pairs, pairs) * 2 + twin(i)

    def cols(t):
        return pl.ds(pl.multiple_of(t * width, LANES), width)

    def part_at(i, t):
        if i == n_ep:
            return mpart.at[:, cols(t)]
        return part.at[dest(i), :, cols(t)]

    def part_load(i, t):
        if i == n_ep:
            return mpart[:, cols(t)].astype(F32)
        return part[dest(i), :, cols(t)].astype(F32)

    enter(n_ep, n_tp, me_e, me_t)
    sends = []

    def go(copy):
        copy.start()
        sends.append(copy)

    def core_copy(i, k):
        dst = mca.at[k] if i == n_ep else ca.at[i, k]
        return remote(
            part_at(i, lax.rem(y + k, n_y) * CORES + (1 - c)),
            dst,
            ca_s.at[i, k],
            ca_r.at[i, k],
            me_e,
            mate,
        )

    def y_copy(i, k):
        src, dst = (msums, mya) if i == n_ep else (sums.at[i], ya.at[i])
        to = lax.rem(y + k, n_y) * CORES + c
        return remote(src.at[k - 1], dst.at[k - 1], ya_s.at[i, k], ya_r.at[i, k], me_e, to)

    def core_step(i):
        for k in list(range(1, n_y)) + [0]:
            go(core_copy(i, k))

    def y_step(i):
        for k in range(1, n_y):
            core_copy(i, k).wait_recv()
            got = (mca[k] if i == n_ep else ca[i, k]).astype(F32)
            value = (got + part_load(i, lax.rem(y + k, n_y) * CORES + c)).astype(BF16)
            if i == n_ep:
                msums[k - 1] = value
            else:
                sums[i, k - 1] = value
            go(y_copy(i, k))

    def ep_copy(i, e):
        return remote(res.at[i], ret.at[i], ep_s.at[i], ep_r.at[i], e, me_t)

    def sum_step(i):
        core_copy(i, 0).wait_recv()
        value = (mca[0] if i == n_ep else ca[i, 0]).astype(F32) + part_load(i, me_t)
        for k in range(1, n_y):
            y_copy(i, k).wait_recv()
            value = value + (mya[k - 1] if i == n_ep else ya[i, k - 1]).astype(F32)
        if i == n_ep:
            mout[:, cols(me_t)] = value.astype(BF16)
        elif i == 0:
            ret[0] = value.astype(BF16)
        else:
            res[i] = value.astype(BF16)
            go(ep_copy(i, dest(i)))

    def expert_step(s):
        base = lax.rem(me_e // 2 + s, pairs) * 2
        rows = arrived[pl.ds(pl.multiple_of(base * capacity, 2 * capacity), 2 * capacity), :]
        if s == 1 % pairs:
            loads[0].wait()
            loads[1].wait()
        gate = jnp.minimum(jnp.dot(rows, gate_w[...], preferred_element_type=F32), CLAMP_LIMIT)
        up = jnp.clip(
            jnp.dot(rows, up_w[...], preferred_element_type=F32), -CLAMP_LIMIT, CLAMP_LIMIT
        )
        hidden = ((up + 1.0) * (gate * jax.nn.sigmoid(SLOPE * gate))).astype(BF16)
        if s == 1 % pairs:
            loads[2].wait()
        value = jnp.dot(hidden, down_w[...], preferred_element_type=F32)
        part[base] = value[:capacity].astype(BF16)
        part[base + 1] = value[capacity:].astype(BF16)

    def out_copy(j, k, t, to, sem_s, sem_r):
        ref = (mout if j == 0 else eout).at[:, cols(t)]
        return remote(ref, ref, sem_s.at[j, k], sem_r.at[j, k], me_e, to)

    def out_send(j):
        for k in range(1, n_y):
            go(out_copy(j, k, me_t, lax.rem(y + k, n_y) * CORES + c, oy_s, oy_r))
        go(out_copy(j, 0, me_t, mate, oc_s, oc_r))

    core_step(n_ep)
    turns = [n % pairs for n in range(1, pairs + 1)]
    for n, turn in enumerate(turns):
        expert_step(turn)
        for i in (2 * turn, 2 * turn + 1):
            core_step(i)
        if n == 0:
            y_step(n_ep)
        for i in (2 * turn, 2 * turn + 1):
            y_step(i)
        if n > 0:
            for i in (2 * turns[n - 1], 2 * turns[n - 1] + 1):
                sum_step(i)
    sum_step(n_ep)
    out_send(0)
    for i in (1, 0):
        sum_step(i)
    acc = None
    for i in [0] + list(range(2, n_ep)) + [1]:
        if i > 0:
            ep_copy(i, source(i)).wait_recv()
        mixing = mix[source(i)]
        high = mixing.astype(BF16)
        low = (mixing - high.astype(F32)).astype(BF16)
        rows = ret[i]
        term = jnp.dot(high, rows, preferred_element_type=F32) + jnp.dot(
            low, rows, preferred_element_type=F32
        )
        acc = term if acc is None else acc + term
    eout[:, cols(me_t)] = acc.astype(BF16)
    out_send(1)
    for j in range(2):
        for k in range(1, n_y):
            t = lax.rem(y - k + n_y, n_y) * CORES + c
            out_copy(j, k, t, me_t, oy_s, oy_r).wait_recv()
            go(out_copy(j, k, t, mate, oc_s, oc_r))
    for j in range(2):
        for k in range(n_y):
            t = lax.rem(y - k + n_y, n_y) * CORES + (1 - c)
            out_copy(j, k, t, mate, oc_s, oc_r).wait_recv()
    for copy in sends:
        copy.wait_send()


def vmem(count):
    return [pl.BlockSpec(memory_space=pltpu.VMEM)] * count


def per_device(
    n_ep,
    n_tp,
    query_latent,
    shared_latent,
    rotary_key,
    query_gain,
    shared_gain,
    query_plain_weight,
    query_turn_weight,
    key_weight,
    value_weight,
    mixer_out_weight,
    expert_input,
    expert_gain,
    routing,
    routing_weight,
    gate_weight,
    up_weight,
    down_weight,
):
    me_e = lax.axis_index("ep")
    me_t = lax.axis_index("tp")
    n_y = n_tp // CORES
    row_count = query_latent.shape[0]
    heads = query_plain_weight.shape[1] // NOPE
    rank = shared_latent.shape[1]

    share = row_count // n_tp
    first = me_t * share
    lat = norm_rows(lax.dynamic_slice_in_dim(shared_latent, first, share, 0), shared_gain)
    own_position = me_e * row_count + first + jnp.arange(share, dtype=jnp.int32)
    turned = rotate_heads(
        lax.dynamic_slice_in_dim(rotary_key, first, share, 0).astype(F32), own_position
    ).astype(BF16)
    lat = jnp.concatenate([lat, turned, jnp.zeros((share, LANES - ROPE), BF16)], axis=1)

    token_count, width = expert_input.shape
    top_count = routing.shape[1]
    capacity = 4 * token_count * top_count // (3 * n_ep)
    capacity = -(-capacity // 8) * 8
    part_width = width // n_tp
    normed = norm_rows(expert_input, expert_gain)
    normed = lax.dynamic_slice_in_dim(normed, me_t * part_width, part_width, 1)
    flattened = routing.reshape(token_count * top_count)
    matches = flattened[:, None] == jnp.arange(n_ep, dtype=jnp.int32)[None, :]
    count = token_count * top_count
    lower = jnp.arange(count)[:, None] > jnp.arange(count)[None, :]
    ranking = jnp.dot(
        lower.astype(BF16), matches.astype(BF16), preferred_element_type=F32
    ).astype(jnp.int32)
    slot_index = jnp.sum(jnp.where(matches, ranking, 0), axis=1)
    target = (flattened * capacity + slot_index).reshape(token_count, top_count)
    slot_ids = jnp.arange(n_ep * capacity, dtype=jnp.int32)
    table = jnp.zeros((n_ep * capacity, token_count), jnp.bool_)
    mixing = jnp.zeros((token_count, n_ep * capacity), F32)
    for k in range(top_count):
        table = table | (target[:, k][None, :] == slot_ids[:, None])
        mixing = mixing + jnp.where(
            target[:, k][:, None] == slot_ids[None, :], routing_weight[:, k][:, None], 0.0
        )
    disp = jnp.dot(table.astype(BF16), normed, preferred_element_type=F32).astype(BF16)
    disp = disp.reshape(n_ep, capacity, part_width)
    mixing = jnp.transpose(mixing.reshape(token_count, n_ep, capacity), (1, 0, 2))

    position = me_e * row_count + jnp.arange(row_count, dtype=jnp.int32)
    query_normed = norm_rows(query_latent, query_gain)
    query_plain = jnp.dot(query_normed, query_plain_weight, preferred_element_type=F32)
    query_plain = query_plain.astype(BF16)
    query_raw = jnp.dot(query_normed, query_turn_weight, preferred_element_type=F32)
    query_turned = rotate_heads(query_raw, position).astype(BF16)
    blank = jnp.zeros((row_count, LANES - ROPE), BF16)
    pieces = []
    for h in range(heads):
        pieces.append(query_plain[:, h * NOPE : (h + 1) * NOPE])
        pieces.append(query_turned[:, h * ROPE : (h + 1) * ROPE])
        pieces.append(blank)
    queries = jnp.concatenate(pieces, axis=1)
    total = n_ep * row_count
    dma = pltpu.SemaphoreType.DMA
    arrived, mixer_partial = pl.pallas_call(
        functools.partial(gather_kernel, n_ep, n_tp, heads),
        out_shape=(
            jax.ShapeDtypeStruct((n_ep, capacity, width), BF16),
            jax.ShapeDtypeStruct((row_count, width), BF16),
        ),
        in_specs=vmem(6),
        out_specs=vmem(2),
        scratch_shapes=[
            pltpu.VMEM((n_ep, n_tp, share, rank + LANES), BF16),
            pltpu.VMEM((row_count, heads * VDIM), BF16),
            pltpu.VMEM((total, heads * (NOPE + LANES)), BF16),
            pltpu.VMEM((total, heads * VDIM), BF16),
            dma((2,)),
            dma((n_ep, 2)),
            dma((n_ep, 2)),
            dma((n_ep, n_y, 2)),
            dma((n_ep, n_y, 2)),
            dma((n_ep, n_y, 2)),
            dma((n_ep, n_y, 2)),
        ],
        compiler_params=pltpu.CompilerParams(
            collective_id=0, has_side_effects=True, vmem_limit_bytes=VMEM_LIMIT
        ),
    )(lat, disp, queries, key_weight, value_weight, mixer_out_weight)
    arrived = arrived.reshape(n_ep * capacity, width)
    units = gate_weight.shape[2]

    expert_output, mixer_output = pl.pallas_call(
        functools.partial(return_kernel, n_ep, n_tp),
        out_shape=(
            jax.ShapeDtypeStruct((token_count, width), BF16),
            jax.ShapeDtypeStruct((row_count, width), BF16),
        ),
        in_specs=vmem(1) + [pl.BlockSpec(memory_space=pl.ANY)] * 3 + vmem(2),
        out_specs=vmem(2),
        scratch_shapes=[
            pltpu.VMEM((width, units), BF16),
            pltpu.VMEM((width, units), BF16),
            pltpu.VMEM((units, width), BF16),
            dma((3,)),
            pltpu.VMEM((n_ep, capacity, width), BF16),
            pltpu.VMEM((n_ep, n_y, capacity, part_width), BF16),
            pltpu.VMEM((n_ep, n_y - 1, capacity, part_width), BF16),
            pltpu.VMEM((n_ep, n_y - 1, capacity, part_width), BF16),
            pltpu.VMEM((n_ep, capacity, part_width), BF16),
            pltpu.VMEM((n_ep, capacity, part_width), BF16),
            pltpu.VMEM((n_y, row_count, part_width), BF16),
            pltpu.VMEM((n_y - 1, row_count, part_width), BF16),
            pltpu.VMEM((n_y - 1, row_count, part_width), BF16),
            dma((n_ep + 1, n_y)),
            dma((n_ep + 1, n_y)),
            dma((n_ep + 1, n_y)),
            dma((n_ep + 1, n_y)),
            dma((n_ep,)),
            dma((n_ep,)),
            dma((2, n_y)),
            dma((2, n_y)),
            dma((2, n_y)),
            dma((2, n_y)),
        ],
        compiler_params=pltpu.CompilerParams(
            collective_id=1, has_side_effects=True, vmem_limit_bytes=VMEM_LIMIT
        ),
    )(arrived, gate_weight, up_weight, down_weight, mixing, mixer_partial)
    return (mixer_output, expert_output)


def take(src, dst, sem):
    copy = pltpu.make_async_copy(src, dst, sem)
    copy.start()
    return copy


def turn_pair(values, cosine, sine):
    half = ROPE // 2
    lane = lax.broadcasted_iota(jnp.int32, values.shape, 1)
    upper = lax.rem(lane, ROPE) >= half
    swapped = jnp.where(
        upper, pltpu.roll(values, half, 1), -pltpu.roll(values, LANES - half, 1)
    )
    return values * cosine + swapped * sine


def step_kernel(n_ep, n_tp, heads, *refs):
    (
        routing_h, share_h, ein_h, egain_h, slat_h, sgain_h, rkey_h, qlat_h, qgain_h, freq_h,
        qp_h, qt_h, kw_h, vw_h, mw_h, gate_h, up_h, down_h,
        eout, mout,
        routing, share, ein, egain, slat, sgain, rkey, qlat, qgain, freq,
        qp_w, qt_w, key_w, value_w, mixer_w, gate_w, up_w, down_w,
        load_sem,
        normed, ranks, weights, disp, arr, mixing,
        lat_all, queries, keys, values, top, total, mixed, out,
        part, ca, sums, ya, res, ret,
        msend, mown, mca, msum, mya,
        d_s, d_r, dy_s, dy_r, dc_s, dc_r,
        lz_s, lz_r, lx_s, lx_r, lc_s, lc_r,
        rc_s, rc_r, ry_s, ry_r, re_s, re_r,
        mc_s, mc_r, my_s, my_r, mo_s, mo_r,
        oy_s, oy_r, oc_s, oc_r,
    ) = refs
    me_e = lax.axis_index("ep")
    me_t = lax.axis_index("tp")
    depth = n_ep // 2
    z = me_e // 2
    x = lax.rem(me_e, 2)
    y = me_t // CORES
    c = lax.rem(me_t, CORES)
    mate = y * CORES + (1 - c)
    over = (1 - y) * CORES + c
    far = (1 - y) * CORES + (1 - c)
    tokens, width = ein.shape
    capacity = arr.shape[1]
    quarter = width // n_tp
    half = width // CORES
    rows = slat.shape[0]
    rank = slat.shape[1]
    head_keys = NOPE + LANES

    loads = []
    pairs = (
        (routing_h, routing), (share_h, share), (ein_h, ein), (egain_h, egain),
        (slat_h, slat), (sgain_h, sgain), (rkey_h, rkey), (freq_h, freq),
        (qlat_h, qlat), (qgain_h, qgain), (qp_h, qp_w), (qt_h, qt_w),
        (gate_h.at[0], gate_w), (up_h.at[0], up_w), (down_h.at[0], down_w),
        (kw_h, key_w), (vw_h, value_w), (mw_h, mixer_w),
    )
    for n, (src, dst) in enumerate(pairs):
        loads.append(take(src, dst, load_sem.at[n]))

    def ready(first, last):
        for n in range(first, last):
            loads[n].wait()

    def ep_at(d, f):
        return lax.rem(z + d + depth, depth) * 2 + (x if f == 0 else 1 - x)

    def cols(t):
        return pl.ds(pl.multiple_of(t * quarter, LANES), quarter)

    def side(core):
        return pl.ds(pl.multiple_of(core * half, LANES), half)

    lat_all[1:] = jnp.zeros((n_ep - 1, rows, rank + LANES), BF16)
    barrier = pltpu.get_barrier_semaphore()
    peers = [(ep_at(d, f), me_t) for d in range(depth) for f in range(2) if d or f]
    peers += [(me_e, t) for t in (mate, over)]
    for peer in peers:
        pl.semaphore_signal(
            barrier, inc=1, device_id=peer, device_id_type=pl.DeviceIdType.MESH
        )

    sends = []

    def go(copy, when=None):
        if when is None:
            copy.start()
        else:
            pl.when(when)(copy.start)
        sends.append((when, copy))

    def landed(copy, when):
        pl.when(when)(copy.wait_recv)

    ready(0, 2)
    expert = lax.broadcasted_iota(jnp.int32, (n_ep, tokens), 0)
    member = jnp.zeros((n_ep, tokens), F32)
    weight = jnp.zeros((n_ep, tokens), F32)
    for k in range(routing.shape[0]):
        named = routing[k : k + 1, :] == expert
        member = member + jnp.where(named, 1.0, 0.0)
        weight = weight + jnp.where(named, share[k : k + 1, :], 0.0)
    before = lax.broadcasted_iota(jnp.int32, (tokens, tokens), 0) < lax.broadcasted_iota(
        jnp.int32, (tokens, tokens), 1
    )
    placed = jnp.dot(
        member.astype(BF16),
        jnp.where(before, 1.0, 0.0).astype(BF16),
        preferred_element_type=F32,
    )
    placed = jnp.where(member > 0.0, placed, -1.0)
    ranks[...] = placed
    ready(2, 4)
    normed[...] = norm_rows(ein[...], egain[...][None, :])
    slot_row = lax.broadcasted_iota(jnp.int32, (capacity, tokens), 0).astype(F32)

    def chosen(e):
        return jnp.where(ranks[pl.ds(e, 1), :] == slot_row, 1.0, 0.0).astype(BF16)

    own_cols = normed[:, cols(me_t)]
    for d in range(depth):
        for f in range(2):
            if d or f:
                disp[2 * d + f] = jnp.dot(
                    chosen(ep_at(d, f)), own_cols, preferred_element_type=F32
                ).astype(BF16)
    pl.semaphore_wait(barrier, len(peers))

    def disp_at(i, t):
        return arr.at[i, :, cols(t)]

    def direct(i):
        return remote(
            disp.at[i], disp_at(i, me_t), d_s.at[i], d_r.at[i], ep_at(i // 2, i % 2), me_t
        )

    spread = [1, depth - 1] + list(range(2, depth - 1))
    go(direct(1))
    for f in range(2):
        go(direct(2 * spread[0] + f))

    ready(4, 8)
    position = lax.broadcasted_iota(jnp.int32, (rows, LANES), 0) + me_e * rows
    angles = position.astype(F32) * freq[...]
    cosine = jnp.cos(angles)
    sine = jnp.sin(angles)
    latent = norm_rows(slat[...], sgain[...][None, :])
    lat_all[0, :, :rank] = latent
    key_rows = jnp.transpose(rkey[...].astype(F32))
    lat_all[0, :, rank:] = turn_pair(
        jnp.concatenate([key_rows, key_rows], axis=1), cosine, sine
    ).astype(BF16)
    lat_rows = rows // CORES

    def lat_at(i, core):
        return lat_all.at[i, pl.ds(pl.multiple_of(core * lat_rows, lat_rows), lat_rows), :]

    def lat_z(d):
        return remote(
            lat_at(2 * d - 2, c), lat_at(2 * d, c), lz_s.at[d], lz_r.at[d], ep_at(1, 0), me_t
        )

    def lat_x(d):
        return remote(
            lat_at(2 * d, c), lat_at(2 * d + 1, c), lx_s.at[d], lx_r.at[d], ep_at(0, 1), me_t
        )

    def lat_c(i, core):
        return remote(lat_at(i, core), lat_at(i, core), lc_s.at[i], lc_r.at[i], me_e, mate)

    def lat_up(d):
        if d + 1 < depth:
            go(lat_z(d + 1), jnp.logical_and(z >= d, z < depth - 1))

    def known(i):
        return x == 1 if i == 1 else z >= i // 2

    go(lat_x(0), x == 0)
    lat_up(0)
    for d in spread[1:]:
        for f in range(2):
            go(direct(2 * d + f))

    def z_arr(d):
        landed(lat_z(d), known(2 * d))
        lat_up(d)
        go(lat_x(d), known(2 * d))
        go(lat_c(2 * d, c), known(2 * d))

    def x_arr(d):
        landed(lat_x(d), known(2 * d + 1))
        go(lat_c(2 * d + 1, c), known(2 * d + 1))

    arr[0] = jnp.dot(chosen(me_e), normed[...], preferred_element_type=F32).astype(BF16)
    placed_t = jnp.transpose(placed)
    weight_t = jnp.transpose(weight)
    lane = lax.broadcasted_iota(jnp.int32, (tokens, n_ep), 1)
    slot_col = lax.broadcasted_iota(jnp.int32, (tokens, capacity), 1).astype(F32)
    for i in range(n_ep):
        mine = lane == ep_at(i // 2, i % 2)
        place = jnp.sum(jnp.where(mine, placed_t, 0.0), axis=1, keepdims=True)
        scale = jnp.sum(jnp.where(mine, weight_t, 0.0), axis=1, keepdims=True)
        mixing[i] = jnp.where(place == slot_col, scale, 0.0)

    ready(8, 12)
    query = norm_rows(qlat[...], qgain[...][None, :])
    plain = jnp.dot(query, qp_w[...], preferred_element_type=F32).astype(BF16)
    raw = jnp.dot(query, qt_w[...], preferred_element_type=F32)
    group = lax.broadcasted_iota(jnp.int32, (rows, LANES), 1) // ROPE
    for h in range(heads):
        j = h * ROPE // LANES
        turned = turn_pair(raw[:, j * LANES : (j + 1) * LANES], cosine, sine)
        turned = jnp.where(group == h % (LANES // ROPE), turned, 0.0)
        queries[:, h * head_keys : h * head_keys + NOPE] = plain[:, h * NOPE : (h + 1) * NOPE]
        queries[:, h * head_keys + NOPE : (h + 1) * head_keys] = turned.astype(BF16)

    def relay(i):
        direct(i).wait_recv()
        here = disp_at(i, me_t)
        go(remote(here, here, dy_s.at[i], dy_r.at[i], me_e, over))
        go(remote(here, here, dc_s.at[i, 0], dc_r.at[i, 0], me_e, mate))

    def forward(i):
        got = disp_at(i, over)
        remote(got, got, dy_s.at[i], dy_r.at[i], me_e, over).wait_recv()
        go(remote(got, got, dc_s.at[i, 1], dc_r.at[i, 1], me_e, mate))

    def arrive(i):
        for k, t in enumerate((mate, far)):
            got = disp_at(i, t)
            remote(got, got, dc_s.at[i, k], dc_r.at[i, k], me_e, mate).wait_recv()

    def project(i):
        at = slice(i * rows, (i + 1) * rows)
        latent = lat_all[i, :, :rank]
        k = jnp.dot(latent, key_w[...], preferred_element_type=F32).astype(BF16)
        values[at, :] = jnp.dot(latent, value_w[...], preferred_element_type=F32).astype(BF16)
        for h in range(heads):
            keys[at, h * head_keys : h * head_keys + NOPE] = k[:, h * NOPE : (h + 1) * NOPE]
            keys[at, h * head_keys + NOPE : (h + 1) * head_keys] = lat_all[i, :, rank:]

    def core_copy(i, k):
        t = mate if k == 0 else far
        return remote(
            part.at[i, :, cols(t)], ca.at[i, k], rc_s.at[i, k], rc_r.at[i, k], me_e, mate
        )

    def y_copy(i):
        return remote(sums.at[i], ya.at[i], ry_s.at[i], ry_r.at[i], me_e, over)

    def back(i):
        return remote(res.at[i], ret.at[i], re_s.at[i], re_r.at[i], ep_at(-(i // 2), i % 2), me_t)

    def y_step(i):
        core_copy(i, 1).wait_recv()
        sums[i] = (ca[i, 1].astype(F32) + part[i, :, cols(over)].astype(F32)).astype(BF16)
        go(y_copy(i))

    def sum_step(i):
        core_copy(i, 0).wait_recv()
        value = ca[i, 0].astype(F32) + part[i, :, cols(me_t)].astype(F32)
        y_copy(i).wait_recv()
        value = (value + ya[i].astype(F32)).astype(BF16)
        if i == 0:
            ret[0] = value
        else:
            res[i] = value
            go(back(i))

    def chunk(d):
        rows_in = arr[2 * d : 2 * d + 2].reshape(2 * capacity, width)
        gate = jnp.minimum(jnp.dot(rows_in, gate_w[...], preferred_element_type=F32), CLAMP_LIMIT)
        up = jnp.clip(
            jnp.dot(rows_in, up_w[...], preferred_element_type=F32), -CLAMP_LIMIT, CLAMP_LIMIT
        )
        hidden = ((up + 1.0) * (gate * jax.nn.sigmoid(SLOPE * gate))).astype(BF16)
        value = jnp.dot(hidden, down_w[...], preferred_element_type=F32)
        part[2 * d] = value[:capacity].astype(BF16)
        part[2 * d + 1] = value[capacity:].astype(BF16)
        for i in (2 * d, 2 * d + 1):
            for k in (1, 0):
                go(core_copy(i, k))

    log2e = 1.4426950408889634
    scaling = (NOPE + ROPE) ** (-0.5) * log2e

    def attend(h, first, last):
        at = slice(first * rows, last * rows)
        head = slice(h * head_keys, (h + 1) * head_keys)
        scores = lax.dot_general(
            queries[:, head], keys[at, head], (((1,), (1,)), ((), ())), preferred_element_type=F32
        )
        pieces = []
        for i in range(first, last):
            piece = scores[:, (i - first) * rows : (i - first + 1) * rows]
            if i == 0:
                row = lax.broadcasted_iota(jnp.int32, (rows, rows), 0)
                piece = jnp.where(
                    lax.broadcasted_iota(jnp.int32, (rows, rows), 1) <= row, piece, NEGATIVE
                )
            else:
                piece = piece + jnp.where(ep_at(-(i // 2), i % 2) < me_e, 0.0, NEGATIVE)
            pieces.append(piece)
        scores = jnp.concatenate(pieces, axis=1)
        peak = jnp.max(scores, axis=-1, keepdims=True)
        if first > 0:
            old = top[h]
            peak = jnp.maximum(peak, old)
        weight = jnp.exp2((scores - peak) * scaling)
        sum_of = jnp.sum(weight, axis=-1, keepdims=True)
        term = jnp.dot(
            weight.astype(BF16), values[at, h * VDIM : (h + 1) * VDIM], preferred_element_type=F32
        )
        if first > 0:
            fade = jnp.exp2((old - peak) * scaling)
            sum_of = sum_of + fade * total[h]
            term = term + fade * mixed[h]
        if last < n_ep:
            top[h] = peak
            total[h] = sum_of
            mixed[h] = term
        else:
            out[:, h * VDIM : (h + 1) * VDIM] = (term / sum_of).astype(BF16)

    def lat_arrive(i):
        landed(lat_c(i, 1 - c), known(i))

    acc = []

    def mix(i):
        if i > 0:
            back(i).wait_recv()
        table = mixing[i]
        high = table.astype(BF16)
        low = (table - high.astype(F32)).astype(BF16)
        term = jnp.dot(high, ret[i], preferred_element_type=F32) + jnp.dot(
            low, ret[i], preferred_element_type=F32
        )
        acc[:] = [term if not acc else acc[0] + term]

    def out_copy(k, t, to):
        ref = eout.at[:, cols(t)]
        s, r = (oy_s, oy_r) if k == 0 else (oc_s, oc_r)
        n = 0 if k < 2 else 1
        return remote(ref, ref, s.at[n], r.at[n], me_e, to)

    pieces = 4
    step = rows // pieces

    def mix_rows(n):
        return slice(n * step, (n + 1) * step)

    def mixer_core(n):
        return remote(
            msend.at[mix_rows(n)], mca.at[mix_rows(n)], mc_s.at[n], mc_r.at[n], me_e, mate
        )

    def mixer_y(n):
        return remote(
            msum.at[mix_rows(n)], mya.at[mix_rows(n)], my_s.at[n], my_r.at[n], me_e, over
        )

    def mixer_out(n, core):
        ref = mout.at[mix_rows(n), side(core)]
        return remote(ref, ref, mo_s.at[n], mo_r.at[n], me_e, mate)

    first, second, third = (2 * d for d in spread)
    middle = n_ep // 2
    ready(15, 17)
    project(0)
    relay(1)
    relay(first)
    relay(first + 1)
    forward(1)
    x_arr(0)
    z_arr(1)
    arrive(1)
    ready(12, 15)
    chunk(0)
    forward(first)
    forward(first + 1)
    relay(second)
    relay(second + 1)
    y_step(0)
    y_step(1)
    z_arr(2)
    x_arr(1)
    arrive(first)
    arrive(first + 1)
    chunk(first // 2)
    lat_arrive(1)
    project(1)
    forward(second)
    forward(second + 1)
    relay(third)
    relay(third + 1)
    z_arr(3)
    x_arr(2)
    y_step(first)
    y_step(first + 1)
    sum_step(0)
    sum_step(1)
    arrive(second)
    arrive(second + 1)
    chunk(second // 2)
    for i in range(2, middle):
        lat_arrive(i)
        project(i)
    forward(third)
    forward(third + 1)
    x_arr(3)
    y_step(second)
    y_step(second + 1)
    sum_step(first)
    sum_step(first + 1)
    for h in range(heads // 2):
        attend(h, 0, middle)
    arrive(third)
    arrive(third + 1)
    chunk(third // 2)
    for h in range(heads // 2, heads):
        attend(h, 0, middle)
    y_step(third)
    y_step(third + 1)
    for i in range(middle, n_ep):
        lat_arrive(i)
        project(i)
    sum_step(second)
    sum_step(second + 1)
    for h in range(heads):
        attend(h, middle, n_ep)
    ready(17, 18)
    msend[...] = jnp.dot(
        out[...], mixer_w[:, side(1 - c)], preferred_element_type=F32
    ).astype(BF16)
    for n in range(pieces):
        go(mixer_core(n))
    mown[...] = jnp.dot(out[...], mixer_w[:, side(c)], preferred_element_type=F32)
    sum_step(third)
    sum_step(third + 1)
    for n in range(pieces):
        mixer_core(n).wait_recv()
        at = mix_rows(n)
        msum[at] = (mown[at] + mca[at].astype(F32)).astype(BF16)
        go(mixer_y(n))
    for i in (0, first, second, third):
        mix(i)
        mix(i + 1)
    eout[:, cols(me_t)] = acc[0].astype(BF16)
    go(out_copy(0, me_t, over))
    go(out_copy(1, me_t, mate))
    for n in range(pieces):
        mixer_y(n).wait_recv()
        at = mix_rows(n)
        mout[at, side(c)] = (msum[at].astype(F32) + mya[at].astype(F32)).astype(BF16)
        go(mixer_out(n, c))
    out_copy(0, over, over).wait_recv()
    go(out_copy(2, over, mate))
    out_copy(1, mate, mate).wait_recv()
    out_copy(2, far, mate).wait_recv()
    for n in range(pieces):
        mixer_out(n, 1 - c).wait_recv()
    for when, copy in sends:
        if when is None:
            copy.wait_send()
        else:
            pl.when(when)(copy.wait_send)


def fused(
    n_ep,
    n_tp,
    query_latent,
    shared_latent,
    rotary_key,
    query_gain,
    shared_gain,
    query_plain_weight,
    query_turn_weight,
    key_weight,
    value_weight,
    mixer_out_weight,
    expert_input,
    expert_gain,
    routing,
    routing_weight,
    gate_weight,
    up_weight,
    down_weight,
):
    rows, query_rank = query_latent.shape
    rank = shared_latent.shape[1]
    heads = query_plain_weight.shape[1] // NOPE
    tokens, width = expert_input.shape
    top_count = routing.shape[1]
    units = gate_weight.shape[2]
    capacity = 4 * tokens * top_count // (3 * n_ep)
    capacity = -(-capacity // 8) * 8
    quarter = width // n_tp
    half = width // CORES
    depth = n_ep // 2
    total = n_ep * rows
    lane = np.arange(LANES)
    freq = ROTARY_BASE ** (-2.0 * (lane % (ROPE // 2)) / ROPE)
    freq = jnp.asarray(freq.astype(np.float32)[None, :])
    args = (
        routing.T,
        routing_weight.T,
        expert_input,
        expert_gain,
        shared_latent,
        shared_gain,
        rotary_key.T,
        query_latent,
        query_gain,
        freq,
        query_plain_weight,
        query_turn_weight,
        key_weight,
        value_weight,
        mixer_out_weight,
        gate_weight,
        up_weight,
        down_weight,
    )
    dma = pltpu.SemaphoreType.DMA
    held = [pltpu.VMEM(a.shape[1:] if a.ndim == 3 else a.shape, a.dtype) for a in args]
    expert_output, mixer_output = pl.pallas_call(
        functools.partial(step_kernel, n_ep, n_tp, heads),
        out_shape=(
            jax.ShapeDtypeStruct((tokens, width), BF16),
            jax.ShapeDtypeStruct((rows, width), BF16),
        ),
        in_specs=[pl.BlockSpec(memory_space=pltpu.HBM)] * len(args),
        out_specs=vmem(2),
        scratch_shapes=held
        + [
            dma((len(args),)),
            pltpu.VMEM((tokens, width), BF16),
            pltpu.VMEM((n_ep, tokens), F32),
            pltpu.VMEM((n_ep, tokens), F32),
            pltpu.VMEM((n_ep, capacity, quarter), BF16),
            pltpu.VMEM((n_ep, capacity, width), BF16),
            pltpu.VMEM((n_ep, tokens, capacity), F32),
            pltpu.VMEM((n_ep, rows, rank + LANES), BF16),
            pltpu.VMEM((rows, heads * (NOPE + LANES)), BF16),
            pltpu.VMEM((total, heads * (NOPE + LANES)), BF16),
            pltpu.VMEM((total, heads * VDIM), BF16),
            pltpu.VMEM((heads, rows, 1), F32),
            pltpu.VMEM((heads, rows, 1), F32),
            pltpu.VMEM((heads, rows, VDIM), F32),
            pltpu.VMEM((rows, heads * VDIM), BF16),
            pltpu.VMEM((n_ep, capacity, width), BF16),
            pltpu.VMEM((n_ep, CORES, capacity, quarter), BF16),
            pltpu.VMEM((n_ep, capacity, quarter), BF16),
            pltpu.VMEM((n_ep, capacity, quarter), BF16),
            pltpu.VMEM((n_ep, capacity, quarter), BF16),
            pltpu.VMEM((n_ep, capacity, quarter), BF16),
            pltpu.VMEM((rows, half), BF16),
            pltpu.VMEM((rows, half), F32),
            pltpu.VMEM((rows, half), BF16),
            pltpu.VMEM((rows, half), BF16),
            pltpu.VMEM((rows, half), BF16),
            dma((n_ep,)),
            dma((n_ep,)),
            dma((n_ep,)),
            dma((n_ep,)),
            dma((n_ep, 2)),
            dma((n_ep, 2)),
            dma((depth,)),
            dma((depth,)),
            dma((depth,)),
            dma((depth,)),
            dma((n_ep,)),
            dma((n_ep,)),
            dma((n_ep, 2)),
            dma((n_ep, 2)),
            dma((n_ep,)),
            dma((n_ep,)),
            dma((n_ep,)),
            dma((n_ep,)),
            dma((4,)),
            dma((4,)),
            dma((4,)),
            dma((4,)),
            dma((4,)),
            dma((4,)),
            dma((1,)),
            dma((1,)),
            dma((2,)),
            dma((2,)),
        ],
        compiler_params=pltpu.CompilerParams(
            collective_id=2, has_side_effects=True, vmem_limit_bytes=FUSED_LIMIT
        ),
    )(*args)
    return (mixer_output, expert_output)


def pick(mesh):
    small = mesh.shape["tp"] == 2 * CORES and mesh.shape["ep"] == 8
    return fused if small else per_device


def solution(mesh):
    return jax.shard_map(
        functools.partial(pick(mesh), mesh.shape["ep"], mesh.shape["tp"]),
        mesh=mesh,
        in_specs=(
            P("ep", None),
            P("ep", None),
            P("ep", None),
            P(),
            P(),
            P(None, "tp"),
            P(None, "tp"),
            P(None, "tp"),
            P(None, "tp"),
            P("tp", None),
            P("ep", None),
            P(),
            P("ep", None),
            P("ep", None),
            P("ep", None, "tp"),
            P("ep", None, "tp"),
            P("ep", "tp", None),
        ),
        out_specs=(P("ep", None), P("ep", None)),
        check_vma=False,
    )
```

```python
import functools

import jax
import jax.numpy as jnp
import numpy as np
from jax import lax
from jax.experimental import pallas as pl
from jax.experimental.pallas import tpu as pltpu
from jax.sharding import PartitionSpec as P

NOPE = 128
ROPE = 64
VDIM = 128
LANES = 128
CORES = 2

EPSILON = 1e-06
CLAMP_LIMIT = 7.0
SLOPE = 1.702
ROTARY_BASE = 10000.0
NEGATIVE = -1e30
VMEM_LIMIT = 60 * 1024 * 1024
PARTS = 4
FUSED_LIMIT = 58 * 1024 * 1024
F32 = jnp.float32
BF16 = jnp.bfloat16


def norm_scale(values):
    widened = values.astype(F32)
    return widened * lax.rsqrt(jnp.mean(widened * widened, axis=-1, keepdims=True) + EPSILON)


def norm_rows(values, gains):
    return (norm_scale(values) * gains).astype(BF16)


def rotate_heads(values, position):
    half = ROPE // 2
    lane = jnp.arange(values.shape[-1], dtype=jnp.int32)
    frequency = ROTARY_BASE ** (-2.0 * (lane % half).astype(F32) / ROPE)
    angles = position.astype(F32)[:, None] * frequency[None, :]
    upper = (lane % ROPE >= half)[None, :]
    swapped = jnp.where(upper, jnp.roll(values, half, axis=1), -jnp.roll(values, -half, axis=1))
    return values * jnp.cos(angles) + swapped * jnp.sin(angles)


def remote(src, dst, send_sem, recv_sem, ep, tp):
    return pltpu.make_async_remote_copy(
        src_ref=src,
        dst_ref=dst,
        send_sem=send_sem,
        recv_sem=recv_sem,
        device_id=(ep, tp),
        device_id_type=pl.DeviceIdType.MESH,
    )


def enter(n_ep, n_tp, me_e, me_t):
    barrier = pltpu.get_barrier_semaphore()
    for d in range(1, n_ep):
        pl.semaphore_signal(
            barrier,
            inc=1,
            device_id=(lax.rem(me_e + d, n_ep), me_t),
            device_id_type=pl.DeviceIdType.MESH,
        )
    for k in range(1, n_tp):
        pl.semaphore_signal(
            barrier,
            inc=1,
            device_id=(me_e, lax.rem(me_t + k, n_tp)),
            device_id_type=pl.DeviceIdType.MESH,
        )
    pl.semaphore_wait(barrier, n_ep - 1 + n_tp - 1)


def gather_kernel(
    n_ep,
    n_tp,
    heads,
    lat,
    disp,
    queries,
    key_w,
    value_w,
    mixer_w,
    arr,
    mpart,
    lat_all,
    out,
    keys,
    values,
    loc_sem,
    ep_s,
    ep_r,
    y_s,
    y_r,
    c_s,
    c_r,
):
    me_e = lax.axis_index("ep")
    me_t = lax.axis_index("tp")
    n_y = n_tp // CORES
    y = me_t // CORES
    c = lax.rem(me_t, CORES)
    mate = y * CORES + (1 - c)
    width = disp.shape[2]

    def place(j, e, t):
        if j == 0:
            return lat_all.at[e, t]
        return arr.at[e, :, pl.ds(pl.multiple_of(t * width, LANES), width)]

    local = []
    for j in range(2):
        copy = pltpu.make_async_copy(
            lat if j == 0 else disp.at[me_e], place(j, me_e, me_t), loc_sem.at[j]
        )
        copy.start()
        local.append(copy)
    enter(n_ep, n_tp, me_e, me_t)
    sends = []
    for j in range(2):
        for d in range(1, n_ep):
            peer = lax.rem(me_e + d, n_ep)
            copy = remote(
                lat if j == 0 else disp.at[peer],
                place(j, me_e, me_t),
                ep_s.at[d, j],
                ep_r.at[d, j],
                peer,
                me_t,
            )
            copy.start()
            sends.append(copy)

    def relay(j, d):
        src = lax.rem(me_e - d + n_ep, n_ep)
        here = place(j, src, me_t)
        if d == 0:
            local[j].wait()
        else:
            remote(here, here, ep_s.at[d, j], ep_r.at[d, j], src, me_t).wait_recv()
        for k in range(1, n_y):
            to = lax.rem(y + k, n_y) * CORES + c
            copy = remote(here, here, y_s.at[d, k, j], y_r.at[d, k, j], me_e, to)
            copy.start()
            sends.append(copy)
        copy = remote(here, here, c_s.at[d, 0, j], c_r.at[d, 0, j], me_e, mate)
        copy.start()
        sends.append(copy)

    def forward(j, d):
        src = lax.rem(me_e - d + n_ep, n_ep)
        for k in range(1, n_y):
            got = place(j, src, lax.rem(y - k + n_y, n_y) * CORES + c)
            remote(got, got, y_s.at[d, k, j], y_r.at[d, k, j], me_e, me_t).wait_recv()
            copy = remote(got, got, c_s.at[d, k, j], c_r.at[d, k, j], me_e, mate)
            copy.start()
            sends.append(copy)

    def arrive(j, d):
        src = lax.rem(me_e - d + n_ep, n_ep)
        for k in range(n_y):
            got = place(j, src, lax.rem(y - k + n_y, n_y) * CORES + (1 - c))
            remote(got, got, c_s.at[d, k, j], c_r.at[d, k, j], me_e, mate).wait_recv()

    for d in range(n_ep):
        relay(0, d)
        if d > 0:
            forward(0, d - 1)
    relay(1, 0)
    forward(0, n_ep - 1)
    for d in range(n_ep):
        arrive(0, d)
        if d % 2 == 1 and d // 2 + 1 < n_ep // 2:
            relay(1, d // 2 + 1)
        project(
            lax.rem(me_e - d + n_ep, n_ep), n_tp, heads, lat_all, key_w, value_w, keys, values
        )
    done = n_ep // 2
    for h in range(heads):
        attend(h, me_e, queries, keys, values, out)
        until = n_ep if h == heads - 1 else n_ep // 2 + (h + 1) * (n_ep // 2) // heads
        for d in range(done, until):
            relay(1, d)
        done = until
    mpart[...] = jnp.dot(out[...], mixer_w[...], preferred_element_type=F32).astype(BF16)
    for d in range(n_ep):
        forward(1, d)
    for d in range(n_ep):
        arrive(1, d)
    for copy in sends:
        copy.wait_send()


def project(e, n_tp, heads, lat_all, key_w, value_w, keys, values):
    share = lat_all.shape[2]
    rows = n_tp * share
    rank = key_w.shape[0]
    head_keys = NOPE + LANES
    at = pl.ds(pl.multiple_of(e * rows, rows), rows)
    block = lat_all[e].reshape(rows, rank + LANES)
    latent = block[:, :rank]
    k = jnp.dot(latent, key_w[...], preferred_element_type=F32).astype(BF16)
    values[at, :] = jnp.dot(latent, value_w[...], preferred_element_type=F32).astype(BF16)
    for h in range(heads):
        keys[at, h * head_keys : h * head_keys + NOPE] = k[:, h * NOPE : (h + 1) * NOPE]
        keys[at, h * head_keys + NOPE : (h + 1) * head_keys] = block[:, rank:]


def attend(h, me_e, queries, keys, values, out):
    rows = queries.shape[0]
    total = keys.shape[0]
    head_keys = NOPE + LANES
    row = lax.broadcasted_iota(jnp.int32, (rows, total), 0) + me_e * rows
    visible = lax.broadcasted_iota(jnp.int32, (rows, total), 1) <= row
    scaling = (NOPE + ROPE) ** (-0.5)
    cols = slice(h * head_keys, (h + 1) * head_keys)
    scores = lax.dot_general(
        queries[:, cols], keys[:, cols], (((1,), (1,)), ((), ())), preferred_element_type=F32
    )
    scores = jnp.where(visible, scores * scaling, NEGATIVE)
    weight = jnp.exp(scores - jnp.max(scores, axis=-1, keepdims=True))
    sums = jnp.sum(weight, axis=-1, keepdims=True)
    mixed = jnp.dot(
        weight.astype(BF16), values[:, h * VDIM : (h + 1) * VDIM], preferred_element_type=F32
    )
    out[:, h * VDIM : (h + 1) * VDIM] = (mixed / sums).astype(BF16)


def return_kernel(
    n_ep,
    n_tp,
    arrived,
    gate_hbm,
    up_hbm,
    down_hbm,
    mix,
    mpart,
    eout,
    mout,
    gate_w,
    up_w,
    down_w,
    load_sem,
    part,
    ca,
    sums,
    ya,
    res,
    ret,
    mca,
    msums,
    mya,
    ca_s,
    ca_r,
    ya_s,
    ya_r,
    ep_s,
    ep_r,
    oy_s,
    oy_r,
    oc_s,
    oc_r,
):
    me_e = lax.axis_index("ep")
    me_t = lax.axis_index("tp")
    n_y = n_tp // CORES
    y = me_t // CORES
    c = lax.rem(me_t, CORES)
    mate = y * CORES + (1 - c)
    width = res.shape[2]
    capacity = res.shape[1]
    pairs = n_ep // 2
    parity = lax.rem(me_e, 2)
    loads = []
    for n, (src, dst) in enumerate(((gate_hbm, gate_w), (up_hbm, up_w), (down_hbm, down_w))):
        copy = pltpu.make_async_copy(src.at[0], dst, load_sem.at[n])
        copy.start()
        loads.append(copy)

    def twin(i):
        return parity if i % 2 == 0 else 1 - parity

    def dest(i):
        return lax.rem(me_e // 2 + i // 2, pairs) * 2 + twin(i)

    def source(i):
        return lax.rem(me_e // 2 - i // 2 + pairs, pairs) * 2 + twin(i)

    def cols(t):
        return pl.ds(pl.multiple_of(t * width, LANES), width)

    def part_at(i, t):
        if i == n_ep:
            return mpart.at[:, cols(t)]
        return part.at[dest(i), :, cols(t)]

    def part_load(i, t):
        if i == n_ep:
            return mpart[:, cols(t)].astype(F32)
        return part[dest(i), :, cols(t)].astype(F32)

    enter(n_ep, n_tp, me_e, me_t)
    sends = []

    def go(copy):
        copy.start()
        sends.append(copy)

    def core_copy(i, k):
        dst = mca.at[k] if i == n_ep else ca.at[i, k]
        return remote(
            part_at(i, lax.rem(y + k, n_y) * CORES + (1 - c)),
            dst,
            ca_s.at[i, k],
            ca_r.at[i, k],
            me_e,
            mate,
        )

    def y_copy(i, k):
        src, dst = (msums, mya) if i == n_ep else (sums.at[i], ya.at[i])
        to = lax.rem(y + k, n_y) * CORES + c
        return remote(src.at[k - 1], dst.at[k - 1], ya_s.at[i, k], ya_r.at[i, k], me_e, to)

    def core_step(i):
        for k in list(range(1, n_y)) + [0]:
            go(core_copy(i, k))

    def y_step(i):
        for k in range(1, n_y):
            core_copy(i, k).wait_recv()
            got = (mca[k] if i == n_ep else ca[i, k]).astype(F32)
            value = (got + part_load(i, lax.rem(y + k, n_y) * CORES + c)).astype(BF16)
            if i == n_ep:
                msums[k - 1] = value
            else:
                sums[i, k - 1] = value
            go(y_copy(i, k))

    def ep_copy(i, e):
        return remote(res.at[i], ret.at[i], ep_s.at[i], ep_r.at[i], e, me_t)

    def sum_step(i):
        core_copy(i, 0).wait_recv()
        value = (mca[0] if i == n_ep else ca[i, 0]).astype(F32) + part_load(i, me_t)
        for k in range(1, n_y):
            y_copy(i, k).wait_recv()
            value = value + (mya[k - 1] if i == n_ep else ya[i, k - 1]).astype(F32)
        if i == n_ep:
            mout[:, cols(me_t)] = value.astype(BF16)
        elif i == 0:
            ret[0] = value.astype(BF16)
        else:
            res[i] = value.astype(BF16)
            go(ep_copy(i, dest(i)))

    def expert_step(s):
        base = lax.rem(me_e // 2 + s, pairs) * 2
        rows = arrived[pl.ds(pl.multiple_of(base * capacity, 2 * capacity), 2 * capacity), :]
        if s == 1 % pairs:
            loads[0].wait()
            loads[1].wait()
        gate = jnp.minimum(jnp.dot(rows, gate_w[...], preferred_element_type=F32), CLAMP_LIMIT)
        up = jnp.clip(
            jnp.dot(rows, up_w[...], preferred_element_type=F32), -CLAMP_LIMIT, CLAMP_LIMIT
        )
        hidden = ((up + 1.0) * (gate * jax.nn.sigmoid(SLOPE * gate))).astype(BF16)
        if s == 1 % pairs:
            loads[2].wait()
        value = jnp.dot(hidden, down_w[...], preferred_element_type=F32)
        part[base] = value[:capacity].astype(BF16)
        part[base + 1] = value[capacity:].astype(BF16)

    def out_copy(j, k, t, to, sem_s, sem_r):
        ref = (mout if j == 0 else eout).at[:, cols(t)]
        return remote(ref, ref, sem_s.at[j, k], sem_r.at[j, k], me_e, to)

    def out_send(j):
        for k in range(1, n_y):
            go(out_copy(j, k, me_t, lax.rem(y + k, n_y) * CORES + c, oy_s, oy_r))
        go(out_copy(j, 0, me_t, mate, oc_s, oc_r))

    core_step(n_ep)
    turns = [n % pairs for n in range(1, pairs + 1)]
    for n, turn in enumerate(turns):
        expert_step(turn)
        for i in (2 * turn, 2 * turn + 1):
            core_step(i)
        if n == 0:
            y_step(n_ep)
        for i in (2 * turn, 2 * turn + 1):
            y_step(i)
        if n > 0:
            for i in (2 * turns[n - 1], 2 * turns[n - 1] + 1):
                sum_step(i)
    sum_step(n_ep)
    out_send(0)
    for i in (1, 0):
        sum_step(i)
    acc = None
    for i in [0] + list(range(2, n_ep)) + [1]:
        if i > 0:
            ep_copy(i, source(i)).wait_recv()
        mixing = mix[source(i)]
        high = mixing.astype(BF16)
        low = (mixing - high.astype(F32)).astype(BF16)
        rows = ret[i]
        term = jnp.dot(high, rows, preferred_element_type=F32) + jnp.dot(
            low, rows, preferred_element_type=F32
        )
        acc = term if acc is None else acc + term
    eout[:, cols(me_t)] = acc.astype(BF16)
    out_send(1)
    for j in range(2):
        for k in range(1, n_y):
            t = lax.rem(y - k + n_y, n_y) * CORES + c
            out_copy(j, k, t, me_t, oy_s, oy_r).wait_recv()
            go(out_copy(j, k, t, mate, oc_s, oc_r))
    for j in range(2):
        for k in range(n_y):
            t = lax.rem(y - k + n_y, n_y) * CORES + (1 - c)
            out_copy(j, k, t, mate, oc_s, oc_r).wait_recv()
    for copy in sends:
        copy.wait_send()


def vmem(count):
    return [pl.BlockSpec(memory_space=pltpu.VMEM)] * count


def per_device(
    n_ep,
    n_tp,
    query_latent,
    shared_latent,
    rotary_key,
    query_gain,
    shared_gain,
    query_plain_weight,
    query_turn_weight,
    key_weight,
    value_weight,
    mixer_out_weight,
    expert_input,
    expert_gain,
    routing,
    routing_weight,
    gate_weight,
    up_weight,
    down_weight,
):
    me_e = lax.axis_index("ep")
    me_t = lax.axis_index("tp")
    n_y = n_tp // CORES
    row_count = query_latent.shape[0]
    heads = query_plain_weight.shape[1] // NOPE
    rank = shared_latent.shape[1]

    share = row_count // n_tp
    first = me_t * share
    lat = norm_rows(lax.dynamic_slice_in_dim(shared_latent, first, share, 0), shared_gain)
    own_position = me_e * row_count + first + jnp.arange(share, dtype=jnp.int32)
    turned = rotate_heads(
        lax.dynamic_slice_in_dim(rotary_key, first, share, 0).astype(F32), own_position
    ).astype(BF16)
    lat = jnp.concatenate([lat, turned, jnp.zeros((share, LANES - ROPE), BF16)], axis=1)

    token_count, width = expert_input.shape
    top_count = routing.shape[1]
    capacity = 4 * token_count * top_count // (3 * n_ep)
    capacity = -(-capacity // 8) * 8
    part_width = width // n_tp
    normed = norm_rows(expert_input, expert_gain)
    normed = lax.dynamic_slice_in_dim(normed, me_t * part_width, part_width, 1)
    flattened = routing.reshape(token_count * top_count)
    matches = flattened[:, None] == jnp.arange(n_ep, dtype=jnp.int32)[None, :]
    count = token_count * top_count
    lower = jnp.arange(count)[:, None] > jnp.arange(count)[None, :]
    ranking = jnp.dot(
        lower.astype(BF16), matches.astype(BF16), preferred_element_type=F32
    ).astype(jnp.int32)
    slot_index = jnp.sum(jnp.where(matches, ranking, 0), axis=1)
    target = (flattened * capacity + slot_index).reshape(token_count, top_count)
    slot_ids = jnp.arange(n_ep * capacity, dtype=jnp.int32)
    table = jnp.zeros((n_ep * capacity, token_count), jnp.bool_)
    mixing = jnp.zeros((token_count, n_ep * capacity), F32)
    for k in range(top_count):
        table = table | (target[:, k][None, :] == slot_ids[:, None])
        mixing = mixing + jnp.where(
            target[:, k][:, None] == slot_ids[None, :], routing_weight[:, k][:, None], 0.0
        )
    disp = jnp.dot(table.astype(BF16), normed, preferred_element_type=F32).astype(BF16)
    disp = disp.reshape(n_ep, capacity, part_width)
    mixing = jnp.transpose(mixing.reshape(token_count, n_ep, capacity), (1, 0, 2))

    position = me_e * row_count + jnp.arange(row_count, dtype=jnp.int32)
    query_normed = norm_rows(query_latent, query_gain)
    query_plain = jnp.dot(query_normed, query_plain_weight, preferred_element_type=F32)
    query_plain = query_plain.astype(BF16)
    query_raw = jnp.dot(query_normed, query_turn_weight, preferred_element_type=F32)
    query_turned = rotate_heads(query_raw, position).astype(BF16)
    blank = jnp.zeros((row_count, LANES - ROPE), BF16)
    pieces = []
    for h in range(heads):
        pieces.append(query_plain[:, h * NOPE : (h + 1) * NOPE])
        pieces.append(query_turned[:, h * ROPE : (h + 1) * ROPE])
        pieces.append(blank)
    queries = jnp.concatenate(pieces, axis=1)
    total = n_ep * row_count
    dma = pltpu.SemaphoreType.DMA
    arrived, mixer_partial = pl.pallas_call(
        functools.partial(gather_kernel, n_ep, n_tp, heads),
        out_shape=(
            jax.ShapeDtypeStruct((n_ep, capacity, width), BF16),
            jax.ShapeDtypeStruct((row_count, width), BF16),
        ),
        in_specs=vmem(6),
        out_specs=vmem(2),
        scratch_shapes=[
            pltpu.VMEM((n_ep, n_tp, share, rank + LANES), BF16),
            pltpu.VMEM((row_count, heads * VDIM), BF16),
            pltpu.VMEM((total, heads * (NOPE + LANES)), BF16),
            pltpu.VMEM((total, heads * VDIM), BF16),
            dma((2,)),
            dma((n_ep, 2)),
            dma((n_ep, 2)),
            dma((n_ep, n_y, 2)),
            dma((n_ep, n_y, 2)),
            dma((n_ep, n_y, 2)),
            dma((n_ep, n_y, 2)),
        ],
        compiler_params=pltpu.CompilerParams(
            collective_id=0, has_side_effects=True, vmem_limit_bytes=VMEM_LIMIT
        ),
    )(lat, disp, queries, key_weight, value_weight, mixer_out_weight)
    arrived = arrived.reshape(n_ep * capacity, width)
    units = gate_weight.shape[2]

    expert_output, mixer_output = pl.pallas_call(
        functools.partial(return_kernel, n_ep, n_tp),
        out_shape=(
            jax.ShapeDtypeStruct((token_count, width), BF16),
            jax.ShapeDtypeStruct((row_count, width), BF16),
        ),
        in_specs=vmem(1) + [pl.BlockSpec(memory_space=pl.ANY)] * 3 + vmem(2),
        out_specs=vmem(2),
        scratch_shapes=[
            pltpu.VMEM((width, units), BF16),
            pltpu.VMEM((width, units), BF16),
            pltpu.VMEM((units, width), BF16),
            dma((3,)),
            pltpu.VMEM((n_ep, capacity, width), BF16),
            pltpu.VMEM((n_ep, n_y, capacity, part_width), BF16),
            pltpu.VMEM((n_ep, n_y - 1, capacity, part_width), BF16),
            pltpu.VMEM((n_ep, n_y - 1, capacity, part_width), BF16),
            pltpu.VMEM((n_ep, capacity, part_width), BF16),
            pltpu.VMEM((n_ep, capacity, part_width), BF16),
            pltpu.VMEM((n_y, row_count, part_width), BF16),
            pltpu.VMEM((n_y - 1, row_count, part_width), BF16),
            pltpu.VMEM((n_y - 1, row_count, part_width), BF16),
            dma((n_ep + 1, n_y)),
            dma((n_ep + 1, n_y)),
            dma((n_ep + 1, n_y)),
            dma((n_ep + 1, n_y)),
            dma((n_ep,)),
            dma((n_ep,)),
            dma((2, n_y)),
            dma((2, n_y)),
            dma((2, n_y)),
            dma((2, n_y)),
        ],
        compiler_params=pltpu.CompilerParams(
            collective_id=1, has_side_effects=True, vmem_limit_bytes=VMEM_LIMIT
        ),
    )(arrived, gate_weight, up_weight, down_weight, mixing, mixer_partial)
    return (mixer_output, expert_output)


def take(src, dst, sem):
    copy = pltpu.make_async_copy(src, dst, sem)
    copy.start()
    return copy


def turn_pair(values, cosine, sine):
    half = ROPE // 2
    lane = lax.broadcasted_iota(jnp.int32, values.shape, 1)
    upper = lax.rem(lane, ROPE) >= half
    swapped = jnp.where(
        upper, pltpu.roll(values, half, 1), -pltpu.roll(values, LANES - half, 1)
    )
    return values * cosine + swapped * sine


def step_kernel(n_ep, n_tp, heads, *refs):
    (
        routing_h, share_h, ein_h, egain_h, slat_h, sgain_h, rkey_h, qlat_h, qgain_h, freq_h,
        qp_h, qt_h, kw_h, vw_h, mw_h, gate_h, up_h, down_h,
        eout_h, mout_h,
        eout, mout, keep_sem,
        routing, share, ein, egain, slat, sgain, rkey, qlat, qgain, freq,
        qp_w, qt_w, key_w, value_w, mixer_w, gate_w, up_w, down_w,
        load_sem,
        normed, ranks, weights, disp, arr, mixing,
        lat_all, queries, keys, values, top, total, mixed, out,
        part, ca, sums, ya, res, ret,
        msend, mown, mca, msum, mya,
        d_s, d_r, dy_s, dy_r, dc_s, dc_r,
        lz_s, lz_r, lx_s, lx_r, lc_s, lc_r,
        rc_s, rc_r, ry_s, ry_r, re_s, re_r,
        mc_s, mc_r, my_s, my_r, mo_s, mo_r,
        oy_s, oy_r, oc_s, oc_r,
    ) = refs
    me_e = lax.axis_index("ep")
    me_t = lax.axis_index("tp")
    depth = n_ep // 2
    z = me_e // 2
    x = lax.rem(me_e, 2)
    y = me_t // CORES
    c = lax.rem(me_t, CORES)
    mate = y * CORES + (1 - c)
    over = (1 - y) * CORES + c
    far = (1 - y) * CORES + (1 - c)
    tokens, width = ein.shape
    capacity = arr.shape[1]
    quarter = width // n_tp
    half = width // CORES
    rows = slat.shape[0]
    rank = slat.shape[1]
    head_keys = NOPE + LANES

    loads = []
    pairs = (
        (slat_h, slat), (sgain_h, sgain), (rkey_h, rkey), (freq_h, freq),
        (routing_h, routing), (share_h, share), (ein_h, ein), (egain_h, egain),
        (qlat_h, qlat), (qgain_h, qgain), (qp_h, qp_w), (qt_h, qt_w),
        (gate_h.at[0], gate_w), (up_h.at[0], up_w), (down_h.at[0], down_w),
        (kw_h, key_w), (vw_h, value_w), (mw_h, mixer_w),
    )
    for n, (src, dst) in enumerate(pairs):
        loads.append(take(src, dst, load_sem.at[n]))

    def ready(first, last):
        for n in range(first, last):
            loads[n].wait()

    def ep_at(d, f):
        return lax.rem(z + d + depth, depth) * 2 + (x if f == 0 else 1 - x)

    def cols(t):
        return pl.ds(pl.multiple_of(t * quarter, LANES), quarter)

    def side(core):
        return pl.ds(pl.multiple_of(core * half, LANES), half)

    lat_all[1:] = jnp.zeros((n_ep - 1, rows, rank + LANES), BF16)
    barrier = pltpu.get_barrier_semaphore()
    peers = [(ep_at(d, f), me_t) for d in range(depth) for f in range(2) if d or f]
    peers += [(me_e, t) for t in (mate, over)]
    for peer in peers:
        pl.semaphore_signal(
            barrier, inc=1, device_id=peer, device_id_type=pl.DeviceIdType.MESH
        )

    sends = []

    def go(copy, when=None):
        if when is None:
            copy.start()
        else:
            pl.when(when)(copy.start)
        sends.append((when, copy))

    def landed(copy, when):
        pl.when(when)(copy.wait_recv)

    lat_rows = rows // CORES

    def lat_at(i, core):
        return lat_all.at[i, pl.ds(pl.multiple_of(core * lat_rows, lat_rows), lat_rows), :]

    def lat_z(d):
        return remote(
            lat_at(2 * d - 2, c), lat_at(2 * d, c), lz_s.at[d], lz_r.at[d], ep_at(1, 0), me_t
        )

    def lat_x(d):
        return remote(
            lat_at(2 * d, c), lat_at(2 * d + 1, c), lx_s.at[d], lx_r.at[d], ep_at(0, 1), me_t
        )

    def lat_c(i, core):
        return remote(lat_at(i, core), lat_at(i, core), lc_s.at[i], lc_r.at[i], me_e, mate)

    def lat_up(d):
        if d + 1 < depth:
            go(lat_z(d + 1), jnp.logical_and(z >= d, z < depth - 1))

    def known(i):
        return x == 1 if i == 1 else z >= i // 2


    def z_arr(d):
        landed(lat_z(d), known(2 * d))
        lat_up(d)
        go(lat_x(d), known(2 * d))
        go(lat_c(2 * d, c), known(2 * d))

    def x_arr(d):
        landed(lat_x(d), known(2 * d + 1))
        go(lat_c(2 * d + 1, c), known(2 * d + 1))

    def chosen(e):
        return jnp.where(ranks[pl.ds(e, 1), :] == slot_row, 1.0, 0.0).astype(BF16)

    def disp_at(i, t):
        return arr.at[i, :, cols(t)]

    def direct(i):
        return remote(
            disp.at[i], disp_at(i, me_t), d_s.at[i], d_r.at[i], ep_at(i // 2, i % 2), me_t
        )

    kept = []

    def keep(src, dst, at):
        kept.append(take(src.at[at], dst.at[at], keep_sem.at[len(kept)]))

    def relay(i):
        direct(i).wait_recv()
        here = disp_at(i, me_t)
        go(remote(here, here, dy_s.at[i], dy_r.at[i], me_e, over))
        go(remote(here, here, dc_s.at[i, 0], dc_r.at[i, 0], me_e, mate))

    def forward(i):
        got = disp_at(i, over)
        remote(got, got, dy_s.at[i], dy_r.at[i], me_e, over).wait_recv()
        go(remote(got, got, dc_s.at[i, 1], dc_r.at[i, 1], me_e, mate))

    def arrive(i):
        for k, t in enumerate((mate, far)):
            got = disp_at(i, t)
            remote(got, got, dc_s.at[i, k], dc_r.at[i, k], me_e, mate).wait_recv()

    def project(i):
        at = slice(i * rows, (i + 1) * rows)
        latent = lat_all[i, :, :rank]
        k = jnp.dot(latent, key_w[...], preferred_element_type=F32).astype(BF16)
        values[at, :] = jnp.dot(latent, value_w[...], preferred_element_type=F32).astype(BF16)
        for h in range(heads):
            keys[at, h * head_keys : h * head_keys + NOPE] = k[:, h * NOPE : (h + 1) * NOPE]
            keys[at, h * head_keys + NOPE : (h + 1) * head_keys] = lat_all[i, :, rank:]

    def core_copy(i, k):
        t = mate if k == 0 else far
        return remote(
            part.at[i, :, cols(t)], ca.at[i, k], rc_s.at[i, k], rc_r.at[i, k], me_e, mate
        )

    def y_copy(i):
        return remote(sums.at[i], ya.at[i], ry_s.at[i], ry_r.at[i], me_e, over)

    def back(i):
        return remote(res.at[i], ret.at[i], re_s.at[i], re_r.at[i], ep_at(-(i // 2), i % 2), me_t)

    def y_step(i):
        core_copy(i, 1).wait_recv()
        sums[i] = (ca[i, 1].astype(F32) + part[i, :, cols(over)].astype(F32)).astype(BF16)
        go(y_copy(i))

    def sum_step(i):
        core_copy(i, 0).wait_recv()
        value = ca[i, 0].astype(F32) + part[i, :, cols(me_t)].astype(F32)
        y_copy(i).wait_recv()
        value = (value + ya[i].astype(F32)).astype(BF16)
        if i == 0:
            ret[0] = value
        else:
            res[i] = value
            go(back(i))

    def chunk(d):
        rows_in = arr[2 * d : 2 * d + 2].reshape(2 * capacity, width)
        gate = jnp.minimum(jnp.dot(rows_in, gate_w[...], preferred_element_type=F32), CLAMP_LIMIT)
        up = jnp.clip(
            jnp.dot(rows_in, up_w[...], preferred_element_type=F32), -CLAMP_LIMIT, CLAMP_LIMIT
        )
        hidden = ((up + 1.0) * (gate * jax.nn.sigmoid(SLOPE * gate))).astype(BF16)
        value = jnp.dot(hidden, down_w[...], preferred_element_type=F32)
        part[2 * d] = value[:capacity].astype(BF16)
        part[2 * d + 1] = value[capacity:].astype(BF16)
        for i in (2 * d, 2 * d + 1):
            for k in (1, 0):
                go(core_copy(i, k))

    log2e = 1.4426950408889634
    scaling = (NOPE + ROPE) ** (-0.5) * log2e

    def attend(h, first, last):
        at = slice(first * rows, last * rows)
        head = slice(h * head_keys, (h + 1) * head_keys)
        scores = lax.dot_general(
            queries[:, head], keys[at, head], (((1,), (1,)), ((), ())), preferred_element_type=F32
        )
        pieces = []
        for i in range(first, last):
            piece = scores[:, (i - first) * rows : (i - first + 1) * rows]
            if i == 0:
                row = lax.broadcasted_iota(jnp.int32, (rows, rows), 0)
                piece = jnp.where(
                    lax.broadcasted_iota(jnp.int32, (rows, rows), 1) <= row, piece, NEGATIVE
                )
            else:
                piece = piece + jnp.where(ep_at(-(i // 2), i % 2) < me_e, 0.0, NEGATIVE)
            pieces.append(piece)
        scores = jnp.concatenate(pieces, axis=1)
        peak = jnp.max(scores, axis=-1, keepdims=True)
        if first > 0:
            old = top[h]
            peak = jnp.maximum(peak, old)
        weight = jnp.exp2((scores - peak) * scaling)
        sum_of = jnp.sum(weight, axis=-1, keepdims=True)
        term = jnp.dot(
            weight.astype(BF16), values[at, h * VDIM : (h + 1) * VDIM], preferred_element_type=F32
        )
        if first > 0:
            fade = jnp.exp2((old - peak) * scaling)
            sum_of = sum_of + fade * total[h]
            term = term + fade * mixed[h]
        if last < n_ep:
            top[h] = peak
            total[h] = sum_of
            mixed[h] = term
        else:
            out[:, h * VDIM : (h + 1) * VDIM] = (term / sum_of).astype(BF16)

    def lat_arrive(i):
        landed(lat_c(i, 1 - c), known(i))

    acc = []

    def mix(i):
        if i > 0:
            back(i).wait_recv()
        table = mixing[i]
        high = table.astype(BF16)
        low = (table - high.astype(F32)).astype(BF16)
        term = jnp.dot(high, ret[i], preferred_element_type=F32) + jnp.dot(
            low, ret[i], preferred_element_type=F32
        )
        acc[:] = [term if not acc else acc[0] + term]

    def out_copy(k, t, to):
        ref = eout.at[:, cols(t)]
        s, r = (oy_s, oy_r) if k == 0 else (oc_s, oc_r)
        n = 0 if k < 2 else 1
        return remote(ref, ref, s.at[n], r.at[n], me_e, to)

    pieces = 4
    step = rows // pieces

    def mix_rows(n):
        return slice(n * step, (n + 1) * step)

    def mixer_core(n):
        return remote(
            msend.at[mix_rows(n)], mca.at[mix_rows(n)], mc_s.at[n], mc_r.at[n], me_e, mate
        )

    def mixer_y(n):
        return remote(
            msum.at[mix_rows(n)], mya.at[mix_rows(n)], my_s.at[n], my_r.at[n], me_e, over
        )

    def mixer_out(n, core):
        ref = mout.at[mix_rows(n), side(core)]
        return remote(ref, ref, mo_s.at[n], mo_r.at[n], me_e, mate)

    def mixer_turn(n):
        mixer_core(n).wait_recv()
        at = mix_rows(n)
        msum[at] = (mown[at] + mca[at].astype(F32)).astype(BF16)
        go(mixer_y(n))

    def mixer_end(n):
        mixer_y(n).wait_recv()
        at = mix_rows(n)
        mout[at, side(c)] = (msum[at].astype(F32) + mya[at].astype(F32)).astype(BF16)
        go(mixer_out(n, c))
        keep(mout, mout_h, (mix_rows(n), side(c)))

    middle = n_ep // 2
    ready(4, 6)
    expert = lax.broadcasted_iota(jnp.int32, (n_ep, tokens), 0)
    member = jnp.zeros((n_ep, tokens), F32)
    weight = jnp.zeros((n_ep, tokens), F32)
    for k in range(routing.shape[0]):
        named = routing[k : k + 1, :] == expert
        member = member + jnp.where(named, 1.0, 0.0)
        weight = weight + jnp.where(named, share[k : k + 1, :], 0.0)
    before = lax.broadcasted_iota(jnp.int32, (tokens, tokens), 0) < lax.broadcasted_iota(
        jnp.int32, (tokens, tokens), 1
    )
    placed = jnp.dot(
        member.astype(BF16),
        jnp.where(before, 1.0, 0.0).astype(BF16),
        preferred_element_type=F32,
    )
    placed = jnp.where(member > 0.0, placed, -1.0)
    ranks[...] = placed
    ready(6, 8)
    normed[...] = norm_rows(ein[...], egain[...][None, :])
    slot_row = lax.broadcasted_iota(jnp.int32, (capacity, tokens), 0).astype(F32)

    own_cols = normed[:, cols(me_t)]
    for d in range(depth):
        for f in range(2):
            if d or f:
                disp[2 * d + f] = jnp.dot(
                    chosen(ep_at(d, f)), own_cols, preferred_element_type=F32
                ).astype(BF16)
    pl.semaphore_wait(barrier, len(peers))
    go(direct(3))
    ready(0, 4)
    position = lax.broadcasted_iota(jnp.int32, (rows, LANES), 0) + me_e * rows
    angles = position.astype(F32) * freq[...]
    cosine = jnp.cos(angles)
    sine = jnp.sin(angles)
    latent = norm_rows(slat[...], sgain[...][None, :])
    lat_all[0, :, :rank] = latent
    key_rows = jnp.transpose(rkey[...].astype(F32))
    lat_all[0, :, rank:] = turn_pair(
        jnp.concatenate([key_rows, key_rows], axis=1), cosine, sine
    ).astype(BF16)
    go(direct(2))
    go(direct(1))
    ready(15, 17)
    project(0)
    lat_up(0)
    go(direct(7))
    relay(1)
    relay(3)
    go(lat_x(0), x == 0)
    go(direct(6))
    forward(1)
    relay(2)
    relay(7)
    z_arr(1)
    forward(3)
    x_arr(0)
    forward(2)
    relay(6)
    arrive(1)
    lat_arrive(2)
    go(direct(5))
    arr[0] = jnp.dot(chosen(me_e), normed[...], preferred_element_type=F32).astype(BF16)
    placed_t = jnp.transpose(placed)
    weight_t = jnp.transpose(weight)
    lane = lax.broadcasted_iota(jnp.int32, (tokens, n_ep), 1)
    slot_col = lax.broadcasted_iota(jnp.int32, (tokens, capacity), 1).astype(F32)
    for i in range(n_ep):
        mine = lane == ep_at(i // 2, i % 2)
        place = jnp.sum(jnp.where(mine, placed_t, 0.0), axis=1, keepdims=True)
        scale = jnp.sum(jnp.where(mine, weight_t, 0.0), axis=1, keepdims=True)
        mixing[i] = jnp.where(place == slot_col, scale, 0.0)

    arrive(3)
    ready(12, 15)
    chunk(0)
    z_arr(2)
    arrive(2)
    chunk(1)
    y_step(1)
    lat_arrive(1)
    forward(7)
    x_arr(1)
    go(direct(4))
    project(1)
    y_step(2)
    ready(8, 12)
    query = norm_rows(qlat[...], qgain[...][None, :])
    plain = jnp.dot(query, qp_w[...], preferred_element_type=F32).astype(BF16)
    raw = jnp.dot(query, qt_w[...], preferred_element_type=F32)
    group = lax.broadcasted_iota(jnp.int32, (rows, LANES), 1) // ROPE
    for h in range(heads):
        j = h * ROPE // LANES
        turned = turn_pair(raw[:, j * LANES : (j + 1) * LANES], cosine, sine)
        turned = jnp.where(group == h % (LANES // ROPE), turned, 0.0)
        queries[:, h * head_keys : h * head_keys + NOPE] = plain[:, h * NOPE : (h + 1) * NOPE]
        queries[:, h * head_keys + NOPE : (h + 1) * head_keys] = turned.astype(BF16)

    lat_arrive(3)
    forward(6)
    arrive(7)
    project(2)
    arrive(6)
    project(3)
    sum_step(1)
    lat_arrive(4)
    relay(5)
    chunk(3)
    relay(4)
    z_arr(3)
    x_arr(2)
    attend(0, 0, middle)
    project(4)
    forward(5)
    y_step(3)
    sum_step(2)
    y_step(7)
    attend(2, 0, middle)
    lat_arrive(6)
    mix(1)
    attend(3, 0, middle)
    y_step(6)
    lat_arrive(5)
    project(6)
    forward(4)
    project(5)
    attend(1, 0, middle)
    arrive(4)
    y_step(0)
    arrive(5)
    x_arr(3)
    chunk(2)
    sum_step(3)
    lat_arrive(7)
    project(7)
    attend(3, middle, n_ep)
    attend(0, middle, n_ep)
    y_step(5)
    attend(2, middle, n_ep)
    sum_step(7)
    sum_step(6)
    y_step(4)
    attend(1, middle, n_ep)
    ready(17, 18)
    msend[...] = jnp.dot(
        out[...], mixer_w[:, side(1 - c)], preferred_element_type=F32
    ).astype(BF16)
    for n in range(pieces):
        go(mixer_core(n))
    sum_step(0)
    mown[...] = jnp.dot(out[...], mixer_w[:, side(c)], preferred_element_type=F32)
    sum_step(5)
    mixer_turn(0)
    mixer_turn(3)
    sum_step(4)
    mix(2)
    mixer_turn(1)
    mix(6)
    mix(7)
    mix(0)
    mixer_turn(2)
    mix(3)
    mix(5)
    mixer_end(1)
    mix(4)
    eout[:, cols(me_t)] = acc[0].astype(BF16)
    go(out_copy(0, me_t, over))
    go(out_copy(1, me_t, mate))
    keep(eout, eout_h, (slice(None), cols(me_t)))
    mixer_end(0)
    mixer_end(3)
    mixer_end(2)
    out_copy(0, over, over).wait_recv()
    go(out_copy(2, over, mate))
    keep(eout, eout_h, (slice(None), cols(over)))
    for n in range(pieces):
        mixer_out(n, 1 - c).wait_recv()
        keep(mout, mout_h, (mix_rows(n), side(1 - c)))
    out_copy(1, mate, mate).wait_recv()
    keep(eout, eout_h, (slice(None), cols(mate)))
    out_copy(2, far, mate).wait_recv()
    keep(eout, eout_h, (slice(None), cols(far)))
    for copy in kept:
        copy.wait()
    for when, copy in sends:
        if when is None:
            copy.wait_send()
        else:
            pl.when(when)(copy.wait_send)


def fused(
    n_ep,
    n_tp,
    query_latent,
    shared_latent,
    rotary_key,
    query_gain,
    shared_gain,
    query_plain_weight,
    query_turn_weight,
    key_weight,
    value_weight,
    mixer_out_weight,
    expert_input,
    expert_gain,
    routing,
    routing_weight,
    gate_weight,
    up_weight,
    down_weight,
):
    rows, query_rank = query_latent.shape
    rank = shared_latent.shape[1]
    heads = query_plain_weight.shape[1] // NOPE
    tokens, width = expert_input.shape
    top_count = routing.shape[1]
    units = gate_weight.shape[2]
    capacity = 4 * tokens * top_count // (3 * n_ep)
    capacity = -(-capacity // 8) * 8
    quarter = width // n_tp
    half = width // CORES
    depth = n_ep // 2
    total = n_ep * rows
    lane = np.arange(LANES)
    freq = ROTARY_BASE ** (-2.0 * (lane % (ROPE // 2)) / ROPE)
    freq = jnp.asarray(freq.astype(np.float32)[None, :])
    args = (
        routing.T,
        routing_weight.T,
        expert_input,
        expert_gain,
        shared_latent,
        shared_gain,
        rotary_key.T,
        query_latent,
        query_gain,
        freq,
        query_plain_weight,
        query_turn_weight,
        key_weight,
        value_weight,
        mixer_out_weight,
        gate_weight,
        up_weight,
        down_weight,
    )
    dma = pltpu.SemaphoreType.DMA
    held = [pltpu.VMEM(a.shape[1:] if a.ndim == 3 else a.shape, a.dtype) for a in args]
    expert_output, mixer_output = pl.pallas_call(
        functools.partial(step_kernel, n_ep, n_tp, heads),
        out_shape=(
            jax.ShapeDtypeStruct((tokens, width), BF16),
            jax.ShapeDtypeStruct((rows, width), BF16),
        ),
        in_specs=[pl.BlockSpec(memory_space=pltpu.HBM)] * len(args),
        out_specs=[pl.BlockSpec(memory_space=pltpu.HBM)] * 2,
        scratch_shapes=[
            pltpu.VMEM((tokens, width), BF16),
            pltpu.VMEM((rows, width), BF16),
            dma((12,)),
        ]
        + held
        + [
            dma((len(args),)),
            pltpu.VMEM((tokens, width), BF16),
            pltpu.VMEM((n_ep, tokens), F32),
            pltpu.VMEM((n_ep, tokens), F32),
            pltpu.VMEM((n_ep, capacity, quarter), BF16),
            pltpu.VMEM((n_ep, capacity, width), BF16),
            pltpu.VMEM((n_ep, tokens, capacity), F32),
            pltpu.VMEM((n_ep, rows, rank + LANES), BF16),
            pltpu.VMEM((rows, heads * (NOPE + LANES)), BF16),
            pltpu.VMEM((total, heads * (NOPE + LANES)), BF16),
            pltpu.VMEM((total, heads * VDIM), BF16),
            pltpu.VMEM((heads, rows, 1), F32),
            pltpu.VMEM((heads, rows, 1), F32),
            pltpu.VMEM((heads, rows, VDIM), F32),
            pltpu.VMEM((rows, heads * VDIM), BF16),
            pltpu.VMEM((n_ep, capacity, width), BF16),
            pltpu.VMEM((n_ep, CORES, capacity, quarter), BF16),
            pltpu.VMEM((n_ep, capacity, quarter), BF16),
            pltpu.VMEM((n_ep, capacity, quarter), BF16),
            pltpu.VMEM((n_ep, capacity, quarter), BF16),
            pltpu.VMEM((n_ep, capacity, quarter), BF16),
            pltpu.VMEM((rows, half), BF16),
            pltpu.VMEM((rows, half), F32),
            pltpu.VMEM((rows, half), BF16),
            pltpu.VMEM((rows, half), BF16),
            pltpu.VMEM((rows, half), BF16),
            dma((n_ep,)),
            dma((n_ep,)),
            dma((n_ep,)),
            dma((n_ep,)),
            dma((n_ep, 2)),
            dma((n_ep, 2)),
            dma((depth,)),
            dma((depth,)),
            dma((depth,)),
            dma((depth,)),
            dma((n_ep,)),
            dma((n_ep,)),
            dma((n_ep, 2)),
            dma((n_ep, 2)),
            dma((n_ep,)),
            dma((n_ep,)),
            dma((n_ep,)),
            dma((n_ep,)),
            dma((4,)),
            dma((4,)),
            dma((4,)),
            dma((4,)),
            dma((4,)),
            dma((4,)),
            dma((1,)),
            dma((1,)),
            dma((2,)),
            dma((2,)),
        ],
        compiler_params=pltpu.CompilerParams(
            collective_id=2, has_side_effects=True, vmem_limit_bytes=FUSED_LIMIT
        ),
    )(*args)
    results = (mixer_output, expert_output)
    return tuple(
        pl.pallas_call(
            settle,
            out_shape=tuple(jax.ShapeDtypeStruct(r.shape, r.dtype) for r in results),
            in_specs=[pl.BlockSpec(memory_space=pltpu.HBM)] * 2,
            out_specs=[pl.BlockSpec(memory_space=pltpu.HBM)] * 2,
            scratch_shapes=[pltpu.VMEM(r.shape, r.dtype) for r in results]
            + [dma((2, PARTS)), dma((2, PARTS))],
        )(*results)
    )


def settle(first_in, second_in, first_out, second_out, first_held, second_held, in_sem, out_sem):
    arrays = ((first_in, first_held, first_out), (second_in, second_held, second_out))
    coming = []
    for j, (src, held, dst) in enumerate(arrays):
        step = held.shape[0] // PARTS
        for n in range(PARTS):
            at = slice(n * step, (n + 1) * step)
            coming.append((take(src.at[at], held.at[at], in_sem.at[j, n]), held, dst, at, j, n))
    leaving = []
    for copy, held, dst, at, j, n in coming:
        copy.wait()
        leaving.append(take(held.at[at], dst.at[at], out_sem.at[j, n]))
    for copy in leaving:
        copy.wait()


def pick(mesh):
    small = mesh.shape["tp"] == 2 * CORES and mesh.shape["ep"] == 8
    return fused if small else per_device


def solution(mesh):
    return jax.shard_map(
        functools.partial(pick(mesh), mesh.shape["ep"], mesh.shape["tp"]),
        mesh=mesh,
        in_specs=(
            P("ep", None),
            P("ep", None),
            P("ep", None),
            P(),
            P(),
            P(None, "tp"),
            P(None, "tp"),
            P(None, "tp"),
            P(None, "tp"),
            P("tp", None),
            P("ep", None),
            P(),
            P("ep", None),
            P("ep", None),
            P("ep", None, "tp"),
            P("ep", None, "tp"),
            P("ep", "tp", None),
        ),
        out_specs=(P("ep", None), P("ep", None)),
        check_vma=False,
    )
```

```python
import functools

import jax
import jax.numpy as jnp
import numpy as np
from jax import lax
from jax.experimental import pallas as pl
from jax.experimental.pallas import tpu as pltpu
from jax.sharding import PartitionSpec as P

NOPE = 128
ROPE = 64
VDIM = 128
LANES = 128
CORES = 2

EPSILON = 1e-06
CLAMP_LIMIT = 7.0
SLOPE = 1.702
ROTARY_BASE = 10000.0
NEGATIVE = -1e30
VMEM_LIMIT = 60 * 1024 * 1024
PARTS = 4
FUSED_LIMIT = 58 * 1024 * 1024
F32 = jnp.float32
BF16 = jnp.bfloat16


def norm_scale(values):
    widened = values.astype(F32)
    return widened * lax.rsqrt(jnp.mean(widened * widened, axis=-1, keepdims=True) + EPSILON)


def norm_rows(values, gains):
    return (norm_scale(values) * gains).astype(BF16)


def rotate_heads(values, position):
    half = ROPE // 2
    lane = jnp.arange(values.shape[-1], dtype=jnp.int32)
    frequency = ROTARY_BASE ** (-2.0 * (lane % half).astype(F32) / ROPE)
    angles = position.astype(F32)[:, None] * frequency[None, :]
    upper = (lane % ROPE >= half)[None, :]
    swapped = jnp.where(upper, jnp.roll(values, half, axis=1), -jnp.roll(values, -half, axis=1))
    return values * jnp.cos(angles) + swapped * jnp.sin(angles)


def remote(src, dst, send_sem, recv_sem, ep, tp):
    return pltpu.make_async_remote_copy(
        src_ref=src,
        dst_ref=dst,
        send_sem=send_sem,
        recv_sem=recv_sem,
        device_id=(ep, tp),
        device_id_type=pl.DeviceIdType.MESH,
    )


def enter(n_ep, n_tp, me_e, me_t):
    barrier = pltpu.get_barrier_semaphore()
    for d in range(1, n_ep):
        pl.semaphore_signal(
            barrier,
            inc=1,
            device_id=(lax.rem(me_e + d, n_ep), me_t),
            device_id_type=pl.DeviceIdType.MESH,
        )
    for k in range(1, n_tp):
        pl.semaphore_signal(
            barrier,
            inc=1,
            device_id=(me_e, lax.rem(me_t + k, n_tp)),
            device_id_type=pl.DeviceIdType.MESH,
        )
    pl.semaphore_wait(barrier, n_ep - 1 + n_tp - 1)


def gather_kernel(
    n_ep,
    n_tp,
    heads,
    lat,
    disp,
    queries,
    key_w,
    value_w,
    mixer_w,
    arr,
    mpart,
    lat_all,
    out,
    keys,
    values,
    loc_sem,
    ep_s,
    ep_r,
    y_s,
    y_r,
    c_s,
    c_r,
):
    me_e = lax.axis_index("ep")
    me_t = lax.axis_index("tp")
    n_y = n_tp // CORES
    y = me_t // CORES
    c = lax.rem(me_t, CORES)
    mate = y * CORES + (1 - c)
    width = disp.shape[2]

    def place(j, e, t):
        if j == 0:
            return lat_all.at[e, t]
        return arr.at[e, :, pl.ds(pl.multiple_of(t * width, LANES), width)]

    local = []
    for j in range(2):
        copy = pltpu.make_async_copy(
            lat if j == 0 else disp.at[me_e], place(j, me_e, me_t), loc_sem.at[j]
        )
        copy.start()
        local.append(copy)
    enter(n_ep, n_tp, me_e, me_t)
    sends = []
    for j in range(2):
        for d in range(1, n_ep):
            peer = lax.rem(me_e + d, n_ep)
            copy = remote(
                lat if j == 0 else disp.at[peer],
                place(j, me_e, me_t),
                ep_s.at[d, j],
                ep_r.at[d, j],
                peer,
                me_t,
            )
            copy.start()
            sends.append(copy)

    def relay(j, d):
        src = lax.rem(me_e - d + n_ep, n_ep)
        here = place(j, src, me_t)
        if d == 0:
            local[j].wait()
        else:
            remote(here, here, ep_s.at[d, j], ep_r.at[d, j], src, me_t).wait_recv()
        for k in range(1, n_y):
            to = lax.rem(y + k, n_y) * CORES + c
            copy = remote(here, here, y_s.at[d, k, j], y_r.at[d, k, j], me_e, to)
            copy.start()
            sends.append(copy)
        copy = remote(here, here, c_s.at[d, 0, j], c_r.at[d, 0, j], me_e, mate)
        copy.start()
        sends.append(copy)

    def forward(j, d):
        src = lax.rem(me_e - d + n_ep, n_ep)
        for k in range(1, n_y):
            got = place(j, src, lax.rem(y - k + n_y, n_y) * CORES + c)
            remote(got, got, y_s.at[d, k, j], y_r.at[d, k, j], me_e, me_t).wait_recv()
            copy = remote(got, got, c_s.at[d, k, j], c_r.at[d, k, j], me_e, mate)
            copy.start()
            sends.append(copy)

    def arrive(j, d):
        src = lax.rem(me_e - d + n_ep, n_ep)
        for k in range(n_y):
            got = place(j, src, lax.rem(y - k + n_y, n_y) * CORES + (1 - c))
            remote(got, got, c_s.at[d, k, j], c_r.at[d, k, j], me_e, mate).wait_recv()

    for d in range(n_ep):
        relay(0, d)
        if d > 0:
            forward(0, d - 1)
    relay(1, 0)
    forward(0, n_ep - 1)
    for d in range(n_ep):
        arrive(0, d)
        if d % 2 == 1 and d // 2 + 1 < n_ep // 2:
            relay(1, d // 2 + 1)
        project(
            lax.rem(me_e - d + n_ep, n_ep), n_tp, heads, lat_all, key_w, value_w, keys, values
        )
    done = n_ep // 2
    for h in range(heads):
        attend(h, me_e, queries, keys, values, out)
        until = n_ep if h == heads - 1 else n_ep // 2 + (h + 1) * (n_ep // 2) // heads
        for d in range(done, until):
            relay(1, d)
        done = until
    mpart[...] = jnp.dot(out[...], mixer_w[...], preferred_element_type=F32).astype(BF16)
    for d in range(n_ep):
        forward(1, d)
    for d in range(n_ep):
        arrive(1, d)
    for copy in sends:
        copy.wait_send()


def project(e, n_tp, heads, lat_all, key_w, value_w, keys, values):
    share = lat_all.shape[2]
    rows = n_tp * share
    rank = key_w.shape[0]
    head_keys = NOPE + LANES
    at = pl.ds(pl.multiple_of(e * rows, rows), rows)
    block = lat_all[e].reshape(rows, rank + LANES)
    latent = block[:, :rank]
    k = jnp.dot(latent, key_w[...], preferred_element_type=F32).astype(BF16)
    values[at, :] = jnp.dot(latent, value_w[...], preferred_element_type=F32).astype(BF16)
    for h in range(heads):
        keys[at, h * head_keys : h * head_keys + NOPE] = k[:, h * NOPE : (h + 1) * NOPE]
        keys[at, h * head_keys + NOPE : (h + 1) * head_keys] = block[:, rank:]


def attend(h, me_e, queries, keys, values, out):
    rows = queries.shape[0]
    total = keys.shape[0]
    head_keys = NOPE + LANES
    row = lax.broadcasted_iota(jnp.int32, (rows, total), 0) + me_e * rows
    visible = lax.broadcasted_iota(jnp.int32, (rows, total), 1) <= row
    scaling = (NOPE + ROPE) ** (-0.5)
    cols = slice(h * head_keys, (h + 1) * head_keys)
    scores = lax.dot_general(
        queries[:, cols], keys[:, cols], (((1,), (1,)), ((), ())), preferred_element_type=F32
    )
    scores = jnp.where(visible, scores * scaling, NEGATIVE)
    weight = jnp.exp(scores - jnp.max(scores, axis=-1, keepdims=True))
    sums = jnp.sum(weight, axis=-1, keepdims=True)
    mixed = jnp.dot(
        weight.astype(BF16), values[:, h * VDIM : (h + 1) * VDIM], preferred_element_type=F32
    )
    out[:, h * VDIM : (h + 1) * VDIM] = (mixed / sums).astype(BF16)


def return_kernel(
    n_ep,
    n_tp,
    arrived,
    gate_hbm,
    up_hbm,
    down_hbm,
    mix,
    mpart,
    eout,
    mout,
    gate_w,
    up_w,
    down_w,
    load_sem,
    part,
    ca,
    sums,
    ya,
    res,
    ret,
    mca,
    msums,
    mya,
    ca_s,
    ca_r,
    ya_s,
    ya_r,
    ep_s,
    ep_r,
    oy_s,
    oy_r,
    oc_s,
    oc_r,
):
    me_e = lax.axis_index("ep")
    me_t = lax.axis_index("tp")
    n_y = n_tp // CORES
    y = me_t // CORES
    c = lax.rem(me_t, CORES)
    mate = y * CORES + (1 - c)
    width = res.shape[2]
    capacity = res.shape[1]
    pairs = n_ep // 2
    parity = lax.rem(me_e, 2)
    loads = []
    for n, (src, dst) in enumerate(((gate_hbm, gate_w), (up_hbm, up_w), (down_hbm, down_w))):
        copy = pltpu.make_async_copy(src.at[0], dst, load_sem.at[n])
        copy.start()
        loads.append(copy)

    def twin(i):
        return parity if i % 2 == 0 else 1 - parity

    def dest(i):
        return lax.rem(me_e // 2 + i // 2, pairs) * 2 + twin(i)

    def source(i):
        return lax.rem(me_e // 2 - i // 2 + pairs, pairs) * 2 + twin(i)

    def cols(t):
        return pl.ds(pl.multiple_of(t * width, LANES), width)

    def part_at(i, t):
        if i == n_ep:
            return mpart.at[:, cols(t)]
        return part.at[dest(i), :, cols(t)]

    def part_load(i, t):
        if i == n_ep:
            return mpart[:, cols(t)].astype(F32)
        return part[dest(i), :, cols(t)].astype(F32)

    enter(n_ep, n_tp, me_e, me_t)
    sends = []

    def go(copy):
        copy.start()
        sends.append(copy)

    def core_copy(i, k):
        dst = mca.at[k] if i == n_ep else ca.at[i, k]
        return remote(
            part_at(i, lax.rem(y + k, n_y) * CORES + (1 - c)),
            dst,
            ca_s.at[i, k],
            ca_r.at[i, k],
            me_e,
            mate,
        )

    def y_copy(i, k):
        src, dst = (msums, mya) if i == n_ep else (sums.at[i], ya.at[i])
        to = lax.rem(y + k, n_y) * CORES + c
        return remote(src.at[k - 1], dst.at[k - 1], ya_s.at[i, k], ya_r.at[i, k], me_e, to)

    def core_step(i):
        for k in list(range(1, n_y)) + [0]:
            go(core_copy(i, k))

    def y_step(i):
        for k in range(1, n_y):
            core_copy(i, k).wait_recv()
            got = (mca[k] if i == n_ep else ca[i, k]).astype(F32)
            value = (got + part_load(i, lax.rem(y + k, n_y) * CORES + c)).astype(BF16)
            if i == n_ep:
                msums[k - 1] = value
            else:
                sums[i, k - 1] = value
            go(y_copy(i, k))

    def ep_copy(i, e):
        return remote(res.at[i], ret.at[i], ep_s.at[i], ep_r.at[i], e, me_t)

    def sum_step(i):
        core_copy(i, 0).wait_recv()
        value = (mca[0] if i == n_ep else ca[i, 0]).astype(F32) + part_load(i, me_t)
        for k in range(1, n_y):
            y_copy(i, k).wait_recv()
            value = value + (mya[k - 1] if i == n_ep else ya[i, k - 1]).astype(F32)
        if i == n_ep:
            mout[:, cols(me_t)] = value.astype(BF16)
        elif i == 0:
            ret[0] = value.astype(BF16)
        else:
            res[i] = value.astype(BF16)
            go(ep_copy(i, dest(i)))

    def expert_step(s):
        base = lax.rem(me_e // 2 + s, pairs) * 2
        rows = arrived[pl.ds(pl.multiple_of(base * capacity, 2 * capacity), 2 * capacity), :]
        if s == 1 % pairs:
            loads[0].wait()
            loads[1].wait()
        gate = jnp.minimum(jnp.dot(rows, gate_w[...], preferred_element_type=F32), CLAMP_LIMIT)
        up = jnp.clip(
            jnp.dot(rows, up_w[...], preferred_element_type=F32), -CLAMP_LIMIT, CLAMP_LIMIT
        )
        hidden = ((up + 1.0) * (gate * jax.nn.sigmoid(SLOPE * gate))).astype(BF16)
        if s == 1 % pairs:
            loads[2].wait()
        value = jnp.dot(hidden, down_w[...], preferred_element_type=F32)
        part[base] = value[:capacity].astype(BF16)
        part[base + 1] = value[capacity:].astype(BF16)

    def out_copy(j, k, t, to, sem_s, sem_r):
        ref = (mout if j == 0 else eout).at[:, cols(t)]
        return remote(ref, ref, sem_s.at[j, k], sem_r.at[j, k], me_e, to)

    def out_send(j):
        for k in range(1, n_y):
            go(out_copy(j, k, me_t, lax.rem(y + k, n_y) * CORES + c, oy_s, oy_r))
        go(out_copy(j, 0, me_t, mate, oc_s, oc_r))

    core_step(n_ep)
    turns = [n % pairs for n in range(1, pairs + 1)]
    for n, turn in enumerate(turns):
        expert_step(turn)
        for i in (2 * turn, 2 * turn + 1):
            core_step(i)
        if n == 0:
            y_step(n_ep)
        for i in (2 * turn, 2 * turn + 1):
            y_step(i)
        if n > 0:
            for i in (2 * turns[n - 1], 2 * turns[n - 1] + 1):
                sum_step(i)
    sum_step(n_ep)
    out_send(0)
    for i in (1, 0):
        sum_step(i)
    acc = None
    for i in [0] + list(range(2, n_ep)) + [1]:
        if i > 0:
            ep_copy(i, source(i)).wait_recv()
        mixing = mix[source(i)]
        high = mixing.astype(BF16)
        low = (mixing - high.astype(F32)).astype(BF16)
        rows = ret[i]
        term = jnp.dot(high, rows, preferred_element_type=F32) + jnp.dot(
            low, rows, preferred_element_type=F32
        )
        acc = term if acc is None else acc + term
    eout[:, cols(me_t)] = acc.astype(BF16)
    out_send(1)
    for j in range(2):
        for k in range(1, n_y):
            t = lax.rem(y - k + n_y, n_y) * CORES + c
            out_copy(j, k, t, me_t, oy_s, oy_r).wait_recv()
            go(out_copy(j, k, t, mate, oc_s, oc_r))
    for j in range(2):
        for k in range(n_y):
            t = lax.rem(y - k + n_y, n_y) * CORES + (1 - c)
            out_copy(j, k, t, mate, oc_s, oc_r).wait_recv()
    for copy in sends:
        copy.wait_send()


def vmem(count):
    return [pl.BlockSpec(memory_space=pltpu.VMEM)] * count


def per_device(
    n_ep,
    n_tp,
    query_latent,
    shared_latent,
    rotary_key,
    query_gain,
    shared_gain,
    query_plain_weight,
    query_turn_weight,
    key_weight,
    value_weight,
    mixer_out_weight,
    expert_input,
    expert_gain,
    routing,
    routing_weight,
    gate_weight,
    up_weight,
    down_weight,
):
    me_e = lax.axis_index("ep")
    me_t = lax.axis_index("tp")
    n_y = n_tp // CORES
    row_count = query_latent.shape[0]
    heads = query_plain_weight.shape[1] // NOPE
    rank = shared_latent.shape[1]

    share = row_count // n_tp
    first = me_t * share
    lat = norm_rows(lax.dynamic_slice_in_dim(shared_latent, first, share, 0), shared_gain)
    own_position = me_e * row_count + first + jnp.arange(share, dtype=jnp.int32)
    turned = rotate_heads(
        lax.dynamic_slice_in_dim(rotary_key, first, share, 0).astype(F32), own_position
    ).astype(BF16)
    lat = jnp.concatenate([lat, turned, jnp.zeros((share, LANES - ROPE), BF16)], axis=1)

    token_count, width = expert_input.shape
    top_count = routing.shape[1]
    capacity = 4 * token_count * top_count // (3 * n_ep)
    capacity = -(-capacity // 8) * 8
    part_width = width // n_tp
    normed = norm_rows(expert_input, expert_gain)
    normed = lax.dynamic_slice_in_dim(normed, me_t * part_width, part_width, 1)
    flattened = routing.reshape(token_count * top_count)
    matches = flattened[:, None] == jnp.arange(n_ep, dtype=jnp.int32)[None, :]
    count = token_count * top_count
    lower = jnp.arange(count)[:, None] > jnp.arange(count)[None, :]
    ranking = jnp.dot(
        lower.astype(BF16), matches.astype(BF16), preferred_element_type=F32
    ).astype(jnp.int32)
    slot_index = jnp.sum(jnp.where(matches, ranking, 0), axis=1)
    target = (flattened * capacity + slot_index).reshape(token_count, top_count)
    slot_ids = jnp.arange(n_ep * capacity, dtype=jnp.int32)
    table = jnp.zeros((n_ep * capacity, token_count), jnp.bool_)
    mixing = jnp.zeros((token_count, n_ep * capacity), F32)
    for k in range(top_count):
        table = table | (target[:, k][None, :] == slot_ids[:, None])
        mixing = mixing + jnp.where(
            target[:, k][:, None] == slot_ids[None, :], routing_weight[:, k][:, None], 0.0
        )
    disp = jnp.dot(table.astype(BF16), normed, preferred_element_type=F32).astype(BF16)
    disp = disp.reshape(n_ep, capacity, part_width)
    mixing = jnp.transpose(mixing.reshape(token_count, n_ep, capacity), (1, 0, 2))

    position = me_e * row_count + jnp.arange(row_count, dtype=jnp.int32)
    query_normed = norm_rows(query_latent, query_gain)
    query_plain = jnp.dot(query_normed, query_plain_weight, preferred_element_type=F32)
    query_plain = query_plain.astype(BF16)
    query_raw = jnp.dot(query_normed, query_turn_weight, preferred_element_type=F32)
    query_turned = rotate_heads(query_raw, position).astype(BF16)
    blank = jnp.zeros((row_count, LANES - ROPE), BF16)
    pieces = []
    for h in range(heads):
        pieces.append(query_plain[:, h * NOPE : (h + 1) * NOPE])
        pieces.append(query_turned[:, h * ROPE : (h + 1) * ROPE])
        pieces.append(blank)
    queries = jnp.concatenate(pieces, axis=1)
    total = n_ep * row_count
    dma = pltpu.SemaphoreType.DMA
    arrived, mixer_partial = pl.pallas_call(
        functools.partial(gather_kernel, n_ep, n_tp, heads),
        out_shape=(
            jax.ShapeDtypeStruct((n_ep, capacity, width), BF16),
            jax.ShapeDtypeStruct((row_count, width), BF16),
        ),
        in_specs=vmem(6),
        out_specs=vmem(2),
        scratch_shapes=[
            pltpu.VMEM((n_ep, n_tp, share, rank + LANES), BF16),
            pltpu.VMEM((row_count, heads * VDIM), BF16),
            pltpu.VMEM((total, heads * (NOPE + LANES)), BF16),
            pltpu.VMEM((total, heads * VDIM), BF16),
            dma((2,)),
            dma((n_ep, 2)),
            dma((n_ep, 2)),
            dma((n_ep, n_y, 2)),
            dma((n_ep, n_y, 2)),
            dma((n_ep, n_y, 2)),
            dma((n_ep, n_y, 2)),
        ],
        compiler_params=pltpu.CompilerParams(
            collective_id=0, has_side_effects=True, vmem_limit_bytes=VMEM_LIMIT
        ),
    )(lat, disp, queries, key_weight, value_weight, mixer_out_weight)
    arrived = arrived.reshape(n_ep * capacity, width)
    units = gate_weight.shape[2]

    expert_output, mixer_output = pl.pallas_call(
        functools.partial(return_kernel, n_ep, n_tp),
        out_shape=(
            jax.ShapeDtypeStruct((token_count, width), BF16),
            jax.ShapeDtypeStruct((row_count, width), BF16),
        ),
        in_specs=vmem(1) + [pl.BlockSpec(memory_space=pl.ANY)] * 3 + vmem(2),
        out_specs=vmem(2),
        scratch_shapes=[
            pltpu.VMEM((width, units), BF16),
            pltpu.VMEM((width, units), BF16),
            pltpu.VMEM((units, width), BF16),
            dma((3,)),
            pltpu.VMEM((n_ep, capacity, width), BF16),
            pltpu.VMEM((n_ep, n_y, capacity, part_width), BF16),
            pltpu.VMEM((n_ep, n_y - 1, capacity, part_width), BF16),
            pltpu.VMEM((n_ep, n_y - 1, capacity, part_width), BF16),
            pltpu.VMEM((n_ep, capacity, part_width), BF16),
            pltpu.VMEM((n_ep, capacity, part_width), BF16),
            pltpu.VMEM((n_y, row_count, part_width), BF16),
            pltpu.VMEM((n_y - 1, row_count, part_width), BF16),
            pltpu.VMEM((n_y - 1, row_count, part_width), BF16),
            dma((n_ep + 1, n_y)),
            dma((n_ep + 1, n_y)),
            dma((n_ep + 1, n_y)),
            dma((n_ep + 1, n_y)),
            dma((n_ep,)),
            dma((n_ep,)),
            dma((2, n_y)),
            dma((2, n_y)),
            dma((2, n_y)),
            dma((2, n_y)),
        ],
        compiler_params=pltpu.CompilerParams(
            collective_id=1, has_side_effects=True, vmem_limit_bytes=VMEM_LIMIT
        ),
    )(arrived, gate_weight, up_weight, down_weight, mixing, mixer_partial)
    return (mixer_output, expert_output)


def take(src, dst, sem):
    copy = pltpu.make_async_copy(src, dst, sem)
    copy.start()
    return copy


def turn_pair(values, cosine, sine):
    half = ROPE // 2
    lane = lax.broadcasted_iota(jnp.int32, values.shape, 1)
    upper = lax.rem(lane, ROPE) >= half
    swapped = jnp.where(
        upper, pltpu.roll(values, half, 1), -pltpu.roll(values, LANES - half, 1)
    )
    return values * cosine + swapped * sine


def step_kernel(n_ep, n_tp, heads, *refs):
    (
        routing_h, share_h, ein_h, egain_h, slat_h, sgain_h, rkey_h, qlat_h, qgain_h, freq_h,
        qp_h, qt_h, kw_h, vw_h, mw_h, gate_h, up_h, down_h,
        eout_h, mout_h,
        eout, mout, keep_sem,
        routing, share, ein, egain, slat, sgain, rkey, qlat, qgain, freq,
        qp_w, qt_w, key_w, value_w, mixer_w, gate_w, up_w, down_w,
        load_sem,
        normed, ranks, weights, disp, arr, mixing,
        lat_all, queries, keys, values, top, total, mixed, out,
        part, ca, sums, ya, res, ret,
        msend, mown, mca, msum, mya,
        d_s, d_r, dy_s, dy_r, dc_s, dc_r,
        lz_s, lz_r, lx_s, lx_r, lc_s, lc_r,
        rc_s, rc_r, ry_s, ry_r, re_s, re_r,
        mc_s, mc_r, my_s, my_r, mo_s, mo_r,
        oy_s, oy_r, oc_s, oc_r,
    ) = refs
    me_e = lax.axis_index("ep")
    me_t = lax.axis_index("tp")
    depth = n_ep // 2
    z = me_e // 2
    x = lax.rem(me_e, 2)
    y = me_t // CORES
    c = lax.rem(me_t, CORES)
    mate = y * CORES + (1 - c)
    over = (1 - y) * CORES + c
    far = (1 - y) * CORES + (1 - c)
    tokens, width = ein.shape
    capacity = arr.shape[1]
    quarter = width // n_tp
    half = width // CORES
    rows = slat.shape[0]
    rank = slat.shape[1]
    head_keys = NOPE + LANES

    loads = []
    pairs = (
        (slat_h, slat), (sgain_h, sgain), (rkey_h, rkey), (freq_h, freq),
        (routing_h, routing), (share_h, share), (ein_h, ein), (egain_h, egain),
        (qlat_h, qlat), (qgain_h, qgain), (qp_h, qp_w), (qt_h, qt_w),
        (gate_h.at[0], gate_w), (up_h.at[0], up_w), (down_h.at[0], down_w),
        (kw_h, key_w), (vw_h, value_w), (mw_h, mixer_w),
    )
    for n, (src, dst) in enumerate(pairs):
        loads.append(take(src, dst, load_sem.at[n]))

    def ready(first, last):
        for n in range(first, last):
            loads[n].wait()

    def ep_at(d, f):
        return lax.rem(z + d + depth, depth) * 2 + (x if f == 0 else 1 - x)

    def cols(t):
        return pl.ds(pl.multiple_of(t * quarter, LANES), quarter)

    def side(core):
        return pl.ds(pl.multiple_of(core * half, LANES), half)

    lat_all[1:] = jnp.zeros((n_ep - 1, rows, rank + LANES), BF16)
    barrier = pltpu.get_barrier_semaphore()
    peers = [(ep_at(d, f), me_t) for d in range(depth) for f in range(2) if d or f]
    peers += [(me_e, t) for t in (mate, over)]
    for peer in peers:
        pl.semaphore_signal(
            barrier, inc=1, device_id=peer, device_id_type=pl.DeviceIdType.MESH
        )

    sends = []

    def go(copy, when=None):
        if when is None:
            copy.start()
        else:
            pl.when(when)(copy.start)
        sends.append((when, copy))

    def landed(copy, when):
        pl.when(when)(copy.wait_recv)

    lat_rows = rows // CORES

    def lat_at(i, core):
        return lat_all.at[i, pl.ds(pl.multiple_of(core * lat_rows, lat_rows), lat_rows), :]

    def lat_z(d):
        return remote(
            lat_at(2 * d - 2, c), lat_at(2 * d, c), lz_s.at[d], lz_r.at[d], ep_at(1, 0), me_t
        )

    def lat_x(d):
        return remote(
            lat_at(2 * d, c), lat_at(2 * d + 1, c), lx_s.at[d], lx_r.at[d], ep_at(0, 1), me_t
        )

    def lat_c(i, core):
        return remote(lat_at(i, core), lat_at(i, core), lc_s.at[i], lc_r.at[i], me_e, mate)

    def lat_up(d):
        if d + 1 < depth:
            go(lat_z(d + 1), jnp.logical_and(z >= d, z < depth - 1))

    def known(i):
        return x == 1 if i == 1 else z >= i // 2


    def z_arr(d):
        landed(lat_z(d), known(2 * d))
        lat_up(d)
        go(lat_x(d), known(2 * d))
        go(lat_c(2 * d, c), known(2 * d))

    def x_arr(d):
        landed(lat_x(d), known(2 * d + 1))
        go(lat_c(2 * d + 1, c), known(2 * d + 1))

    def chosen(e):
        return jnp.where(ranks[pl.ds(e, 1), :] == slot_row, 1.0, 0.0).astype(BF16)

    def disp_at(i, t):
        return arr.at[i, :, cols(t)]

    def direct(i):
        return remote(
            disp.at[i], disp_at(i, me_t), d_s.at[i], d_r.at[i], ep_at(i // 2, i % 2), me_t
        )

    kept = []

    def keep(src, dst, at):
        kept.append(take(src.at[at], dst.at[at], keep_sem.at[len(kept)]))

    def relay(i):
        direct(i).wait_recv()
        here = disp_at(i, me_t)
        go(remote(here, here, dy_s.at[i], dy_r.at[i], me_e, over))
        go(remote(here, here, dc_s.at[i, 0], dc_r.at[i, 0], me_e, mate))

    def forward(i):
        got = disp_at(i, over)
        remote(got, got, dy_s.at[i], dy_r.at[i], me_e, over).wait_recv()
        go(remote(got, got, dc_s.at[i, 1], dc_r.at[i, 1], me_e, mate))

    def arrive(i):
        for k, t in enumerate((mate, far)):
            got = disp_at(i, t)
            remote(got, got, dc_s.at[i, k], dc_r.at[i, k], me_e, mate).wait_recv()

    def project(i):
        at = slice(i * rows, (i + 1) * rows)
        latent = lat_all[i, :, :rank]
        k = jnp.dot(latent, key_w[...], preferred_element_type=F32).astype(BF16)
        values[at, :] = jnp.dot(latent, value_w[...], preferred_element_type=F32).astype(BF16)
        for h in range(heads):
            keys[at, h * head_keys : h * head_keys + NOPE] = k[:, h * NOPE : (h + 1) * NOPE]
            keys[at, h * head_keys + NOPE : (h + 1) * head_keys] = lat_all[i, :, rank:]

    def core_copy(i, k):
        t = mate if k == 0 else far
        return remote(
            part.at[i, :, cols(t)], ca.at[i, k], rc_s.at[i, k], rc_r.at[i, k], me_e, mate
        )

    def y_copy(i):
        return remote(sums.at[i], ya.at[i], ry_s.at[i], ry_r.at[i], me_e, over)

    def back(i):
        return remote(res.at[i], ret.at[i], re_s.at[i], re_r.at[i], ep_at(-(i // 2), i % 2), me_t)

    def y_step(i):
        core_copy(i, 1).wait_recv()
        sums[i] = (ca[i, 1].astype(F32) + part[i, :, cols(over)].astype(F32)).astype(BF16)
        go(y_copy(i))

    def sum_step(i):
        core_copy(i, 0).wait_recv()
        value = ca[i, 0].astype(F32) + part[i, :, cols(me_t)].astype(F32)
        y_copy(i).wait_recv()
        value = (value + ya[i].astype(F32)).astype(BF16)
        if i == 0:
            ret[0] = value
        else:
            res[i] = value
            go(back(i))

    def chunk(d):
        rows_in = arr[2 * d : 2 * d + 2].reshape(2 * capacity, width)
        gate = jnp.minimum(jnp.dot(rows_in, gate_w[...], preferred_element_type=F32), CLAMP_LIMIT)
        up = jnp.clip(
            jnp.dot(rows_in, up_w[...], preferred_element_type=F32), -CLAMP_LIMIT, CLAMP_LIMIT
        )
        hidden = ((up + 1.0) * (gate * jax.nn.sigmoid(SLOPE * gate))).astype(BF16)
        value = jnp.dot(hidden, down_w[...], preferred_element_type=F32)
        part[2 * d] = value[:capacity].astype(BF16)
        part[2 * d + 1] = value[capacity:].astype(BF16)
        for i in (2 * d, 2 * d + 1):
            for k in (1, 0):
                go(core_copy(i, k))

    log2e = 1.4426950408889634
    scaling = (NOPE + ROPE) ** (-0.5) * log2e

    def attend(h, first, last):
        at = slice(first * rows, last * rows)
        head = slice(h * head_keys, (h + 1) * head_keys)
        scores = lax.dot_general(
            queries[:, head], keys[at, head], (((1,), (1,)), ((), ())), preferred_element_type=F32
        )
        pieces = []
        for i in range(first, last):
            piece = scores[:, (i - first) * rows : (i - first + 1) * rows]
            if i == 0:
                row = lax.broadcasted_iota(jnp.int32, (rows, rows), 0)
                piece = jnp.where(
                    lax.broadcasted_iota(jnp.int32, (rows, rows), 1) <= row, piece, NEGATIVE
                )
            else:
                piece = piece + jnp.where(ep_at(-(i // 2), i % 2) < me_e, 0.0, NEGATIVE)
            pieces.append(piece)
        scores = jnp.concatenate(pieces, axis=1)
        peak = jnp.max(scores, axis=-1, keepdims=True)
        if first > 0:
            old = top[h]
            peak = jnp.maximum(peak, old)
        weight = jnp.exp2((scores - peak) * scaling)
        sum_of = jnp.sum(weight, axis=-1, keepdims=True)
        term = jnp.dot(
            weight.astype(BF16), values[at, h * VDIM : (h + 1) * VDIM], preferred_element_type=F32
        )
        if first > 0:
            fade = jnp.exp2((old - peak) * scaling)
            sum_of = sum_of + fade * total[h]
            term = term + fade * mixed[h]
        if last < n_ep:
            top[h] = peak
            total[h] = sum_of
            mixed[h] = term
        else:
            out[:, h * VDIM : (h + 1) * VDIM] = (term / sum_of).astype(BF16)

    def lat_arrive(i):
        landed(lat_c(i, 1 - c), known(i))

    acc = []

    def mix(i):
        if i > 0:
            back(i).wait_recv()
        table = mixing[i]
        high = table.astype(BF16)
        low = (table - high.astype(F32)).astype(BF16)
        term = jnp.dot(high, ret[i], preferred_element_type=F32) + jnp.dot(
            low, ret[i], preferred_element_type=F32
        )
        acc[:] = [term if not acc else acc[0] + term]

    def out_copy(k, t, to):
        ref = eout.at[:, cols(t)]
        s, r = (oy_s, oy_r) if k == 0 else (oc_s, oc_r)
        n = 0 if k < 2 else 1
        return remote(ref, ref, s.at[n], r.at[n], me_e, to)

    pieces = 4
    step = rows // pieces

    def mix_rows(n):
        return slice(n * step, (n + 1) * step)

    def mixer_core(n):
        return remote(
            msend.at[mix_rows(n)], mca.at[mix_rows(n)], mc_s.at[n], mc_r.at[n], me_e, mate
        )

    def mixer_y(n):
        return remote(
            msum.at[mix_rows(n)], mya.at[mix_rows(n)], my_s.at[n], my_r.at[n], me_e, over
        )

    def mixer_out(n, core):
        ref = mout.at[mix_rows(n), side(core)]
        return remote(ref, ref, mo_s.at[n], mo_r.at[n], me_e, mate)

    def mixer_turn(n):
        mixer_core(n).wait_recv()
        at = mix_rows(n)
        msum[at] = (mown[at] + mca[at].astype(F32)).astype(BF16)
        go(mixer_y(n))

    def mixer_end(n):
        mixer_y(n).wait_recv()
        at = mix_rows(n)
        mout[at, side(c)] = (msum[at].astype(F32) + mya[at].astype(F32)).astype(BF16)
        go(mixer_out(n, c))
        keep(mout, mout_h, (mix_rows(n), side(c)))

    middle = n_ep // 2
    ready(4, 6)
    expert = lax.broadcasted_iota(jnp.int32, (n_ep, tokens), 0)
    member = jnp.zeros((n_ep, tokens), F32)
    weight = jnp.zeros((n_ep, tokens), F32)
    for k in range(routing.shape[0]):
        named = routing[k : k + 1, :] == expert
        member = member + jnp.where(named, 1.0, 0.0)
        weight = weight + jnp.where(named, share[k : k + 1, :], 0.0)
    before = lax.broadcasted_iota(jnp.int32, (tokens, tokens), 0) < lax.broadcasted_iota(
        jnp.int32, (tokens, tokens), 1
    )
    placed = jnp.dot(
        member.astype(BF16),
        jnp.where(before, 1.0, 0.0).astype(BF16),
        preferred_element_type=F32,
    )
    placed = jnp.where(member > 0.0, placed, -1.0)
    ranks[...] = placed
    ready(6, 8)
    normed[...] = norm_rows(ein[...], egain[...][None, :])
    slot_row = lax.broadcasted_iota(jnp.int32, (capacity, tokens), 0).astype(F32)

    own_cols = normed[:, cols(me_t)]
    for d in range(depth):
        for f in range(2):
            if d or f:
                disp[2 * d + f] = jnp.dot(
                    chosen(ep_at(d, f)), own_cols, preferred_element_type=F32
                ).astype(BF16)
    pl.semaphore_wait(barrier, len(peers))
    go(direct(3))
    ready(0, 4)
    position = lax.broadcasted_iota(jnp.int32, (rows, LANES), 0) + me_e * rows
    angles = position.astype(F32) * freq[...]
    cosine = jnp.cos(angles)
    sine = jnp.sin(angles)
    latent = norm_rows(slat[...], sgain[...][None, :])
    lat_all[0, :, :rank] = latent
    key_rows = jnp.transpose(rkey[...].astype(F32))
    lat_all[0, :, rank:] = turn_pair(
        jnp.concatenate([key_rows, key_rows], axis=1), cosine, sine
    ).astype(BF16)
    go(direct(2))
    go(direct(1))
    arr[0] = jnp.dot(chosen(me_e), normed[...], preferred_element_type=F32).astype(BF16)
    placed_t = jnp.transpose(placed)
    weight_t = jnp.transpose(weight)
    lane = lax.broadcasted_iota(jnp.int32, (tokens, n_ep), 1)
    slot_col = lax.broadcasted_iota(jnp.int32, (tokens, capacity), 1).astype(F32)
    for i in range(n_ep):
        mine = lane == ep_at(i // 2, i % 2)
        place = jnp.sum(jnp.where(mine, placed_t, 0.0), axis=1, keepdims=True)
        scale = jnp.sum(jnp.where(mine, weight_t, 0.0), axis=1, keepdims=True)
        mixing[i] = jnp.where(place == slot_col, scale, 0.0)

    go(direct(7))
    lat_up(0)
    relay(3)
    relay(1)
    go(lat_x(0), x == 0)
    relay(2)
    go(direct(6))
    forward(1)
    forward(3)
    z_arr(1)
    relay(7)
    arrive(1)
    ready(15, 17)
    project(0)
    relay(6)
    forward(2)
    ready(12, 15)
    chunk(0)
    go(direct(5))
    x_arr(1)
    forward(7)
    y_step(0)
    z_arr(2)
    arrive(2)
    y_step(1)
    arrive(7)
    arrive(3)
    chunk(1)
    lat_arrive(3)
    x_arr(0)
    go(direct(4))
    project(3)
    forward(6)
    lat_arrive(2)
    project(2)
    y_step(3)
    lat_arrive(1)
    relay(5)
    ready(8, 12)
    query = norm_rows(qlat[...], qgain[...][None, :])
    plain = jnp.dot(query, qp_w[...], preferred_element_type=F32).astype(BF16)
    raw = jnp.dot(query, qt_w[...], preferred_element_type=F32)
    group = lax.broadcasted_iota(jnp.int32, (rows, LANES), 1) // ROPE
    for h in range(heads):
        j = h * ROPE // LANES
        turned = turn_pair(raw[:, j * LANES : (j + 1) * LANES], cosine, sine)
        turned = jnp.where(group == h % (LANES // ROPE), turned, 0.0)
        queries[:, h * head_keys : h * head_keys + NOPE] = plain[:, h * NOPE : (h + 1) * NOPE]
        queries[:, h * head_keys + NOPE : (h + 1) * head_keys] = turned.astype(BF16)

    project(1)
    z_arr(3)
    arrive(6)
    attend(1, 0, middle)
    chunk(3)
    x_arr(2)
    relay(4)
    y_step(2)
    attend(2, 0, middle)
    forward(5)
    y_step(6)
    lat_arrive(4)
    attend(3, 0, middle)
    lat_arrive(5)
    sum_step(3)
    attend(0, 0, middle)
    lat_arrive(6)
    x_arr(3)
    project(4)
    project(6)
    forward(4)
    project(5)
    lat_arrive(7)
    arrive(5)
    project(7)
    attend(2, middle, n_ep)
    y_step(7)
    sum_step(2)
    arrive(4)
    chunk(2)
    attend(3, middle, n_ep)
    sum_step(0)
    sum_step(6)
    mix(3)
    y_step(4)
    attend(1, middle, n_ep)
    attend(0, middle, n_ep)
    sum_step(7)
    y_step(5)
    ready(17, 18)
    msend[...] = jnp.dot(
        out[...], mixer_w[:, side(1 - c)], preferred_element_type=F32
    ).astype(BF16)
    for n in range(pieces):
        go(mixer_core(n))
    sum_step(1)
    mown[...] = jnp.dot(out[...], mixer_w[:, side(c)], preferred_element_type=F32)
    sum_step(4)
    mixer_turn(0)
    mix(6)
    mixer_turn(3)
    mix(2)
    mix(0)
    mixer_turn(1)
    mix(7)
    sum_step(5)
    mixer_turn(2)
    mix(4)
    mixer_end(3)
    mixer_end(1)
    mix(5)
    mix(1)
    mixer_end(0)
    eout[:, cols(me_t)] = acc[0].astype(BF16)
    go(out_copy(0, me_t, over))
    go(out_copy(1, me_t, mate))
    keep(eout, eout_h, (slice(None), cols(me_t)))
    mixer_end(2)
    for n in range(pieces):
        mixer_out(n, 1 - c).wait_recv()
        keep(mout, mout_h, (mix_rows(n), side(1 - c)))
    out_copy(0, over, over).wait_recv()
    go(out_copy(2, over, mate))
    keep(eout, eout_h, (slice(None), cols(over)))
    out_copy(1, mate, mate).wait_recv()
    keep(eout, eout_h, (slice(None), cols(mate)))
    out_copy(2, far, mate).wait_recv()
    keep(eout, eout_h, (slice(None), cols(far)))
    for copy in kept:
        copy.wait()
    for when, copy in sends:
        if when is None:
            copy.wait_send()
        else:
            pl.when(when)(copy.wait_send)


def fused(
    n_ep,
    n_tp,
    query_latent,
    shared_latent,
    rotary_key,
    query_gain,
    shared_gain,
    query_plain_weight,
    query_turn_weight,
    key_weight,
    value_weight,
    mixer_out_weight,
    expert_input,
    expert_gain,
    routing,
    routing_weight,
    gate_weight,
    up_weight,
    down_weight,
):
    rows, query_rank = query_latent.shape
    rank = shared_latent.shape[1]
    heads = query_plain_weight.shape[1] // NOPE
    tokens, width = expert_input.shape
    top_count = routing.shape[1]
    units = gate_weight.shape[2]
    capacity = 4 * tokens * top_count // (3 * n_ep)
    capacity = -(-capacity // 8) * 8
    quarter = width // n_tp
    half = width // CORES
    depth = n_ep // 2
    total = n_ep * rows
    lane = np.arange(LANES)
    freq = ROTARY_BASE ** (-2.0 * (lane % (ROPE // 2)) / ROPE)
    freq = jnp.asarray(freq.astype(np.float32)[None, :])
    args = (
        routing.T,
        routing_weight.T,
        expert_input,
        expert_gain,
        shared_latent,
        shared_gain,
        rotary_key.T,
        query_latent,
        query_gain,
        freq,
        query_plain_weight,
        query_turn_weight,
        key_weight,
        value_weight,
        mixer_out_weight,
        gate_weight,
        up_weight,
        down_weight,
    )
    dma = pltpu.SemaphoreType.DMA
    held = [pltpu.VMEM(a.shape[1:] if a.ndim == 3 else a.shape, a.dtype) for a in args]
    expert_output, mixer_output = pl.pallas_call(
        functools.partial(step_kernel, n_ep, n_tp, heads),
        out_shape=(
            jax.ShapeDtypeStruct((tokens, width), BF16),
            jax.ShapeDtypeStruct((rows, width), BF16),
        ),
        in_specs=[pl.BlockSpec(memory_space=pltpu.HBM)] * len(args),
        out_specs=[pl.BlockSpec(memory_space=pltpu.HBM)] * 2,
        scratch_shapes=[
            pltpu.VMEM((tokens, width), BF16),
            pltpu.VMEM((rows, width), BF16),
            dma((12,)),
        ]
        + held
        + [
            dma((len(args),)),
            pltpu.VMEM((tokens, width), BF16),
            pltpu.VMEM((n_ep, tokens), F32),
            pltpu.VMEM((n_ep, tokens), F32),
            pltpu.VMEM((n_ep, capacity, quarter), BF16),
            pltpu.VMEM((n_ep, capacity, width), BF16),
            pltpu.VMEM((n_ep, tokens, capacity), F32),
            pltpu.VMEM((n_ep, rows, rank + LANES), BF16),
            pltpu.VMEM((rows, heads * (NOPE + LANES)), BF16),
            pltpu.VMEM((total, heads * (NOPE + LANES)), BF16),
            pltpu.VMEM((total, heads * VDIM), BF16),
            pltpu.VMEM((heads, rows, 1), F32),
            pltpu.VMEM((heads, rows, 1), F32),
            pltpu.VMEM((heads, rows, VDIM), F32),
            pltpu.VMEM((rows, heads * VDIM), BF16),
            pltpu.VMEM((n_ep, capacity, width), BF16),
            pltpu.VMEM((n_ep, CORES, capacity, quarter), BF16),
            pltpu.VMEM((n_ep, capacity, quarter), BF16),
            pltpu.VMEM((n_ep, capacity, quarter), BF16),
            pltpu.VMEM((n_ep, capacity, quarter), BF16),
            pltpu.VMEM((n_ep, capacity, quarter), BF16),
            pltpu.VMEM((rows, half), BF16),
            pltpu.VMEM((rows, half), F32),
            pltpu.VMEM((rows, half), BF16),
            pltpu.VMEM((rows, half), BF16),
            pltpu.VMEM((rows, half), BF16),
            dma((n_ep,)),
            dma((n_ep,)),
            dma((n_ep,)),
            dma((n_ep,)),
            dma((n_ep, 2)),
            dma((n_ep, 2)),
            dma((depth,)),
            dma((depth,)),
            dma((depth,)),
            dma((depth,)),
            dma((n_ep,)),
            dma((n_ep,)),
            dma((n_ep, 2)),
            dma((n_ep, 2)),
            dma((n_ep,)),
            dma((n_ep,)),
            dma((n_ep,)),
            dma((n_ep,)),
            dma((4,)),
            dma((4,)),
            dma((4,)),
            dma((4,)),
            dma((4,)),
            dma((4,)),
            dma((1,)),
            dma((1,)),
            dma((2,)),
            dma((2,)),
        ],
        compiler_params=pltpu.CompilerParams(
            collective_id=2, has_side_effects=True, vmem_limit_bytes=FUSED_LIMIT
        ),
    )(*args)
    results = (mixer_output, expert_output)
    return tuple(
        pl.pallas_call(
            settle,
            out_shape=tuple(jax.ShapeDtypeStruct(r.shape, r.dtype) for r in results),
            in_specs=[pl.BlockSpec(memory_space=pltpu.HBM)] * 2,
            out_specs=[pl.BlockSpec(memory_space=pltpu.HBM)] * 2,
            scratch_shapes=[pltpu.VMEM(r.shape, r.dtype) for r in results]
            + [dma((2, PARTS)), dma((2, PARTS))],
        )(*results)
    )


def settle(first_in, second_in, first_out, second_out, first_held, second_held, in_sem, out_sem):
    arrays = ((first_in, first_held, first_out), (second_in, second_held, second_out))
    coming = []
    for j, (src, held, dst) in enumerate(arrays):
        step = held.shape[0] // PARTS
        for n in range(PARTS):
            at = slice(n * step, (n + 1) * step)
            coming.append((take(src.at[at], held.at[at], in_sem.at[j, n]), held, dst, at, j, n))
    leaving = []
    for copy, held, dst, at, j, n in coming:
        copy.wait()
        leaving.append(take(held.at[at], dst.at[at], out_sem.at[j, n]))
    for copy in leaving:
        copy.wait()


def pick(mesh):
    small = mesh.shape["tp"] == 2 * CORES and mesh.shape["ep"] == 8
    return fused if small else per_device


def solution(mesh):
    return jax.shard_map(
        functools.partial(pick(mesh), mesh.shape["ep"], mesh.shape["tp"]),
        mesh=mesh,
        in_specs=(
            P("ep", None),
            P("ep", None),
            P("ep", None),
            P(),
            P(),
            P(None, "tp"),
            P(None, "tp"),
            P(None, "tp"),
            P(None, "tp"),
            P("tp", None),
            P("ep", None),
            P(),
            P("ep", None),
            P("ep", None),
            P("ep", None, "tp"),
            P("ep", None, "tp"),
            P("ep", "tp", None),
        ),
        out_specs=(P("ep", None), P("ep", None)),
        check_vma=False,
    )
```
